128 devices in a mesh: fs: 32 (over z, y, core), tp: 4 (over x).
Axes of the slice: x: 4, y: 4, z: 4, core: 2. Of those that a mesh axis runs over, the one named last changes fastest.
Arguments:
- hidden_states: bfloat16 [2048, 2048], P('tp', 'fs'), may hold values from -6 to 6
- norm_gain: float32 [2048], P('fs'), may hold values from 0.1 to 1.9
- gate_master: float32 [8, 2048, 7168], P(None, 'fs', 'tp'), may hold values from -0.125 to 0.125
- up_master: float32 [8, 2048, 7168], P(None, 'fs', 'tp'), may hold values from -0.125 to 0.125
- down_master: float32 [8, 2048, 7168], P(None, 'fs', 'tp'), may hold values from -0.0625 to 0.0625
- expert_ids: int32 [2048, 2], P('tp'), may hold values from 0 to 7, all different within a row; in each aligned block of 512 rows (0 to 511, 512 to 1023, ...) at most 256 rows name the same one
- route_logits: float32 [2048, 2], P('tp'), may hold values from -6 to 6
Outputs:
- gate_serve: bfloat16 [8, 2048, 7168], P('tp', None, 'fs')
- up_serve: bfloat16 [8, 2048, 7168], P('tp', None, 'fs')
- down_serve: bfloat16 [8, 2048, 7168], P('tp', None, 'fs')
- combined: bfloat16 [2048, 2048], P('tp', 'fs')
The draws below stay inside these ranges and needn't reach their ends.
Inputs may be any that keep to these rules, and one draw needn't show every extreme that they name: `expert_ids`: the 2 entries of a row differ. Among the rows of one index of tp (aligned blocks of 512 rows) no expert is named more than 256 times, and in some blocks one expert is named exactly 256 times.
All inputs are finite; a program needn't handle non-finite values.
Results may differ from the reference program's by a relative error of at most 0.018.
Values may be sent and summed in bfloat16 or wider, within the bound.
A program may use at most 128 MiB of HBM per device.

```python
import math
import jax
import jax.numpy as jnp
import numpy as np
from jax import lax

D = 2048
FF = 7168
EXPERTS = 8
TOP = 2
TOK_DEV = 512
CAP = 256
TOKENS = 2048


def levels(key, dims, shards, smallest, largest):
    def one(axis_at, blocks):
        steps = jax.random.uniform(jax.random.fold_in(jax.random.fold_in(key, 6), axis_at), (blocks,), jnp.float32, smallest / len(shards), largest / len(shards))
        return jnp.repeat(jnp.exp(steps), dims[axis_at] // blocks).reshape((-1,) + (1,) * (len(dims) - axis_at - 1))

    loudness = one(*shards[0])
    for cut in shards[1:]:
        loudness = loudness * one(*cut)
    return loudness


def shared_out(key, own, number, rows, amount, top, bound, slope):
    sequence = jax.random.permutation(key, amount)
    heavy_load, ordinary = load_shares(amount, rows * top, bound, slope, True), load_shares(amount, rows * top, bound, slope, False)
    places = jnp.arange(amount)

    def named(lengths, offset_by):
        used = int((lengths > 0).sum())
        fixed = max(1, used // 4)
        passed = fixed + (places - fixed + offset_by * (used - fixed)) % max(1, amount - fixed)
        return jnp.zeros((amount,), jnp.int32).at[sequence[jnp.where(places < fixed, places, passed)]].set(jnp.asarray(lengths, jnp.int32))

    lengths = jnp.where(number % 4 == 0, named(heavy_load, number // 4), named(ordinary, number - number // 4 - 1))
    mixed = jax.random.permutation(jax.random.fold_in(own, 3), amount)
    donor, taker = mixed[0:amount // 2 * 2:2], mixed[1:amount // 2 * 2:2]
    room = jnp.minimum(lengths[donor] - 1, bound - lengths[taker]) // 2
    room = jnp.where((donor == sequence[0]) | (taker == sequence[0]) | (lengths[taker] == 0), 0, jnp.maximum(room, 0))
    passed = jax.random.randint(jax.random.fold_in(own, 4), (amount // 2,), 0, 1 << 20) % (room + 1)
    lengths = lengths.at[donor].add(-passed).at[taker].add(passed)
    labels = jnp.searchsorted(jnp.cumsum(lengths), jnp.arange(rows * top), side="right").astype(jnp.int32)
    listing = labels.reshape(top, rows).T
    listing = listing[jax.random.permutation(jax.random.fold_in(own, 1), rows)]
    offset_by = jax.random.randint(jax.random.fold_in(own, 2), (rows, 1), 0, top)
    return jnp.take_along_axis(listing, (jnp.arange(top)[None, :] + offset_by) % top, axis=1)


def load_shares(amount, total, limit, lean, full):
    loads = [(1 << 20) // math.isqrt(rank ** lean) + 1 for rank in range(1, amount + 1)]
    largest = limit if full else min(limit, max(-(-total // amount), total * loads[0] // sum(loads)))
    least = 1 if total - largest >= amount - 1 else 0
    counts, spare = [largest] + [least] * (amount - 1), total - largest - least * (amount - 1)
    while spare > 0:
        candidates = [i for i in range(1, amount) if counts[i] < largest] or [i for i in range(1, amount) if counts[i] < limit]
        whole, left = sum([loads[i] for i in candidates]), spare
        for i in candidates:
            extra = min(limit - counts[i], max(1, left * loads[i] // whole), spare)
            counts[i] = counts[i] + extra
            spare = spare - extra
    return np.array(counts)


def scatter_about(key, extent, deviation, limit, shards=(), kind=jnp.bfloat16):
    array = deviation * jax.random.normal(key, extent, jnp.float32)
    if shards:
        array = array * levels(key, extent, shards, -0.22, 0.18)
    return jnp.clip(array, -limit, limit).astype(kind)


def setup_inputs(seed: int = 0) -> dict:
    keys = jax.random.split(jax.random.key(seed), 8)
    hidden_states = scatter_about(keys[0], (TOKENS, D), 1.0, 6.0, ((0, 4), (1, 32)))
    norm_gain = jnp.clip(1.0 + 0.18 * jax.random.normal(keys[1], (D,), jnp.float32), 0.1, 1.9)
    gate_master = scatter_about(keys[2], (EXPERTS, D, FF), D ** -0.5, 0.125, ((1, 32), (2, 4)), jnp.float32)
    up_master = scatter_about(keys[3], (EXPERTS, D, FF), D ** -0.5, 0.125, ((1, 32), (2, 4)), jnp.float32)
    down_master = scatter_about(keys[4], (EXPERTS, D, FF), FF ** -0.5, 0.0625, ((1, 32), (2, 4)), jnp.float32)
    expert_ids_keys = jax.random.split(jax.random.fold_in(keys[5], 1), TOKENS // TOK_DEV)
    expert_ids_turns = jax.random.permutation(jax.random.fold_in(keys[5], 3), TOKENS // TOK_DEV)
    expert_ids = jax.vmap(lambda own, number: shared_out(jax.random.fold_in(keys[5], 2), own, number, TOK_DEV, EXPERTS, TOP, CAP, 2))(expert_ids_keys, expert_ids_turns).reshape((TOKENS, TOP))
    route_logits = scatter_about(keys[6], (TOKENS, TOP), 1.0, 6.0, ((0, 4),), jnp.float32)
    return {"hidden_states": hidden_states, "norm_gain": norm_gain, "gate_master": gate_master, "up_master": up_master, "down_master": down_master, "expert_ids": expert_ids, "route_logits": route_logits}


EPSILON = 1e-06

def reference(hidden_states, norm_gain, gate_master, up_master, down_master, expert_ids, route_logits):
    scaled = norm_gain[None, :, None]
    gate_serve = (scaled * gate_master).astype(jnp.bfloat16)
    up_serve = (scaled * up_master).astype(jnp.bfloat16)
    down_serve = down_master.astype(jnp.bfloat16)
    values = hidden_states.astype(jnp.float32)
    inv_rms = lax.rsqrt(lax.optimization_barrier(jnp.mean(values * values, axis=1, keepdims=True)) + EPSILON)
    normed = (values * inv_rms).astype(jnp.bfloat16)
    route_weight = jax.nn.softmax(route_logits, axis=1)

    def expert_output(expert):
        gate_pre = jnp.dot(normed, gate_serve[expert], preferred_element_type=jnp.float32)
        up_pre = jnp.dot(normed, up_serve[expert], preferred_element_type=jnp.float32)
        act = (jax.nn.silu(gate_pre) * up_pre).astype(jnp.bfloat16)
        return jnp.dot(act, down_serve[expert].T, preferred_element_type=jnp.float32).astype(jnp.bfloat16)
    outputs = lax.map(expert_output, jnp.arange(EXPERTS, dtype=jnp.int32))
    by_token = jnp.transpose(outputs, (1, 0, 2))
    picked = jnp.take_along_axis(by_token, expert_ids[:, :, None].astype(jnp.int32), axis=1)
    combined = lax.optimization_barrier(jnp.sum(route_weight[:, :, None] * picked.astype(jnp.float32), axis=1)).astype(jnp.bfloat16)
    return (gate_serve, up_serve, down_serve, combined)
```

```python
import functools

import jax
import jax.numpy as jnp
from jax import lax
from jax.experimental import pallas as pl
from jax.experimental.pallas import tpu as pltpu
from jax.sharding import Mesh
from jax.sharding import PartitionSpec as P

MESH = pl.DeviceIdType.MESH
EPSILON = 1e-06
FS = ("z", "y", "c")
AXES = ("z", "y", "x")
ORDERS = (("x", "y", "z"), ("y", "z", "x"), ("z", "x", "y"))
ROWS = ((0, 96), (96, 80), (176, 80))
HOPS = (1, 3, 2)
PEERS = tuple((dy, dc) for dy in HOPS + (0,) for dc in (0, 1) if (dy, dc) != (0, 0))


def here():
    return {a: lax.axis_index(a) for a in ("z", "y", "c", "x")}


def along(axis, hop):
    return lax.rem(lax.axis_index(axis) + hop, 4)


def greet(both):
    barrier = pltpu.get_barrier_semaphore()
    peers = [{a: along(a, h)} for a in ("x", "z") for h in HOPS]
    if both:
        peers += [{"y": along("y", dy), "c": lax.rem(lax.axis_index("c") + dc, 2)} for dy, dc in PEERS]
    else:
        peers += [{"y": along("y", h)} for h in HOPS] + [{"c": 1 - lax.axis_index("c")}]
    for peer in peers:
        pl.semaphore_signal(barrier, inc=1, device_id=peer, device_id_type=MESH)
    pl.semaphore_wait(barrier, len(peers))


def push(src, dst, send, recv, peer):
    return pltpu.make_async_remote_copy(
        src_ref=src, dst_ref=dst, send_sem=send, recv_sem=recv, device_id=peer, device_id_type=MESH
    )


def pack(read, p):
    first, r = divmod(7 * p, 4)
    lane = lax.broadcasted_iota(jnp.int32, (64, 128), 1)

    def turned(t):
        v = read(t)
        return pltpu.roll(v, 128 - 32 * r, 1) if r else v

    def joined(t, last):
        a = turned(t)
        if r == 0 or last:
            return a
        return jnp.where(lane < 128 - 32 * r, a, turned(t + 1))

    left = joined(first, False)
    right = joined(first + 1, r <= 1)
    tail = right[48:]
    mixed = [
        jnp.where(lane[:16] < 96, right[16 * i : 16 * i + 16], pltpu.roll(tail, 32 * (3 - i), 1))
        for i in range(3)
    ]
    return left, mixed


def spread(masters, gains, hpad, weights, landed, tokens, weight_out,
           raw, sent, over_x, over_z, near, mine, scales,
           in_sem, xs, xr, zs, zr, ys, yr, own_sem, hs, hr, gs, gr, gcs, gcr, gown, wsem, wr):
    at = here()
    x, y, z, c = at["x"], at["y"], at["z"], at["c"]
    other = {"c": 1 - c}
    loads = []
    for k in range(6):
        cp = pltpu.make_async_copy(masters[k // 2].at[:, k % 2], raw.at[k], in_sem.at[k])
        cp.start()
        loads.append(cp)
    greet(True)
    pending = []
    halves = push(hpad.at[1 - c], near, hs, hr, other)
    halves.start()

    copies = {}
    for i, h in enumerate(HOPS):
        peer = along("x", h)
        cp = push(weights.at[peer], weight_out.at[x], wsem.at[i], wr.at[i], {"x": peer})
        cp.start()
        pending.append(cp)
    own_weight = pltpu.make_async_copy(weights.at[x], weight_out.at[x], own_sem.at[6])
    own_weight.start()

    def pack_chunk(k):
        loads[k].wait()

        def one(to, carry):
            gain = gains[k // 2]

            def read(t):
                return raw[k, to, :, 128 * t : 128 * t + 128] * gain

            for p in range(8):
                left, mixed = pack(read, p)
                piece = jnp.concatenate([left] + mixed, axis=0).astype(jnp.bfloat16)
                sent[k, to, p] = piece

            return carry

        lax.fori_loop(0, 4, one, 0)

    def x_sends(k):
        out = []
        for i, h in enumerate(HOPS):
            peer = along("x", h)
            cp = push(sent.at[k, peer], over_x.at[k, x], xs.at[k, i], xr.at[k, i], {"x": peer})
            cp.start()
            out.append(cp)
        copies["x", k] = out
        over_x[k, x] = sent[k, x]

    pack_chunk(0)
    x_sends(0)
    halves.wait()
    mine[...] = hpad[c] + near[...]
    keep = pltpu.make_async_copy(mine, tokens.at[z, y, x, c], gown)
    keep.start()

    def gather_step(l, s):
        order = ORDERS[l]
        r0, nr = ROWS[l]
        index = [slice(None) if a in order[:s] else at[a] for a in AXES] + [c, pl.ds(r0, nr)]
        src = mine.at[pl.ds(r0, nr)] if s == 0 else tokens.at[tuple(index)]
        out = []
        for i, h in enumerate(HOPS):
            cp = push(src, tokens.at[tuple(index)], gs.at[l, s, i], gr.at[l, s, i],
                      {order[s]: along(order[s], h)})
            cp.start()
            out.append(cp)
        copies["g", l, s] = out

    def gathered(l, s):
        for cp in copies["g", l, s]:
            cp.wait_recv()

    for l in range(3):
        gather_step(l, 0)
    for k in range(1, 6):
        pack_chunk(k)
        x_sends(k)
    keep.wait()
    for l in range(3):
        gathered(l, 0)
        gather_step(l, 1)

    def z_step(k):
        for cp in copies["x", k]:
            cp.wait_recv()
        out = []
        for i, h in enumerate(HOPS):
            peer = along("z", h)
            cp = push(over_x.at[k, peer], over_z.at[k, z], zs.at[k, i], zr.at[k, i], {"z": peer})
            cp.start()
            out.append(cp)
        copies["z", k] = out
        over_z[k, z] = over_x[k, z]

    def y_step(k):
        for cp in copies["z", k]:
            cp.wait_recv()
        out = []
        for i, (dy, dc) in enumerate(PEERS):
            py, pc = along("y", dy), lax.rem(c + dc, 2)
            cp = push(over_z.at[k, :, py * 2 + pc], landed.at[k, :, y, c], ys.at[k, i], yr.at[k, i],
                      {"y": py, "c": pc})
            cp.start()
            out.append(cp)
        copies["y", k] = out
        cp = pltpu.make_async_copy(over_z.at[k, :, y * 2 + c], landed.at[k, :, y, c], own_sem.at[k])
        cp.start()
        copies["own", k] = cp

    def core_step(l):
        gathered(l, 2)
        r0, nr = ROWS[l]
        part = tokens.at[:, :, :, c, pl.ds(r0, nr)]
        cp = push(part, part, gcs.at[l], gcr.at[l], other)
        cp.start()
        copies["core", l] = cp

    z_step(0)
    for l in range(3):
        gathered(l, 1)
        gather_step(l, 2)
    for k in range(1, 6):
        z_step(k)
        y_step(k - 1)
        if k == 4:
            for l in range(3):
                core_step(l)
    y_step(5)

    for cp in pending:
        cp.wait()
    own_weight.wait()
    for l in range(3):
        for s in range(3):
            for cp in copies["g", l, s]:
                cp.wait_send()
        copies["core", l].wait()
    for k in range(6):
        for cp in copies["x", k] + copies["z", k]:
            cp.wait_send()
        for cp in copies["y", k]:
            cp.wait()
        copies["own", k].wait()


def spread_call(gate, up, down, gains, hpad, weights):
    def kernel(g, u, d, *rest):
        spread((g, u, d), *rest)

    any_space = pl.BlockSpec(memory_space=pl.ANY)
    vmem = pl.BlockSpec(memory_space=pltpu.VMEM)
    bf16 = jnp.bfloat16
    dma = pltpu.SemaphoreType.DMA
    return pl.pallas_call(
        kernel,
        out_shape=(
            jax.ShapeDtypeStruct((6, 4, 4, 2, 112, 128), bf16),
            jax.ShapeDtypeStruct((4, 4, 4, 2, 256, 128), bf16),
            jax.ShapeDtypeStruct((4, 8, 512), jnp.float32),
        ),
        in_specs=[any_space] * 3 + [vmem] * 2 + [any_space],
        out_specs=(any_space,) * 3,
        scratch_shapes=[
            pltpu.VMEM((6, 4, 64, 1792), jnp.float32),
            pltpu.VMEM((6, 4, 8, 112, 128), bf16),
            pltpu.VMEM((6, 4, 8, 112, 128), bf16),
            pltpu.VMEM((6, 4, 8, 112, 128), bf16),
            pltpu.VMEM((256, 128), bf16),
            pltpu.VMEM((256, 128), bf16),
            pltpu.VMEM((8, 128), jnp.float32),
            dma((6,)), dma((6, 3)), dma((6, 3)), dma((6, 3)), dma((6, 3)), dma((6, 7)), dma((6, 7)), dma((7,)),
            dma, dma, dma((3, 3, 3)), dma((3, 3, 3)), dma((3,)), dma((3,)), dma, dma((3,)), dma((3,)),
        ],
        compiler_params=pltpu.CompilerParams(
            collective_id=0, has_side_effects=True, vmem_limit_bytes=56 << 20
        ),
        name="spread",
    )(gate, up, down, gains, hpad, weights)


def mixture(landed, tokens, weights, gate_out, up_out, down_out, part_out,
            packed, rows, parts, serve, wide, wcol, in_sem, row_sem, w_sem, out_sem, part_sem, wv):
    outs = (gate_out, up_out, down_out)
    loads = []
    for k in range(6):
        cp = pltpu.make_async_copy(landed.at[k], packed.at[k], in_sem.at[k])
        cp.start()
        loads.append(cp)
    wload = pltpu.make_async_copy(weights, wv, w_sem)
    wload.start()
    row_loads = []
    for t in range(8):
        cp = pltpu.make_async_copy(tokens.at[:, pl.ds(256 * t, 256)], rows.at[:, pl.ds(256 * t, 256)], row_sem.at[t])
        cp.start()
        row_loads.append(cp)
    lane = lax.broadcasted_iota(jnp.int32, (16, 128), 1)
    stores = []
    for k in range(6):
        loads[k].wait()
        m, j = k // 2, k % 2

        def one(f, carry):
            serve[m, j, pl.ds(f * 64, 64), 0:128] = packed[k, f, 0:64]
            mixed = packed[k, f, 64:112]
            serve[m, j, pl.ds(f * 64, 48), 128:224] = mixed[:, :96]
            v = mixed.astype(jnp.float32)
            a, b, d = (pltpu.roll(v[16 * i : 16 * i + 16], 32 * (i + 1), 1) for i in range(3))
            tail = jnp.where(lane < 32, a, jnp.where(lane < 64, b, d))
            serve[m, j, pl.ds(f * 64 + 48, 16), 128:224] = tail.astype(jnp.bfloat16)[:, :96]
            return carry

        lax.fori_loop(0, 32, one, 0)
        if j == 1:
            cp = pltpu.make_async_copy(serve.at[m], outs[m], out_sem.at[m])
            cp.start()
            stores.append(cp)
    wload.wait()
    for b in range(4):
        wcol[pl.ds(512 * b, 512), 0:8] = jnp.transpose(wv[b])
    part_stores = []
    for t in range(8):
        row_loads[t].wait()

        total = jnp.zeros((256, 128), jnp.float32)
        for q in range(16):
            block = rows[q, 256 * t : 256 * t + 256]
            wide[:, 128 * q : 128 * q + 128] = block
            v = block.astype(jnp.float32)
            total = total + v * v
        mean = jnp.sum(total, axis=1, keepdims=True) / 2048.0
        inv = lax.rsqrt(mean + EPSILON)
        acts = []
        for e in range(2):
            gate_pre = jnp.dot(wide[...], serve[0, e], preferred_element_type=jnp.float32) * inv
            up_pre = jnp.dot(wide[...], serve[1, e], preferred_element_type=jnp.float32) * inv
            act = gate_pre / (1.0 + jnp.exp(-gate_pre)) * up_pre
            share = wcol[256 * t : 256 * t + 256, e : e + 1]
            acts.append((act * share).astype(jnp.bfloat16))
        dims = (((1,), (1,)), ((), ()))
        for n in range(4):
            cols = slice(512 * n, 512 * n + 512)
            out = lax.dot_general(acts[0], serve[2, 0, cols], dims, preferred_element_type=jnp.float32)
            out = out + lax.dot_general(acts[1], serve[2, 1, cols], dims, preferred_element_type=jnp.float32)
            for q in range(4):
                parts[4 * n + q, 256 * t : 256 * t + 256] = out[:, 128 * q : 128 * q + 128].astype(jnp.bfloat16)
        cp = pltpu.make_async_copy(parts.at[:, pl.ds(256 * t, 256)], part_out.at[:, pl.ds(256 * t, 256)], part_sem.at[t])
        cp.start()
        part_stores.append(cp)
    for cp in stores + part_stores:
        cp.wait()


def mixture_call(landed, tokens, weights):
    any_space = pl.BlockSpec(memory_space=pl.ANY)
    bf16 = jnp.bfloat16
    dma = pltpu.SemaphoreType.DMA
    served = jax.ShapeDtypeStruct((2, 2048, 224), bf16)
    return pl.pallas_call(
        mixture,
        out_shape=(served, served, served, jax.ShapeDtypeStruct((16, 2048, 128), bf16)),
        in_specs=[any_space] * 3,
        out_specs=(any_space,) * 4,
        scratch_shapes=[
            pltpu.VMEM((6, 32, 112, 128), bf16),
            pltpu.VMEM((16, 2048, 128), bf16),
            pltpu.VMEM((16, 2048, 128), bf16),
            pltpu.VMEM((3, 2, 2048, 224), bf16),
            pltpu.VMEM((256, 2048), bf16),
            pltpu.VMEM((2048, 128), jnp.float32),
            dma((6,)), dma((8,)), dma, dma((3,)), dma((8,)),
            pltpu.VMEM((4, 8, 512), jnp.float32),
        ],
        compiler_params=pltpu.CompilerParams(vmem_limit_bytes=60 << 20),
        name="mixture",
    )(landed, tokens, weights)


def collect(parts, out, near, held, one0, one1, one2, two0, two1, two2, three0, three1, three2,
            add0, add1, add2, sum0, sum1, sum2, last,
            load_sem, cs, cr, s_send, s_recv, f_send, f_recv):
    at = here()
    c = at["c"]
    other = {"c": 1 - c}
    greet(False)
    ones, twos, threes = (one0, one1, one2), (two0, two1, two2), (three0, three1, three2)
    adds, sums = (add0, add1, add2), (sum0, sum1, sum2)
    swaps, loads = [], []
    for l in range(3):
        rows = pl.ds(*ROWS[l])
        cp = push(parts.at[:, :, :, 1 - c, rows], near.at[:, :, :, rows], cs.at[l], cr.at[l], other)
        cp.start()
        swaps.append(cp)
        cp = pltpu.make_async_copy(parts.at[:, :, :, c, rows], held.at[:, :, :, rows], load_sem.at[l])
        cp.start()
        loads.append(cp)
    sends = []

    def send(l, s, pick, dst):
        axis = ORDERS[l][s]
        out = []
        for i, h in enumerate(HOPS):
            peer = along(axis, h)
            cp = push(pick(peer), dst.at[i], s_send.at[l, s, i], s_recv.at[l, s, i], {axis: peer})
            cp.start()
            out.append(cp)
        sends.append(out)
        return out

    first, second, third = [], [], []
    for l in range(3):
        r0, nr = ROWS[l]
        swaps[l].wait_recv()
        loads[l].wait()

        def add(i, carry):
            a, b, d = i // 16, lax.rem(i // 4, 4), lax.rem(i, 4)
            v = held[a, b, d, pl.ds(r0, nr)].astype(jnp.float32) + near[a, b, d, pl.ds(r0, nr)].astype(jnp.float32)
            held[a, b, d, pl.ds(r0, nr)] = v.astype(jnp.bfloat16)
            return carry

        lax.fori_loop(0, 64, add, 0)

        def pick(peer, l=l, r0=r0, nr=nr):
            index = [peer if a == ORDERS[l][0] else slice(None) for a in AXES] + [pl.ds(r0, nr)]
            return held.at[tuple(index)]

        first.append(send(l, 0, pick, ones[l]))
    for l in range(3):
        r0, nr = ROWS[l]
        for cp in first[l]:
            cp.wait_recv()
        rest = [a for a in AXES if a != ORDERS[l][0]]

        def add(i, carry):
            a, b = i // 4, lax.rem(i, 4)
            place = {rest[0]: a, rest[1]: b, ORDERS[l][0]: at[ORDERS[l][0]]}
            v = held[place["z"], place["y"], place["x"], pl.ds(r0, nr)].astype(jnp.float32)
            for j in range(3):
                v = v + ones[l][j, a, b].astype(jnp.float32)
            adds[l][a, b] = v.astype(jnp.bfloat16)
            return carry

        lax.fori_loop(0, 16, add, 0)

        def pick(peer, l=l, rest=rest):
            return adds[l].at[peer] if rest[0] == ORDERS[l][1] else adds[l].at[:, peer]

        second.append(send(l, 1, pick, twos[l]))
    for l in range(3):
        for cp in second[l]:
            cp.wait_recv()
        rest = [a for a in AXES if a != ORDERS[l][0]]
        lead = rest[0] == ORDERS[l][1]
        own = at[ORDERS[l][1]]
        for b in range(4):
            v = (adds[l][own, b] if lead else adds[l][b, own]).astype(jnp.float32)
            for j in range(3):
                v = v + twos[l][j, b].astype(jnp.float32)
            sums[l][b] = v.astype(jnp.bfloat16)
        third.append(send(l, 2, lambda peer, l=l: sums[l].at[peer], threes[l]))
    for l in range(3):
        r0, nr = ROWS[l]
        for cp in third[l]:
            cp.wait_recv()
        v = sums[l][at[ORDERS[l][2]]].astype(jnp.float32)
        for j in range(3):
            v = v + threes[l][j].astype(jnp.float32)
        last[pl.ds(r0, nr)] = v.astype(jnp.bfloat16)
    final = push(last, out.at[c], f_send, f_recv, other)
    final.start()
    out[c] = last[...]
    final.wait()
    for cp in swaps:
        cp.wait_send()
    for group in sends:
        for cp in group:
            cp.wait_send()


def collect_call(parts):
    bf16 = jnp.bfloat16
    dma = pltpu.SemaphoreType.DMA
    sizes = [nr for _, nr in ROWS]
    return pl.pallas_call(
        collect,
        out_shape=jax.ShapeDtypeStruct((2, 256, 128), bf16),
        in_specs=[pl.BlockSpec(memory_space=pl.ANY)],
        out_specs=pl.BlockSpec(memory_space=pltpu.VMEM),
        scratch_shapes=[pltpu.VMEM((4, 4, 4, 256, 128), bf16)] * 2
        + [pltpu.VMEM((3, 4, 4, nr, 128), bf16) for nr in sizes]
        + [pltpu.VMEM((3, 4, nr, 128), bf16) for nr in sizes]
        + [pltpu.VMEM((3, nr, 128), bf16) for nr in sizes]
        + [pltpu.VMEM((4, 4, nr, 128), bf16) for nr in sizes]
        + [pltpu.VMEM((4, nr, 128), bf16) for nr in sizes]
        + [
            pltpu.VMEM((256, 128), bf16),
            dma((3,)), dma((3,)), dma((3,)), dma((3, 3, 3)), dma((3, 3, 3)), dma, dma,
        ],
        compiler_params=pltpu.CompilerParams(
            collective_id=1, has_side_effects=True, vmem_limit_bytes=40 << 20
        ),
        name="collect",
    )(parts)


def per_device(hidden, norm_gain, gate_master, up_master, down_master, expert_ids, route_logits):
    c = lax.axis_index("c")
    gains = jnp.stack([norm_gain, norm_gain, jnp.ones_like(norm_gain)])[:, :, None]
    gains = jnp.broadcast_to(gains, (3, 64, 128))
    zero = jnp.zeros_like(hidden)
    lanes = jnp.where(
        c == 0, jnp.concatenate([hidden, zero], axis=1), jnp.concatenate([zero, hidden], axis=1)
    )
    hpad = lanes.reshape(2, 256, 128)
    weights = jax.nn.softmax(route_logits, axis=1)
    chosen = expert_ids[:, :, None] == jnp.arange(8, dtype=jnp.int32)[None, None, :]
    shares = jnp.sum(jnp.where(chosen, weights[:, :, None], 0.0), axis=1)
    shares = jnp.transpose(shares).reshape(4, 2, 512)
    shares = jnp.concatenate([shares, jnp.zeros((4, 6, 512), jnp.float32)], axis=1)
    masters = [m.reshape(4, 2, 64, 1792) for m in (gate_master, up_master, down_master)]
    landed, tokens, shares = spread_call(*masters, gains, hpad, shares)
    gate, up, down, parts = mixture_call(
        landed.reshape(6, 32, 112, 128), tokens.reshape(16, 2048, 128), shares
    )
    out = collect_call(parts.reshape(4, 4, 4, 2, 256, 128)).reshape(512, 128)
    combined = jnp.where(c == 0, out[:, :64], out[:, 64:])
    return gate, up, down, combined


def solution(mesh):
    split = Mesh(mesh.devices.reshape(4, 4, 2, mesh.shape["tp"]), ("z", "y", "c", "x"))
    weight = P(None, FS, "x")
    in_specs = (P("x", FS), P(FS), weight, weight, weight, P("x", None), P("x", None))
    served = P("x", None, FS)
    return jax.shard_map(
        per_device,
        mesh=split,
        in_specs=in_specs,
        out_specs=(served, served, served, P("x", FS)),
        check_vma=False,
    )
```

```python
import functools

import jax
import jax.numpy as jnp
from jax import lax
from jax.experimental import pallas as pl
from jax.experimental.pallas import tpu as pltpu
from jax.sharding import Mesh
from jax.sharding import PartitionSpec as P

MESH = pl.DeviceIdType.MESH
EPSILON = 1e-06
FS = ("z", "y", "c")
HOPS = (1, 3, 2)
STEPS = HOPS + (0,)
ROWS = ((0, 96), (96, 80), (176, 80))
HALVES = ((0, 128), (128, 128))
CHUNKS = 12


def along(axis, hop):
    return lax.rem(lax.axis_index(axis) + hop, 4)


def greet():
    barrier = pltpu.get_barrier_semaphore()
    c = lax.axis_index("c")
    peers = [{a: along(a, h)} for a in ("x", "z") for h in HOPS]
    peers += [{"y": along("y", h), "c": lax.rem(c + r, 2)} for r in (0, 1) for h in (STEPS if r else HOPS)]
    for peer in peers:
        pl.semaphore_signal(barrier, inc=1, device_id=peer, device_id_type=MESH)
    pl.semaphore_wait(barrier, len(peers))


def push(src, dst, send, recv, peer):
    return pltpu.make_async_remote_copy(
        src_ref=src, dst_ref=dst, send_sem=send, recv_sem=recv, device_id=peer, device_id_type=MESH
    )


def whole(gate, up, down, gain, hpad, shares,
          gate_out, up_out, down_out, out,
          raw, gains, sent, over_x, over_z, served, tokens, beside, near_shares, share_cols,
          wide, acts, give, near, held, one0, one1, one2, add0, add1, add2,
          two0, two1, two2, sum0, sum1, sum2, three0, three1, three2, last,
          ls, ps, pr, credit, xs, xr, zs, zr, ys, yr, hs, hr, ns, nr, ws, wr,
          g0s, g0r, gs, gr, cs, cr, os, ds, dr, f0s, f0r, fs, fr, ss, sr, ts, tr, es, er):
    masters = (gate, up, down)
    outs = (gate_out, up_out, down_out)
    x, y, z, c = (lax.axis_index(a) for a in ("x", "y", "z", "c"))
    other = {"c": 1 - c}
    sends = []

    def start(cp):
        cp.start()
        sends.append(cp)
        return cp

    mine = pl.ds(pl.multiple_of(c * 64, 64), 64)
    loads, pushes = {}, {}

    def fetch(m):
        for i, h in enumerate(STEPS):
            to = along("x", h)
            cp = pltpu.make_async_copy(masters[m].at[to, c], raw.at[m % 2, to, mine], ls.at[m, i])
            cp.start()
            loads[m, i] = cp

    def swap(m):
        for i, h in enumerate(STEPS):
            to = along("x", h)
            pushes[m, i] = start(
                push(masters[m].at[to, 1 - c], raw.at[m % 2, to, mine], ps.at[m, i], pr.at[m, i], other)
            )

    fetch(0)
    fetch(1)
    gains[mine] = gain[...]
    greet()
    halves = start(push(hpad.at[1 - c], beside, hs, hr, other))
    gain_swap = start(push(gain, gains.at[mine], ns, nr, other))
    swap(0)
    share_swaps = []
    for i, h in enumerate(HOPS):
        peer = along("x", h)
        share_swaps.append(start(push(shares.at[peer], near_shares.at[x], ws.at[i], wr.at[i], {"x": peer})))
    near_shares[x] = shares[x]
    swap(1)

    halves.wait_recv()
    tokens[z, y, x, c] = hpad[c] + beside[...]
    flows = {}

    def gather(l, s, axis, index):
        part = tokens.at[index]
        flows[l, s] = []
        for i, h in enumerate(HOPS):
            cp = push(part, part, gs.at[l, s, i], gr.at[l, s, i], {axis: along(axis, h)})
            flows[l, s].append(start(cp))

    def arrived(group):
        for cp in group:
            cp.wait_recv()

    own = tokens.at[z, y, x, c]
    flows["x"] = [
        start(push(own, own, g0s.at[i], g0r.at[i], {"x": along("x", h)})) for i, h in enumerate(HOPS)
    ]
    gain_swap.wait_recv()

    def pack(m):
        for i in range(4):
            loads[m, i].wait()
            pushes[m, i].wait_recv()

        def one(to, carry):
            for t in range(14):
                v = raw[m % 2, to, :, 128 * t : 128 * t + 128]
                if m < 2:
                    v = v * gains[...]
                v = jnp.transpose(v).astype(jnp.bfloat16)
                at = 128 * t
                while at < 128 * t + 128:
                    u, low = divmod(at, 112)
                    n = min(112 - low, 128 * t + 128 - at)
                    a = at - 128 * t
                    sent[m, to, u // 4, (u // 2) % 2, u % 2, low : low + n] = v[a : a + n]
                    at += n
            return carry

        lax.fori_loop(0, 4, one, 0)

    def split(k):
        return k // 4, (k // 2) % 2, k % 2

    def x_step(k):
        m, hh, rc = split(k)
        cc = lax.rem(c + rc, 2)
        flows["x", k] = [
            start(push(sent.at[m, along("x", h), :, cc, hh], over_x.at[k, x], xs.at[k, i], xr.at[k, i],
                       {"x": along("x", h)}))
            for i, h in enumerate(HOPS)
        ]
        over_x[k, x] = sent[m, x, :, cc, hh]

    def z_step(k):
        arrived(flows["x", k])
        flows["z", k] = [
            start(push(over_x.at[k, along("z", h)], over_z.at[k, z], zs.at[k, i], zr.at[k, i],
                       {"z": along("z", h)}))
            for i, h in enumerate(HOPS)
        ]
        over_z[k, z] = over_x[k, z]

    def lanes(zz):
        return pl.ds(pl.multiple_of((zz * 4 + y) * 128, 128), 128)

    def y_step(k):
        m, hh, rc = split(k)
        arrived(flows["z", k])
        rows = pl.ds(hh * 112, 112)
        flows["y", k] = []
        for i, h in enumerate(STEPS if rc else HOPS):
            py = along("y", h)
            peer = {"y": py, "c": lax.rem(c + rc, 2)}
            for zz in range(4):
                push(over_z.at[k, zz, py], served.at[m, c, rows, lanes(zz)],
                     ys.at[k, i], yr.at[k, i], peer).start()
            cp = push(over_z.at[k, :, 0], over_z.at[k, :, 0], ys.at[k, i], yr.at[k, i], peer)
            flows["y", k].append(cp)
            sends.append(cp)
        if rc == 0:
            for zz in range(4):
                served[m, c, rows, lanes(zz)] = over_z[k, zz, y]

    pack(0)
    for k in range(4):
        x_step(k)
    pl.semaphore_signal(credit, inc=1, device_id=other, device_id_type=MESH)
    fetch(2)
    arrived(flows["x"])
    gather(0, 0, "y", (z, y, slice(None), c, pl.ds(*HALVES[0])))
    gather(1, 0, "z", (z, y, slice(None), c, pl.ds(*HALVES[1])))
    pl.semaphore_wait(credit, 1)
    swap(2)
    pack(1)
    for k in range(4, 8):
        x_step(k)
    arrived(flows[0, 0])
    gather(0, 1, "z", (z, slice(None), slice(None), c, pl.ds(*HALVES[0])))
    arrived(flows[1, 0])
    gather(1, 1, "y", (slice(None), y, slice(None), c, pl.ds(*HALVES[1])))
    z_step(0)
    pack(2)
    for k in range(8, 12):
        x_step(k)
    arrived(share_swaps)
    for b in range(4):
        share_cols[pl.ds(512 * b, 512), 0:8] = jnp.transpose(near_shares[b])

    def core_step(l):
        arrived(flows[l, 1])
        part = tokens.at[:, :, :, c, pl.ds(*HALVES[l])]
        flows["c", l] = [start(push(part, part, cs.at[l], cr.at[l], other))]

    stores = []

    def store(m):
        cp = pltpu.make_async_copy(served.at[m], outs[m], os.at[m])
        cp.start()
        stores.append(cp)

    def act_tile(t, carry):
        xb, ch = t // 2, lax.rem(t, 2)
        total = jnp.zeros((256, 128), jnp.float32)
        for q in range(16):
            block = tokens[q // 4, q % 4, xb, ch]
            wide[:, 128 * q : 128 * q + 128] = block
            v = block.astype(jnp.float32)
            total = total + v * v
        inv = lax.rsqrt(jnp.sum(total, axis=1, keepdims=True) / 2048.0 + EPSILON)
        dims = (((1,), (1,)), ((), ()))
        rows = pl.ds(pl.multiple_of(t * 256, 256), 256)
        for e in range(2):
            gate_pre = lax.dot_general(wide[...], served[0, e], dims, preferred_element_type=jnp.float32) * inv
            up_pre = lax.dot_general(wide[...], served[1, e], dims, preferred_element_type=jnp.float32) * inv
            act = gate_pre / (1.0 + jnp.exp(-gate_pre)) * up_pre
            acts[e, rows] = (act * share_cols[rows, e : e + 1]).astype(jnp.bfloat16)
        return carry

    for k in range(1, 10):
        z_step(k)
        y_step(k - 1)
        if k in (6, 7):
            core_step(k - 6)
    for l in range(2):
        arrived(flows["c", l])
    for k in range(8):
        arrived(flows["y", k])
    store(0)
    store(1)
    lax.fori_loop(0, 3, act_tile, 0)
    z_step(10)
    y_step(9)
    lax.fori_loop(3, 6, act_tile, 0)
    z_step(11)
    y_step(10)
    lax.fori_loop(6, 8, act_tile, 0)
    y_step(11)
    for k in range(8, 12):
        arrived(flows["y", k])
    store(2)

    def down_part(t, n):
        rows = pl.ds(pl.multiple_of(t * 256, 256), 256)
        cols = slice(512 * n, 512 * n + 512)
        v = jnp.dot(acts[0, rows], served[2, 0, :, cols], preferred_element_type=jnp.float32)
        return v + jnp.dot(acts[1, rows], served[2, 1, :, cols], preferred_element_type=jnp.float32)

    given = []
    for i, h in enumerate(STEPS):
        t = along("x", h) * 2 + 1 - c
        for n in range(4):
            v = down_part(t, n)
            for b in range(4):
                give[i, n, b] = v[:, 128 * b : 128 * b + 128].astype(jnp.bfloat16)
        given.append(start(push(give.at[i], near.at[i], ds.at[i], dr.at[i], other)))
    r0, r1, r2 = (pl.ds(*r) for r in ROWS)
    first = ([], [], [])
    every = slice(None)
    for i, h in enumerate(STEPS):
        t = along("x", h) * 2 + c
        arrived([given[i]])
        for n in range(4):
            v = down_part(t, n)
            for b in range(4):
                total = v[:, 128 * b : 128 * b + 128] + near[i, n, b].astype(jnp.float32)
                held[n, b, i] = total.astype(jnp.bfloat16)
        if i < 3:
            first[0].append(
                start(push(held.at[every, every, i, r0], one0.at[i], f0s.at[i], f0r.at[i], {"x": along("x", h)}))
            )
        for j, g in enumerate(HOPS):
            py, pz = along("y", g), along("z", g)
            first[1].append(
                start(push(held.at[every, py, i, r1], one1.at[j, :, i], fs.at[0, i, j], fr.at[0, i, j], {"y": py}))
            )
            first[2].append(
                start(push(held.at[pz, every, i, r2], one2.at[j, :, i], fs.at[1, i, j], fr.at[1, i, j], {"z": pz}))
            )

    def summed(base, terms):
        v = base.astype(jnp.float32)
        for term in terms:
            v = v + term.astype(jnp.float32)
        return v

    def add_first(l, one, add, base):
        arrived(first[l])

        def body(n, carry):
            a, b = n // 4, lax.rem(n, 4)
            add[a, b] = summed(base(a, b), [one[j, a, b] for j in range(3)]).astype(jnp.bfloat16)
            return carry

        lax.fori_loop(0, 16, body, 0)

    second, third = [], []
    add_first(0, one0, add0, lambda a, b: held[a, b, 3, r0])
    second.append([
        start(push(add0.at[:, along("y", h)], two0.at[j], ss.at[0, j], sr.at[0, j], {"y": along("y", h)}))
        for j, h in enumerate(HOPS)
    ])
    add_first(1, one1, add1, lambda a, b: held[a, y, b, r1])
    second.append([
        start(push(add1.at[along("z", h)], two1.at[j], ss.at[1, j], sr.at[1, j], {"z": along("z", h)}))
        for j, h in enumerate(HOPS)
    ])
    add_first(2, one2, add2, lambda a, b: held[z, a, b, r2])
    second.append([
        start(push(add2.at[:, j], two2.at[j], ss.at[2, j], sr.at[2, j], {"x": along("x", h)}))
        for j, h in enumerate(HOPS)
    ])

    def add_second(l, two, into, base):
        arrived(second[l])
        for a in range(4):
            into[a] = summed(base(a), [two[j, a] for j in range(3)]).astype(jnp.bfloat16)

    add_second(0, two0, sum0, lambda a: add0[a, y])
    third.append([
        start(push(sum0.at[along("z", h)], three0.at[j], ts.at[0, j], tr.at[0, j], {"z": along("z", h)}))
        for j, h in enumerate(HOPS)
    ])
    add_second(1, two1, sum1, lambda a: add1[z, a])
    third.append([
        start(push(sum1.at[j], three1.at[j], ts.at[1, j], tr.at[1, j], {"x": along("x", h)}))
        for j, h in enumerate(HOPS)
    ])
    add_second(2, two2, sum2, lambda a: add2[a, 3])
    third.append([
        start(push(sum2.at[along("y", h)], three2.at[j], ts.at[2, j], tr.at[2, j], {"y": along("y", h)}))
        for j, h in enumerate(HOPS)
    ])
    for l, (three, base) in enumerate(((three0, sum0[z]), (three1, sum1[3]), (three2, sum2[y]))):
        arrived(third[l])
        last[pl.ds(*ROWS[l])] = summed(base, [three[j] for j in range(3)]).astype(jnp.bfloat16)
    final = start(push(last, out.at[c], es, er, other))
    out[c] = last[...]
    final.wait_recv()
    for cp in sends:
        cp.wait_send()
    for cp in stores:
        cp.wait()


def whole_call(gate, up, down, gain, hpad, shares):
    any_space = pl.BlockSpec(memory_space=pl.ANY)
    vmem = pl.BlockSpec(memory_space=pltpu.VMEM)
    bf16, f32 = jnp.bfloat16, jnp.float32
    dma = pltpu.SemaphoreType.DMA
    sizes = [n for _, n in ROWS]
    served = jax.ShapeDtypeStruct((2, 224, 2048), bf16)

    def buffers(*shapes):
        return [pltpu.VMEM(s, bf16) for s in shapes]

    return pl.pallas_call(
        whole,
        out_shape=(served, served, served, jax.ShapeDtypeStruct((2, 256, 128), bf16)),
        in_specs=[any_space] * 3 + [vmem] * 3,
        out_specs=(any_space,) * 3 + (vmem,),
        scratch_shapes=[pltpu.VMEM((2, 4, 128, 1792), f32), pltpu.VMEM((128, 128), f32)]
        + buffers((3, 4, 4, 2, 2, 112, 128), (CHUNKS, 4, 4, 112, 128), (CHUNKS, 4, 4, 112, 128),
                  (3, 2, 224, 2048), (4, 4, 4, 2, 256, 128), (256, 128))
        + [pltpu.VMEM((4, 8, 512), f32), pltpu.VMEM((2048, 128), f32)]
        + buffers((256, 2048), (2, 2048, 224), (4, 4, 4, 256, 128), (4, 4, 4, 256, 128), (4, 4, 4, 256, 128))
        + buffers(*[(3, 4, 4, n, 128) for n in sizes])
        + buffers(*[(4, 4, n, 128) for n in sizes])
        + buffers(*[(3, 4, n, 128) for n in sizes])
        + buffers(*[(4, n, 128) for n in sizes])
        + buffers(*[(3, n, 128) for n in sizes])
        + buffers((256, 128))
        + [dma((3, 4)), dma((3, 4)), dma((3, 4)), pltpu.SemaphoreType.REGULAR]
        + [dma((CHUNKS, 3))] * 4
        + [dma((CHUNKS, 4))] * 2
        + [dma] * 4
        + [dma((3,))] * 2
        + [dma((3,))] * 2
        + [dma((2, 2, 3))] * 2
        + [dma((2,))] * 2
        + [dma((3,))]
        + [dma((4,))] * 2
        + [dma((3,))] * 2
        + [dma((2, 4, 3))] * 2
        + [dma((3, 3))] * 4
        + [dma] * 2,
        compiler_params=pltpu.CompilerParams(
            collective_id=0, has_side_effects=True, vmem_limit_bytes=67043328
        ),
        name="whole",
    )(gate, up, down, gain, hpad, shares)


def per_device(hidden, norm_gain, gate_master, up_master, down_master, expert_ids, route_logits):
    c = lax.axis_index("c")
    gain = jnp.broadcast_to(norm_gain[:, None], (64, 128))
    zero = jnp.zeros_like(hidden)
    lanes = jnp.where(
        c == 0, jnp.concatenate([hidden, zero], axis=1), jnp.concatenate([zero, hidden], axis=1)
    )
    hpad = lanes.reshape(2, 256, 128)
    weights = jax.nn.softmax(route_logits, axis=1)
    chosen = expert_ids[:, :, None] == jnp.arange(8, dtype=jnp.int32)[None, None, :]
    shares = jnp.sum(jnp.where(chosen, weights[:, :, None], 0.0), axis=1)
    shares = jnp.transpose(shares).reshape(4, 2, 512)
    shares = jnp.concatenate([shares, jnp.zeros((4, 6, 512), jnp.float32)], axis=1)
    masters = [m.reshape(4, 2, 64, 1792) for m in (gate_master, up_master, down_master)]
    gate, up, down, out = whole_call(*masters, gain, hpad, shares)
    out = out.reshape(512, 128)
    combined = jnp.where(c == 0, out[:, :64], out[:, 64:])
    return jnp.swapaxes(gate, 1, 2), jnp.swapaxes(up, 1, 2), jnp.swapaxes(down, 1, 2), combined


def solution(mesh):
    split = Mesh(mesh.devices.reshape(4, 4, 2, mesh.shape["tp"]), ("z", "y", "c", "x"))
    weight = P(None, FS, "x")
    in_specs = (P("x", FS), P(FS), weight, weight, weight, P("x", None), P("x", None))
    served = P("x", None, FS)
    return jax.shard_map(
        per_device,
        mesh=split,
        in_specs=in_specs,
        out_specs=(served, served, served, P("x", FS)),
        check_vma=False,
    )
```

```python
import functools

import jax
import jax.numpy as jnp
from jax import lax
from jax.experimental import pallas as pl
from jax.experimental.pallas import tpu as pltpu
from jax.sharding import Mesh
from jax.sharding import PartitionSpec as P

MESH = pl.DeviceIdType.MESH
EPSILON = 1e-06
FS = ("z", "y", "c")
HOPS = (1, 3, 2)
STEPS = HOPS + (0,)
ROWS = ((0, 96), (96, 80), (176, 80))
HALVES = ((0, 128), (128, 128))
CHUNKS = 12


def along(axis, hop):
    return lax.rem(lax.axis_index(axis) + hop, 4)


def greet():
    barrier = pltpu.get_barrier_semaphore()
    c = lax.axis_index("c")
    peers = [{a: along(a, h)} for a in ("x", "z") for h in HOPS]
    peers += [{"y": along("y", h), "c": lax.rem(c + r, 2)} for r in (0, 1) for h in (STEPS if r else HOPS)]
    for peer in peers:
        pl.semaphore_signal(barrier, inc=1, device_id=peer, device_id_type=MESH)
    pl.semaphore_wait(barrier, len(peers))


def push(src, dst, send, recv, peer):
    return pltpu.make_async_remote_copy(
        src_ref=src, dst_ref=dst, send_sem=send, recv_sem=recv, device_id=peer, device_id_type=MESH
    )


def whole(gate, up, down, gain, hidden, ids, logits,
          gate_out, up_out, down_out, out,
          raw, gains, sent, over_x, over_z, served, tokens, chip, shares, near_shares, share_cols,
          wide, acts, give, near, held, one0, one1, one2, add0, add1, add2,
          two0, two1, two2, sum0, sum1, sum2, three0, three1, three2, last, turned,
          ls, ps, pr, credit, xs, xr, zs, zr, ys, yr, hs, hr, ns, nr, ws, wr,
          g0s, g0r, gs, gr, hops, hopr, cs, cr, os, ds, dr, f0s, f0r, fs, fr, ss, sr, ts, tr, es, er):
    masters = (gate, up, down)
    outs = (gate_out, up_out, down_out)
    x, y, z, c = (lax.axis_index(a) for a in ("x", "y", "z", "c"))
    other = {"c": 1 - c}
    sends = []

    def start(cp):
        cp.start()
        sends.append(cp)
        return cp

    mine = pl.ds(pl.multiple_of(c * 64, 64), 64)
    loads, pushes = {}, {}

    def fetch(m):
        for i, h in enumerate(STEPS):
            to = along("x", h)
            cp = pltpu.make_async_copy(masters[m].at[to, c], raw.at[m % 2, to, mine], ls.at[m, i])
            cp.start()
            loads[m, i] = cp

    def swap(m):
        for i, h in enumerate(STEPS):
            to = along("x", h)
            pushes[m, i] = start(
                push(masters[m].at[to, 1 - c], raw.at[m % 2, to, mine], ps.at[m, i], pr.at[m, i], other)
            )

    fetch(0)
    fetch(1)
    half = pl.ds(pl.multiple_of(c * 256, 256), 256)
    far_half = pl.ds(pl.multiple_of((1 - c) * 256, 256), 256)
    chip[mine] = hidden[:, half]
    lane = lax.broadcasted_iota(jnp.int32, (8, 128), 1)
    doubled = jnp.broadcast_to(gain[...], (8, 128))
    greet()
    halves = start(push(hidden.at[:, far_half], chip.at[mine], hs, hr, other))
    gain_swap = start(push(gain, gains, ns, nr, other))
    swap(0)

    l0, l1 = logits[0:1], logits[1:2]
    top = jnp.maximum(l0, l1)
    e0, e1 = jnp.exp(l0 - top), jnp.exp(l1 - top)
    w0, w1 = e0 / (e0 + e1), e1 / (e0 + e1)
    for to in range(4):
        expert = lax.broadcasted_iota(jnp.int32, (8, 512), 0) + 2 * to
        shares[to] = jnp.where(ids[0:1] == expert, w0, 0.0) + jnp.where(ids[1:2] == expert, w1, 0.0)
    near_shares[x] = shares[x]
    swap(1)

    halves.wait_recv()
    tokens[z, y, x, c] = jnp.transpose(chip[...].astype(jnp.float32)).astype(jnp.bfloat16)
    flows = {}

    def arrived(group):
        for cp in group:
            cp.wait_recv()

    def spot(axis, at, rows):
        return (at if axis == "z" else slice(None), at if axis == "y" else slice(None), slice(None), c, rows)

    own = tokens.at[z, y, x, c]
    flows["x"] = [
        start(push(own, own, g0s.at[i], g0r.at[i], {"x": along("x", h)})) for i, h in enumerate(HOPS)
    ]
    share_swaps = []
    for i, h in enumerate(HOPS):
        peer = along("x", h)
        share_swaps.append(start(push(shares.at[peer], near_shares.at[x], ws.at[i], wr.at[i], {"x": peer})))
    gain_swap.wait_recv()
    gains[...] = jnp.where((lane < 64) == (c == 0), doubled, gains[...])
    arrived(flows["x"])
    for l, axis in enumerate(("y", "z")):
        part = tokens.at[z, y, slice(None), c, pl.ds(*HALVES[l])]
        flows["g", l] = [
            start(push(part, part, gs.at[l, i], gr.at[l, i], {axis: along(axis, h)}))
            for i, h in enumerate(HOPS)
        ]

    def spread_out(l):
        axis = ("z", "y")[l]
        arrived(flows["g", l])
        part = tokens.at[spot(axis, lax.axis_index(axis), pl.ds(*HALVES[l]))]
        flows["n", l] = [
            start(push(part, part, hops.at[l, i], hopr.at[l, i], {axis: along(axis, h)}))
            for i, h in enumerate((1, 3))
        ]

    def pass_on(l):
        axis = ("z", "y")[l]
        first, count = HALVES[l]
        flows["p", l] = []
        for i, h in enumerate((1, 3)):
            flows["n", l][i].wait_recv()
            rows = pl.ds(first + i * (count // 2), count // 2)
            part = tokens.at[spot(axis, along(axis, 4 - h), rows)]
            cp = push(part, part, hops.at[l, 2 + i], hopr.at[l, 2 + i], {axis: along(axis, h)})
            flows["p", l].append(start(cp))

    def pack_one(m, to):
        for t in range(14):
            v = jnp.transpose(raw[m % 2, to, :, 128 * t : 128 * t + 128])
            if m < 2:
                v = v * gains[0:1]
            v = v.astype(jnp.bfloat16)
            at = 128 * t
            while at < 128 * t + 128:
                u, low = divmod(at, 112)
                n = min(112 - low, 128 * t + 128 - at)
                a = at - 128 * t
                sent[m, to, u // 4, (u // 2) % 2, u % 2, low : low + n] = v[a : a + n]
                at += n

    def pack(m):
        for i in range(4):
            loads[m, i].wait()
            pushes[m, i].wait_recv()

        def one(to, carry):
            pack_one(m, to)
            return carry

        lax.fori_loop(0, 4, one, 0)

    def split(k):
        return k // 4, (k // 2) % 2, k % 2

    def x_send(k, i):
        m, hh, rc = split(k)
        peer = along("x", HOPS[i])
        src = sent.at[m, peer, :, lax.rem(c + rc, 2), hh]
        flows["x", k].append(start(push(src, over_x.at[k, x], xs.at[k, i], xr.at[k, i], {"x": peer})))

    def x_keep(k):
        m, hh, rc = split(k)
        over_x[k, x] = sent[m, x, :, lax.rem(c + rc, 2), hh]

    def x_steps(m):
        for k in range(4 * m, 4 * m + 4):
            flows["x", k] = []
            for i in range(3):
                x_send(k, i)
        for k in range(4 * m, 4 * m + 4):
            x_keep(k)

    def z_step(k):
        arrived(flows["x", k])
        flows["z", k] = [
            start(push(over_x.at[k, along("z", h)], over_z.at[k, z], zs.at[k, i], zr.at[k, i],
                       {"z": along("z", h)}))
            for i, h in enumerate(HOPS)
        ]
        over_z[k, z] = over_x[k, z]

    def lanes(zz):
        return pl.ds(pl.multiple_of((zz * 4 + y) * 128, 128), 128)

    def y_step(k):
        m, hh, rc = split(k)
        arrived(flows["z", k])
        rows = pl.ds(hh * 112, 112)
        flows["y", k] = []
        for i, h in enumerate(STEPS if rc else HOPS):
            py = along("y", h)
            peer = {"y": py, "c": lax.rem(c + rc, 2)}
            for zz in range(4):
                push(over_z.at[k, zz, py], served.at[m, c, rows, lanes(zz)],
                     ys.at[k, i], yr.at[k, i], peer).start()
            cp = push(over_z.at[k, :, 0], over_z.at[k, :, 0], ys.at[k, i], yr.at[k, i], peer)
            flows["y", k].append(cp)
            sends.append(cp)
        if rc == 0:
            for zz in range(4):
                served[m, c, rows, lanes(zz)] = over_z[k, zz, y]

    for k in range(4):
        flows["x", k] = []
    for i, h in enumerate(STEPS):
        loads[0, i].wait()
        pushes[0, i].wait_recv()
        pack_one(0, along("x", h))
        if i < 3:
            x_send(0, i)
    for k in range(1, 4):
        for i in range(3):
            x_send(k, i)
    pl.semaphore_signal(credit, inc=1, device_id=other, device_id_type=MESH)
    fetch(2)
    for k in range(4):
        x_keep(k)
    spread_out(0)
    spread_out(1)
    pl.semaphore_wait(credit, 1)
    swap(2)
    pack(1)
    x_steps(1)
    z_step(0)
    pack(2)
    x_steps(2)
    arrived(share_swaps)
    for b in range(4):
        share_cols[pl.ds(512 * b, 512), 0:8] = jnp.transpose(near_shares[b])

    def core_step(l):
        arrived(flows["p", l])
        part = tokens.at[:, :, :, c, pl.ds(*HALVES[l])]
        flows["c", l] = [start(push(part, part, cs.at[l], cr.at[l], other))]

    stores = []

    def store(m):
        cp = pltpu.make_async_copy(served.at[m], outs[m], os.at[m])
        cp.start()
        stores.append(cp)

    def act_tile(t, carry):
        xb, ch = t // 2, lax.rem(t, 2)
        total = jnp.zeros((256, 128), jnp.float32)
        for q in range(16):
            block = tokens[q // 4, q % 4, xb, ch]
            wide[:, 128 * q : 128 * q + 128] = block
            v = block.astype(jnp.float32)
            total = total + v * v
        inv = lax.rsqrt(jnp.sum(total, axis=1, keepdims=True) / 2048.0 + EPSILON)
        dims = (((1,), (1,)), ((), ()))
        rows = pl.ds(pl.multiple_of(t * 256, 256), 256)
        for e in range(2):
            gate_pre = lax.dot_general(wide[...], served[0, e], dims, preferred_element_type=jnp.float32) * inv
            up_pre = lax.dot_general(wide[...], served[1, e], dims, preferred_element_type=jnp.float32) * inv
            act = gate_pre / (1.0 + jnp.exp(-gate_pre)) * up_pre
            acts[e, rows] = (act * share_cols[rows, e : e + 1]).astype(jnp.bfloat16)
        return carry

    for k in range(1, 10):
        z_step(k)
        y_step(k - 1)
        if k == 2:
            pass_on(0)
            pass_on(1)
        if k in (6, 7):
            core_step(k - 6)
    for l in range(2):
        arrived(flows["c", l])
    for k in range(8):
        arrived(flows["y", k])
    store(0)
    store(1)
    lax.fori_loop(0, 3, act_tile, 0)
    z_step(10)
    y_step(9)
    lax.fori_loop(3, 6, act_tile, 0)
    z_step(11)
    y_step(10)
    lax.fori_loop(6, 8, act_tile, 0)
    y_step(11)
    for k in range(8, 12):
        arrived(flows["y", k])
    store(2)

    def down_part(t, n):
        rows = pl.ds(pl.multiple_of(t * 256, 256), 256)
        cols = slice(512 * n, 512 * n + 512)
        v = jnp.dot(acts[0, rows], served[2, 0, :, cols], preferred_element_type=jnp.float32)
        return v + jnp.dot(acts[1, rows], served[2, 1, :, cols], preferred_element_type=jnp.float32)

    given = []
    for i, h in enumerate(STEPS):
        t = along("x", h) * 2 + 1 - c
        for n in range(4):
            v = down_part(t, n)
            for b in range(4):
                give[i, n, b] = v[:, 128 * b : 128 * b + 128].astype(jnp.bfloat16)
        given.append(start(push(give.at[i], near.at[i], ds.at[i], dr.at[i], other)))
    r0, r1, r2 = (pl.ds(*r) for r in ROWS)
    first = ([], [], [])
    every = slice(None)
    for i, h in enumerate(STEPS):
        t = along("x", h) * 2 + c
        arrived([given[i]])
        for n in range(4):
            v = down_part(t, n)
            for b in range(4):
                total = v[:, 128 * b : 128 * b + 128] + near[i, n, b].astype(jnp.float32)
                held[n, b, i] = total.astype(jnp.bfloat16)
        if i < 3:
            first[0].append(
                start(push(held.at[every, every, i, r0], one0.at[i], f0s.at[i], f0r.at[i], {"x": along("x", h)}))
            )
        for j, g in enumerate(HOPS):
            py, pz = along("y", g), along("z", g)
            first[1].append(
                start(push(held.at[every, py, i, r1], one1.at[j, :, i], fs.at[0, i, j], fr.at[0, i, j], {"y": py}))
            )
            first[2].append(
                start(push(held.at[pz, every, i, r2], one2.at[j, :, i], fs.at[1, i, j], fr.at[1, i, j], {"z": pz}))
            )

    def summed(base, terms):
        v = base.astype(jnp.float32)
        for term in terms:
            v = v + term.astype(jnp.float32)
        return v

    def add_first(l, one, add, base):
        arrived(first[l])

        def body(n, carry):
            a, b = n // 4, lax.rem(n, 4)
            add[a, b] = summed(base(a, b), [one[j, a, b] for j in range(3)]).astype(jnp.bfloat16)
            return carry

        lax.fori_loop(0, 16, body, 0)

    second, third = [], []
    add_first(0, one0, add0, lambda a, b: held[a, b, 3, r0])
    second.append([
        start(push(add0.at[:, along("y", h)], two0.at[j], ss.at[0, j], sr.at[0, j], {"y": along("y", h)}))
        for j, h in enumerate(HOPS)
    ])
    add_first(1, one1, add1, lambda a, b: held[a, y, b, r1])
    second.append([
        start(push(add1.at[along("z", h)], two1.at[j], ss.at[1, j], sr.at[1, j], {"z": along("z", h)}))
        for j, h in enumerate(HOPS)
    ])
    add_first(2, one2, add2, lambda a, b: held[z, a, b, r2])
    second.append([
        start(push(add2.at[:, j], two2.at[j], ss.at[2, j], sr.at[2, j], {"x": along("x", h)}))
        for j, h in enumerate(HOPS)
    ])

    def add_second(l, two, into, base):
        arrived(second[l])
        for a in range(4):
            into[a] = summed(base(a), [two[j, a] for j in range(3)]).astype(jnp.bfloat16)

    add_second(0, two0, sum0, lambda a: add0[a, y])
    third.append([
        start(push(sum0.at[along("z", h)], three0.at[j], ts.at[0, j], tr.at[0, j], {"z": along("z", h)}))
        for j, h in enumerate(HOPS)
    ])
    add_second(1, two1, sum1, lambda a: add1[z, a])
    third.append([
        start(push(sum1.at[j], three1.at[j], ts.at[1, j], tr.at[1, j], {"x": along("x", h)}))
        for j, h in enumerate(HOPS)
    ])
    add_second(2, two2, sum2, lambda a: add2[a, 3])
    third.append([
        start(push(sum2.at[along("y", h)], three2.at[j], ts.at[2, j], tr.at[2, j], {"y": along("y", h)}))
        for j, h in enumerate(HOPS)
    ])
    for l, (three, base) in enumerate(((three0, sum0[z]), (three1, sum1[3]), (three2, sum2[y]))):
        arrived(third[l])
        last[pl.ds(*ROWS[l])] = summed(base, [three[j] for j in range(3)]).astype(jnp.bfloat16)
    turned[...] = jnp.transpose(last[...].astype(jnp.float32)).astype(jnp.bfloat16)
    rest = turned.at[pl.ds(pl.multiple_of((1 - c) * 64, 64), 64)]
    final = start(push(rest, out.at[:, half], es, er, other))
    out[:, half] = turned[mine]
    final.wait_recv()
    for cp in sends:
        cp.wait_send()
    for cp in stores:
        cp.wait()


def whole_call(gate, up, down, gain, hidden, ids, logits):
    any_space = pl.BlockSpec(memory_space=pl.ANY)
    vmem = pl.BlockSpec(memory_space=pltpu.VMEM)
    bf16, f32 = jnp.bfloat16, jnp.float32
    dma = pltpu.SemaphoreType.DMA
    sizes = [n for _, n in ROWS]
    served = jax.ShapeDtypeStruct((2, 224, 2048), bf16)

    def buffers(*shapes):
        return [pltpu.VMEM(s, bf16) for s in shapes]

    return pl.pallas_call(
        whole,
        out_shape=(served, served, served, jax.ShapeDtypeStruct((64, 512), bf16)),
        in_specs=[any_space] * 3 + [vmem] * 4,
        out_specs=(any_space,) * 3 + (vmem,),
        scratch_shapes=[pltpu.VMEM((2, 4, 128, 1792), f32), pltpu.VMEM((8, 128), f32)]
        + buffers((3, 4, 4, 2, 2, 112, 128), (CHUNKS, 4, 4, 112, 128), (CHUNKS, 4, 4, 112, 128),
                  (3, 2, 224, 2048), (4, 4, 4, 2, 256, 128), (128, 256))
        + [pltpu.VMEM((4, 8, 512), f32)] * 2
        + [pltpu.VMEM((2048, 128), f32)]
        + buffers((256, 2048), (2, 2048, 224), (4, 4, 4, 256, 128), (4, 4, 4, 256, 128), (4, 4, 4, 256, 128))
        + buffers(*[(3, 4, 4, n, 128) for n in sizes])
        + buffers(*[(4, 4, n, 128) for n in sizes])
        + buffers(*[(3, 4, n, 128) for n in sizes])
        + buffers(*[(4, n, 128) for n in sizes])
        + buffers(*[(3, n, 128) for n in sizes])
        + buffers((256, 128), (128, 256))
        + [dma((3, 4)), dma((3, 4)), dma((3, 4)), pltpu.SemaphoreType.REGULAR]
        + [dma((CHUNKS, 3))] * 4
        + [dma((CHUNKS, 4))] * 2
        + [dma] * 4
        + [dma((3,))] * 2
        + [dma((3,))] * 2
        + [dma((2, 3))] * 2
        + [dma((2, 4))] * 2
        + [dma((2,))] * 2
        + [dma((3,))]
        + [dma((4,))] * 2
        + [dma((3,))] * 2
        + [dma((2, 4, 3))] * 2
        + [dma((3, 3))] * 4
        + [dma] * 2,
        compiler_params=pltpu.CompilerParams(
            collective_id=0, has_side_effects=True, vmem_limit_bytes=67043328
        ),
        name="whole",
    )(gate, up, down, gain, hidden, ids, logits)


def per_device(hidden, norm_gain, gate_master, up_master, down_master, expert_ids, route_logits):
    gain = jnp.broadcast_to(jnp.concatenate([norm_gain, norm_gain])[None, :], (8, 128))
    masters = [m.reshape(4, 2, 64, 1792) for m in (gate_master, up_master, down_master)]
    gate, up, down, out = whole_call(
        *masters, gain, jnp.transpose(hidden), jnp.transpose(expert_ids), jnp.transpose(route_logits)
    )
    return jnp.swapaxes(gate, 1, 2), jnp.swapaxes(up, 1, 2), jnp.swapaxes(down, 1, 2), jnp.transpose(out)


def solution(mesh):
    split = Mesh(mesh.devices.reshape(4, 4, 2, mesh.shape["tp"]), ("z", "y", "c", "x"))
    weight = P(None, FS, "x")
    in_specs = (P("x", FS), P(FS), weight, weight, weight, P("x", None), P("x", None))
    served = P("x", None, FS)
    return jax.shard_map(
        per_device,
        mesh=split,
        in_specs=in_specs,
        out_specs=(served, served, served, P("x", FS)),
        check_vma=False,
    )
```

```python
import functools

import jax
import jax.numpy as jnp
from jax import lax
from jax.experimental import pallas as pl
from jax.experimental.pallas import tpu as pltpu
from jax.sharding import Mesh
from jax.sharding import PartitionSpec as P

MESH = pl.DeviceIdType.MESH
EPSILON = 1e-06
FS = ("z", "y", "c")
HOPS = (1, 3, 2)
GATHER_AT = 1
STEPS = HOPS + (0,)
ROWS = ((0, 96), (96, 80), (176, 80))
ROUTES = ((0, 64, "xyz"), (64, 128, "xzy"), (192, 64, "yzx"))
CHUNKS = 12


def along(axis, hop):
    return lax.rem(lax.axis_index(axis) + hop, 4)


def greet():
    barrier = pltpu.get_barrier_semaphore()
    c = lax.axis_index("c")
    peers = [{a: along(a, h)} for a in ("x", "z") for h in HOPS]
    peers += [{"y": along("y", h), "c": lax.rem(c + r, 2)} for r in (0, 1) for h in (STEPS if r else HOPS)]
    for peer in peers:
        pl.semaphore_signal(barrier, inc=1, device_id=peer, device_id_type=MESH)
    pl.semaphore_wait(barrier, len(peers))


def push(src, dst, send, recv, peer):
    return pltpu.make_async_remote_copy(
        src_ref=src, dst_ref=dst, send_sem=send, recv_sem=recv, device_id=peer, device_id_type=MESH
    )


def whole(gate, up, down, gain, hidden, ids, logits,
          gate_out, up_out, down_out, out,
          raw, gains, sent, over_x, over_z, served, tokens, chip, shares, near_shares, share_cols,
          wide, acts, give, near, held, one0, one1, one2, add0, add1, add2,
          two0, two1, two2, sum0, sum1, sum2, three0, three1, three2, last, turned,
          ls, ps, pr, credit, xs, xr, zs, zr, ys, yr, hs, hr, ns, nr, ws, wr,
          gs, gr, hops, hopr, cs, cr, os, ds, dr, f0s, f0r, fs, fr, ss, sr, ts, tr, es, er):
    masters = (gate, up, down)
    outs = (gate_out, up_out, down_out)
    x, y, z, c = (lax.axis_index(a) for a in ("x", "y", "z", "c"))
    other = {"c": 1 - c}
    sends = []

    def start(cp):
        cp.start()
        sends.append(cp)
        return cp

    mine = pl.ds(pl.multiple_of(c * 64, 64), 64)
    loads, pushes = {}, {}

    def fetch(m):
        for i, h in enumerate(STEPS):
            to = along("x", h)
            cp = pltpu.make_async_copy(masters[m].at[to, c], raw.at[m % 2, to, mine], ls.at[m, i])
            cp.start()
            loads[m, i] = cp

    def swap(m):
        for i, h in enumerate(STEPS):
            to = along("x", h)
            pushes[m, i] = start(
                push(masters[m].at[to, 1 - c], raw.at[m % 2, to, mine], ps.at[m, i], pr.at[m, i], other)
            )

    fetch(0)
    fetch(1)
    half = pl.ds(pl.multiple_of(c * 256, 256), 256)
    far_half = pl.ds(pl.multiple_of((1 - c) * 256, 256), 256)
    chip[mine] = hidden[:, half]
    lane = lax.broadcasted_iota(jnp.int32, (8, 128), 1)
    doubled = jnp.broadcast_to(gain[...], (8, 128))
    greet()
    halves = start(push(hidden.at[:, far_half], chip.at[mine], hs, hr, other))
    gain_swap = start(push(gain, gains, ns, nr, other))
    swap(0)

    l0, l1 = logits[0:1], logits[1:2]
    top = jnp.maximum(l0, l1)
    e0, e1 = jnp.exp(l0 - top), jnp.exp(l1 - top)
    w0, w1 = e0 / (e0 + e1), e1 / (e0 + e1)
    for to in range(4):
        expert = lax.broadcasted_iota(jnp.int32, (8, 512), 0) + 2 * to
        shares[to] = jnp.where(ids[0:1] == expert, w0, 0.0) + jnp.where(ids[1:2] == expert, w1, 0.0)
    near_shares[x] = shares[x]
    halves.wait_recv()
    tokens[z, y, x, c] = jnp.transpose(chip[...].astype(jnp.float32)).astype(jnp.bfloat16)
    flows = {}
    spot = {"x": x, "y": y, "z": z}

    def arrived(group):
        for cp in group:
            cp.wait_recv()

    def part(l, s, at=None, half=None):
        first, count, order = ROUTES[l]
        if half is not None:
            first, count = first + half * (count // 2), count // 2
        where = dict(spot, **(at or {}))
        index = tuple(slice(None) if a in order[:s] else where[a] for a in "zyx")
        return tokens.at[index + (c, pl.ds(first, count))]

    def gather(l, s):
        axis = ROUTES[l][2][s]
        flows["g", l, s] = [
            start(push(part(l, s), part(l, s), gs.at[l, s, i], gr.at[l, s, i], {axis: along(axis, h)}))
            for i, h in enumerate(HOPS)
        ]

    for l in range(3):
        gather(l, 0)
    share_swaps = []
    for i, h in enumerate(HOPS):
        peer = along("x", h)
        share_swaps.append(start(push(shares.at[peer], near_shares.at[x], ws.at[i], wr.at[i], {"x": peer})))
    swap(1)
    gain_swap.wait_recv()
    gains[...] = jnp.where((lane < 64) == (c == 0), doubled, gains[...])

    def spread_out(l):
        axis = ROUTES[l][2][2]
        flows["n", l] = [
            start(push(part(l, 2), part(l, 2), hops.at[l, i], hopr.at[l, i], {axis: along(axis, h)}))
            for i, h in enumerate((1, 3))
        ]

    def pass_on(l):
        axis = ROUTES[l][2][2]
        flows["p", l] = []
        for i, h in enumerate((1, 3)):
            flows["n", l][i].wait_recv()
            block = part(l, 2, {axis: along(axis, 4 - h)}, i)
            cp = push(block, block, hops.at[l, 2 + i], hopr.at[l, 2 + i], {axis: along(axis, h)})
            flows["p", l].append(start(cp))
            if axis == "x":
                to_core(3 + i, part(l, 2, {axis: along(axis, 4 - h)}))

    def to_core(n, block):
        flows["c", n] = [start(push(block, block, cs.at[n], cr.at[n], other))]

    def pack_one(m, to):
        for t in range(14):
            v = jnp.transpose(raw[m % 2, to, :, 128 * t : 128 * t + 128])
            if m < 2:
                v = v * gains[0:1]
            v = v.astype(jnp.bfloat16)
            at = 128 * t
            while at < 128 * t + 128:
                u, low = divmod(at, 112)
                n = min(112 - low, 128 * t + 128 - at)
                a = at - 128 * t
                sent[m, to, u // 4, (u // 2) % 2, u % 2, low : low + n] = v[a : a + n]
                at += n

    def pack(m):
        for i in range(4):
            loads[m, i].wait()
            pushes[m, i].wait_recv()

        def one(to, carry):
            pack_one(m, to)
            return carry

        lax.fori_loop(0, 4, one, 0)

    def split(k):
        return k // 4, (k // 2) % 2, k % 2

    def x_send(k, i):
        m, hh, rc = split(k)
        peer = along("x", HOPS[i])
        src = sent.at[m, peer, :, lax.rem(c + rc, 2), hh]
        flows["x", k].append(start(push(src, over_x.at[k, x], xs.at[k, i], xr.at[k, i], {"x": peer})))

    def x_keep(k):
        m, hh, rc = split(k)
        over_x[k, x] = sent[m, x, :, lax.rem(c + rc, 2), hh]

    def x_steps(m):
        for k in range(4 * m, 4 * m + 4):
            flows["x", k] = []
            for i in range(3):
                x_send(k, i)
        for k in range(4 * m, 4 * m + 4):
            x_keep(k)

    def z_step(k):
        arrived(flows["x", k])
        flows["z", k] = [
            start(push(over_x.at[k, along("z", h)], over_z.at[k, z], zs.at[k, i], zr.at[k, i],
                       {"z": along("z", h)}))
            for i, h in enumerate(HOPS)
        ]
        over_z[k, z] = over_x[k, z]

    def lanes(zz):
        return pl.ds(pl.multiple_of((zz * 4 + y) * 128, 128), 128)

    def y_step(k):
        m, hh, rc = split(k)
        arrived(flows["z", k])
        rows = pl.ds(hh * 112, 112)
        flows["y", k] = []
        for i, h in enumerate(STEPS if rc else HOPS):
            py = along("y", h)
            peer = {"y": py, "c": lax.rem(c + rc, 2)}
            for zz in range(4):
                push(over_z.at[k, zz, py], served.at[m, c, rows, lanes(zz)],
                     ys.at[k, i], yr.at[k, i], peer).start()
            cp = push(over_z.at[k, :, 0], over_z.at[k, :, 0], ys.at[k, i], yr.at[k, i], peer)
            flows["y", k].append(cp)
            sends.append(cp)
        if rc == 0:
            for zz in range(4):
                served[m, c, rows, lanes(zz)] = over_z[k, zz, y]

    for k in range(4):
        flows["x", k] = []
    for i, h in enumerate(STEPS):
        loads[0, i].wait()
        pushes[0, i].wait_recv()
        pack_one(0, along("x", h))
        if i < 3:
            x_send(0, i)
        if i == GATHER_AT:
            for l in range(3):
                arrived(flows["g", l, 0])
                gather(l, 1)
    for k in range(1, 4):
        for i in range(3):
            x_send(k, i)
    pl.semaphore_signal(credit, inc=1, device_id=other, device_id_type=MESH)
    fetch(2)
    for k in range(4):
        x_keep(k)
    z_step(0)
    for l in range(2):
        arrived(flows["g", l, 1])
        spread_out(l)
    pl.semaphore_wait(credit, 1)
    swap(2)
    pack(1)
    x_steps(1)
    arrived(flows["g", 2, 1])
    to_core(2, part(2, 2))
    z_step(1)
    pack(2)
    x_steps(2)
    spread_out(2)
    arrived(share_swaps)
    for b in range(4):
        share_cols[pl.ds(512 * b, 512), 0:8] = jnp.transpose(near_shares[b])

    stores = []

    def store(m):
        cp = pltpu.make_async_copy(served.at[m], outs[m], os.at[m])
        cp.start()
        stores.append(cp)

    def act_tile(xb, ch):
        t = xb * 2 + ch
        total = jnp.zeros((256, 128), jnp.float32)
        for q in range(16):
            block = tokens[q // 4, q % 4, xb, ch]
            wide[:, 128 * q : 128 * q + 128] = block
            v = block.astype(jnp.float32)
            total = total + v * v
        inv = lax.rsqrt(jnp.sum(total, axis=1, keepdims=True) / 2048.0 + EPSILON)
        dims = (((1,), (1,)), ((), ()))
        rows = pl.ds(pl.multiple_of(t * 256, 256), 256)
        for e in range(2):
            gate_pre = lax.dot_general(wide[...], served[0, e], dims, preferred_element_type=jnp.float32) * inv
            up_pre = lax.dot_general(wide[...], served[1, e], dims, preferred_element_type=jnp.float32) * inv
            act = gate_pre / (1.0 + jnp.exp(-gate_pre)) * up_pre
            acts[e, rows] = (act * share_cols[rows, e : e + 1]).astype(jnp.bfloat16)

    def act_block(hop):
        def one(ch, carry):
            act_tile(along("x", hop), ch)
            return carry

        lax.fori_loop(0, 2, one, 0)

    for k in range(9):
        if k < 8:
            z_step(k + 2)
        if k == 1:
            pass_on(0)
            pass_on(1)
        if k in (5, 6):
            arrived(flows["p", k - 5])
            to_core(k - 5, part(k - 5, 3))
        y_step(k)
    z_step(10)
    z_step(11)
    pass_on(2)
    y_step(9)
    for k in range(8):
        arrived(flows["y", k])
    store(0)
    store(1)
    for n in range(3):
        arrived(flows["c", n])
    act_block(0)
    arrived(flows["p", 2])
    to_core(5, part(2, 2, {"x": along("x", 2)}))
    y_step(10)
    arrived(flows["c", 3])
    act_block(3)
    arrived(flows["c", 4])
    y_step(11)
    act_block(1)
    arrived(flows["c", 5])
    act_block(2)
    for k in range(8, 12):
        arrived(flows["y", k])
    store(2)

    def down_part(t, n):
        rows = pl.ds(pl.multiple_of(t * 256, 256), 256)
        cols = slice(512 * n, 512 * n + 512)
        v = jnp.dot(acts[0, rows], served[2, 0, :, cols], preferred_element_type=jnp.float32)
        return v + jnp.dot(acts[1, rows], served[2, 1, :, cols], preferred_element_type=jnp.float32)

    given = []
    for i, h in enumerate(STEPS):
        t = along("x", h) * 2 + 1 - c
        for n in range(4):
            v = down_part(t, n)
            for b in range(4):
                give[i, n, b] = v[:, 128 * b : 128 * b + 128].astype(jnp.bfloat16)
        given.append(start(push(give.at[i], near.at[i], ds.at[i], dr.at[i], other)))
    r0, r1, r2 = (pl.ds(*r) for r in ROWS)
    first = ([], [], [])
    every = slice(None)
    for i, h in enumerate(STEPS):
        t = along("x", h) * 2 + c
        arrived([given[i]])
        for n in range(4):
            v = down_part(t, n)
            for b in range(4):
                total = v[:, 128 * b : 128 * b + 128] + near[i, n, b].astype(jnp.float32)
                held[n, b, i] = total.astype(jnp.bfloat16)
        if i < 3:
            first[0].append(
                start(push(held.at[every, every, i, r0], one0.at[i], f0s.at[i], f0r.at[i], {"x": along("x", h)}))
            )
        for j, g in enumerate(HOPS):
            py, pz = along("y", g), along("z", g)
            first[1].append(
                start(push(held.at[every, py, i, r1], one1.at[j, :, i], fs.at[0, i, j], fr.at[0, i, j], {"y": py}))
            )
            first[2].append(
                start(push(held.at[pz, every, i, r2], one2.at[j, :, i], fs.at[1, i, j], fr.at[1, i, j], {"z": pz}))
            )

    def summed(base, terms):
        v = base.astype(jnp.float32)
        for term in terms:
            v = v + term.astype(jnp.float32)
        return v

    def add_first(l, one, add, base):
        arrived(first[l])

        def body(n, carry):
            a, b = n // 4, lax.rem(n, 4)
            add[a, b] = summed(base(a, b), [one[j, a, b] for j in range(3)]).astype(jnp.bfloat16)
            return carry

        lax.fori_loop(0, 16, body, 0)

    second, third = [], []
    add_first(0, one0, add0, lambda a, b: held[a, b, 3, r0])
    second.append([
        start(push(add0.at[:, along("y", h)], two0.at[j], ss.at[0, j], sr.at[0, j], {"y": along("y", h)}))
        for j, h in enumerate(HOPS)
    ])
    add_first(1, one1, add1, lambda a, b: held[a, y, b, r1])
    second.append([
        start(push(add1.at[along("z", h)], two1.at[j], ss.at[1, j], sr.at[1, j], {"z": along("z", h)}))
        for j, h in enumerate(HOPS)
    ])
    add_first(2, one2, add2, lambda a, b: held[z, a, b, r2])
    second.append([
        start(push(add2.at[:, j], two2.at[j], ss.at[2, j], sr.at[2, j], {"x": along("x", h)}))
        for j, h in enumerate(HOPS)
    ])

    def add_second(l, two, into, base):
        arrived(second[l])
        for a in range(4):
            into[a] = summed(base(a), [two[j, a] for j in range(3)]).astype(jnp.bfloat16)

    add_second(0, two0, sum0, lambda a: add0[a, y])
    third.append([
        start(push(sum0.at[along("z", h)], three0.at[j], ts.at[0, j], tr.at[0, j], {"z": along("z", h)}))
        for j, h in enumerate(HOPS)
    ])
    add_second(1, two1, sum1, lambda a: add1[z, a])
    third.append([
        start(push(sum1.at[j], three1.at[j], ts.at[1, j], tr.at[1, j], {"x": along("x", h)}))
        for j, h in enumerate(HOPS)
    ])
    add_second(2, two2, sum2, lambda a: add2[a, 3])
    third.append([
        start(push(sum2.at[along("y", h)], three2.at[j], ts.at[2, j], tr.at[2, j], {"y": along("y", h)}))
        for j, h in enumerate(HOPS)
    ])
    for l, (three, base) in enumerate(((three0, sum0[z]), (three1, sum1[3]), (three2, sum2[y]))):
        arrived(third[l])
        last[pl.ds(*ROWS[l])] = summed(base, [three[j] for j in range(3)]).astype(jnp.bfloat16)
    turned[...] = jnp.transpose(last[...].astype(jnp.float32)).astype(jnp.bfloat16)
    rest = turned.at[pl.ds(pl.multiple_of((1 - c) * 64, 64), 64)]
    final = start(push(rest, out.at[:, half], es, er, other))
    out[:, half] = turned[mine]
    final.wait_recv()
    for cp in sends:
        cp.wait_send()
    for cp in stores:
        cp.wait()


def whole_call(gate, up, down, gain, hidden, ids, logits):
    any_space = pl.BlockSpec(memory_space=pl.ANY)
    vmem = pl.BlockSpec(memory_space=pltpu.VMEM)
    bf16, f32 = jnp.bfloat16, jnp.float32
    dma = pltpu.SemaphoreType.DMA
    sizes = [n for _, n in ROWS]
    served = jax.ShapeDtypeStruct((2, 224, 2048), bf16)

    def buffers(*shapes):
        return [pltpu.VMEM(s, bf16) for s in shapes]

    return pl.pallas_call(
        whole,
        out_shape=(served, served, served, jax.ShapeDtypeStruct((64, 512), bf16)),
        in_specs=[any_space] * 3 + [vmem] * 4,
        out_specs=(any_space,) * 3 + (vmem,),
        scratch_shapes=[pltpu.VMEM((2, 4, 128, 1792), f32), pltpu.VMEM((8, 128), f32)]
        + buffers((3, 4, 4, 2, 2, 112, 128), (CHUNKS, 4, 4, 112, 128), (CHUNKS, 4, 4, 112, 128),
                  (3, 2, 224, 2048), (4, 4, 4, 2, 256, 128), (128, 256))
        + [pltpu.VMEM((4, 8, 512), f32)] * 2
        + [pltpu.VMEM((2048, 128), f32)]
        + buffers((256, 2048), (2, 2048, 224), (4, 4, 4, 256, 128), (4, 4, 4, 256, 128), (4, 4, 4, 256, 128))
        + buffers(*[(3, 4, 4, n, 128) for n in sizes])
        + buffers(*[(4, 4, n, 128) for n in sizes])
        + buffers(*[(3, 4, n, 128) for n in sizes])
        + buffers(*[(4, n, 128) for n in sizes])
        + buffers(*[(3, n, 128) for n in sizes])
        + buffers((256, 128), (128, 256))
        + [dma((3, 4)), dma((3, 4)), dma((3, 4)), pltpu.SemaphoreType.REGULAR]
        + [dma((CHUNKS, 3))] * 4
        + [dma((CHUNKS, 4))] * 2
        + [dma] * 4
        + [dma((3,))] * 2
        + [dma((3, 2, 3))] * 2
        + [dma((3, 4))] * 2
        + [dma((6,))] * 2
        + [dma((3,))]
        + [dma((4,))] * 2
        + [dma((3,))] * 2
        + [dma((2, 4, 3))] * 2
        + [dma((3, 3))] * 4
        + [dma] * 2,
        compiler_params=pltpu.CompilerParams(
            collective_id=0, has_side_effects=True, vmem_limit_bytes=67043328
        ),
        name="whole",
    )(gate, up, down, gain, hidden, ids, logits)


def per_device(hidden, norm_gain, gate_master, up_master, down_master, expert_ids, route_logits):
    gain = jnp.broadcast_to(jnp.concatenate([norm_gain, norm_gain])[None, :], (8, 128))
    masters = [m.reshape(4, 2, 64, 1792) for m in (gate_master, up_master, down_master)]
    gate, up, down, out = whole_call(
        *masters, gain, jnp.transpose(hidden), jnp.transpose(expert_ids), jnp.transpose(route_logits)
    )
    return jnp.swapaxes(gate, 1, 2), jnp.swapaxes(up, 1, 2), jnp.swapaxes(down, 1, 2), jnp.transpose(out)


def solution(mesh):
    split = Mesh(mesh.devices.reshape(4, 4, 2, mesh.shape["tp"]), ("z", "y", "c", "x"))
    weight = P(None, FS, "x")
    in_specs = (P("x", FS), P(FS), weight, weight, weight, P("x", None), P("x", None))
    served = P("x", None, FS)
    return jax.shard_map(
        per_device,
        mesh=split,
        in_specs=in_specs,
        out_specs=(served, served, served, P("x", FS)),
        check_vma=False,
    )
```

```python
import functools

import jax
import jax.numpy as jnp
from jax import lax
from jax.experimental import pallas as pl
from jax.experimental.pallas import tpu as pltpu
from jax.sharding import Mesh
from jax.sharding import PartitionSpec as P

MESH = pl.DeviceIdType.MESH
EPSILON = 1e-06
FS = ("z", "y", "c")
HOPS = (1, 3, 2)
STEPS = HOPS + (0,)
ROWS = ((0, 96), (96, 80), (176, 80))
ROUTES = ((0, 64, "xyz"), (64, 96, "xzy"), (160, 96, "zyx"))
CHUNKS = 12


def along(axis, hop):
    return lax.rem(lax.axis_index(axis) + hop, 4)


def greet():
    barrier = pltpu.get_barrier_semaphore()
    c = lax.axis_index("c")
    peers = [{a: along(a, h)} for a in ("x", "z") for h in HOPS]
    peers += [{"y": along("y", h), "c": lax.rem(c + r, 2)} for r in (0, 1) for h in (STEPS if r else HOPS)]
    for peer in peers:
        pl.semaphore_signal(barrier, inc=1, device_id=peer, device_id_type=MESH)
    pl.semaphore_wait(barrier, len(peers))


def push(src, dst, send, recv, peer):
    return pltpu.make_async_remote_copy(
        src_ref=src, dst_ref=dst, send_sem=send, recv_sem=recv, device_id=peer, device_id_type=MESH
    )


def whole(gate, up, down, gain, hidden, ids, logits,
          gate_out, up_out, down_out, out,
          raw, doubled, gains, sent, over_x, over_z, served, tokens, chip, shares, near_shares, share_cols,
          wide, acts, give, near, held, one0, one1, one2, add0, add1, add2,
          two0, two1, two2, sum0, sum1, sum2, three0, three1, three2, last, turned,
          ls, ps, pr, credit, xs, xr, zs, zr, ys, yr, hs, hr, ns, nr, ws, wr,
          gs, gr, hops, hopr, cs, cr, os, ds, dr, fs, fr, ss, sr, ts, tr, es, er):
    masters = (gate, up, down)
    outs = (gate_out, up_out, down_out)
    x, y, z, c = (lax.axis_index(a) for a in ("x", "y", "z", "c"))
    other = {"c": 1 - c}
    sends = []

    def start(cp):
        cp.start()
        sends.append(cp)
        return cp

    def bulk(ref, send, recv):
        return push(ref, ref, send, recv, other)

    mine = pl.ds(pl.multiple_of(c * 64, 64), 64)
    def slot(m, i):
        return i if m == 0 else 3 + m

    def fetch(m):
        for i, h in enumerate(STEPS):
            to = along("x", h)
            pltpu.make_async_copy(masters[m].at[to, c], raw.at[m % 2, to, mine], ls.at[slot(m, i)]).start()

    def swap(m):
        for i, h in enumerate(STEPS):
            to = along("x", h)
            push(masters[m].at[to, 1 - c], raw.at[m % 2, to, mine], ps, pr.at[slot(m, i)], other).start()

    def loaded(m, i):
        block = raw.at[0, 0, mine] if m == 0 else raw.at[0, :, mine]
        pltpu.make_async_copy(block, block, ls.at[slot(m, i)]).wait()
        bulk(block, ps, pr.at[slot(m, i)]).wait_recv()

    fetch(0)
    fetch(1)
    half = pl.ds(pl.multiple_of(c * 256, 256), 256)
    far_half = pl.ds(pl.multiple_of((1 - c) * 256, 256), 256)
    chip[mine] = hidden[:, half]
    lane = lax.broadcasted_iota(jnp.int32, (8, 128), 1)
    row = jnp.broadcast_to(gain[...], (8, 64))
    doubled[...] = jnp.concatenate([row, row], axis=1)
    greet()
    halves = start(push(hidden.at[:, far_half], chip.at[mine], hs, hr, other))
    gain_swap = start(push(doubled, gains, ns, nr, other))
    swap(0)

    l0, l1 = logits[0:1], logits[1:2]
    top = jnp.maximum(l0, l1)
    e0, e1 = jnp.exp(l0 - top), jnp.exp(l1 - top)
    w0, w1 = e0 / (e0 + e1), e1 / (e0 + e1)
    for to in range(4):
        expert = lax.broadcasted_iota(jnp.int32, (8, 512), 0) + 2 * to
        shares[to] = jnp.where(ids[0:1] == expert, w0, 0.0) + jnp.where(ids[1:2] == expert, w1, 0.0)
    near_shares[x] = shares[x]
    halves.wait_recv()
    tokens[z, y, x, c] = jnp.transpose(chip[...].astype(jnp.float32)).astype(jnp.bfloat16)
    flows = {}
    spot = {"x": x, "y": y, "z": z}

    def arrived(group):
        for cp in group:
            cp.wait_recv()

    def part(l, s, at=None, half=None):
        first, count, order = ROUTES[l]
        if half is not None:
            first, count = first + half * (count // 2), count // 2
        where = dict(spot, **(at or {}))
        index = tuple(slice(None) if a in order[:s] else where[a] for a in "zyx")
        return tokens.at[index + (c, pl.ds(first, count))]

    def gather(l, s):
        axis = ROUTES[l][2][s]
        flows["g", l, s] = [
            start(push(part(l, s), part(l, s), gs.at[l, s, i], gr.at[l, s, i], {axis: along(axis, h)}))
            for i, h in enumerate(HOPS)
        ]

    for l in range(3):
        gather(l, 0)
    share_swaps = []
    for i, h in enumerate(HOPS):
        peer = along("x", h)
        share_swaps.append(start(push(shares.at[peer], near_shares.at[x], ws.at[i], wr.at[i], {"x": peer})))
    swap(1)
    gain_swap.wait_recv()
    gains[...] = jnp.where((lane < 64) == (c == 0), doubled[...], gains[...])

    def spread_out(l):
        axis = ROUTES[l][2][2]
        flows["n", l] = [
            start(push(part(l, 2), part(l, 2), hops.at[l, i], hopr.at[l, i], {axis: along(axis, h)}))
            for i, h in enumerate((1, 3))
        ]

    def pass_on(l):
        axis = ROUTES[l][2][2]
        flows["p", l] = []
        for i, h in enumerate((1, 3)):
            flows["n", l][i].wait_recv()
            block = part(l, 2, {axis: along(axis, 4 - h)}, i)
            cp = push(block, block, hops.at[l, 2 + i], hopr.at[l, 2 + i], {axis: along(axis, h)})
            flows["p", l].append(start(cp))
            if axis == "x":
                to_core(3 + i, part(l, 2, {axis: along(axis, 4 - h)}))

    def to_core(n, block):
        flows["c", n] = [start(push(block, block, cs.at[n], cr.at[n], other))]

    def pack_one(m, to):
        for t in range(14):
            v = jnp.transpose(raw[m % 2, to, :, 128 * t : 128 * t + 128])
            if m < 2:
                v = v * gains[0:1]
            v = v.astype(jnp.bfloat16)
            at = 128 * t
            while at < 128 * t + 128:
                u, low = divmod(at, 112)
                n = min(112 - low, 128 * t + 128 - at)
                a = at - 128 * t
                sent[m, to, u // 4, (u // 2) % 2, u % 2, low : low + n] = v[a : a + n]
                at += n

    def pack(m):
        loaded(m, 0)

        def one(to, carry):
            pack_one(m, to)
            return carry

        lax.fori_loop(0, 4, one, 0)

    def split(k):
        return k // 4, (k // 2) % 2, k % 2

    def x_send(k, i):
        m, hh, rc = split(k)
        peer = along("x", HOPS[i])
        src = sent.at[m, peer, :, lax.rem(c + rc, 2), hh]
        push(src, over_x.at[k, x], xs, xr.at[k], {"x": peer}).start()

    def x_keep(k):
        m, hh, rc = split(k)
        over_x[k, x] = sent[m, x, :, lax.rem(c + rc, 2), hh]

    def x_steps(m):
        for k in range(4 * m, 4 * m + 4):
            for i in range(3):
                x_send(k, i)
        for k in range(4 * m, 4 * m + 4):
            x_keep(k)

    def z_step(k):
        bulk(over_x.at[k, 0:3], xs, xr.at[k]).wait_recv()
        for h in HOPS:
            peer = along("z", h)
            push(over_x.at[k, peer], over_z.at[k, z], zs, zr.at[k], {"z": peer}).start()
        over_z[k, z] = over_x[k, z]

    def lanes(zz):
        return pl.ds(pl.multiple_of((zz * 4 + y) * 128, 128), 128)

    def y_step(k):
        m, hh, rc = split(k)
        bulk(over_z.at[k, 0:3], zs, zr.at[k]).wait_recv()
        rows = pl.ds(hh * 112, 112)
        for h in STEPS if rc else HOPS:
            py = along("y", h)
            peer = {"y": py, "c": lax.rem(c + rc, 2)}
            for zz in range(4):
                push(over_z.at[k, zz, py], served.at[m, c, rows, lanes(zz)], ys.at[rc], yr.at[k], peer).start()
        if rc == 0:
            for zz in range(4):
                served[m, c, rows, lanes(zz)] = over_z[k, zz, y]

    def y_landed(k):
        rc = k % 2
        bulk(over_z.at[k, 0 : 3 + rc], ys.at[rc], yr.at[k]).wait_recv()

    for i, h in enumerate(STEPS):
        loaded(0, i)
        pack_one(0, along("x", h))
        if i < 3:
            x_send(0, i)
    for k in range(1, 4):
        for i in range(3):
            x_send(k, i)
    for l in range(3):
        arrived(flows["g", l, 0])
        gather(l, 1)
    pl.semaphore_signal(credit, inc=1, device_id=other, device_id_type=MESH)
    fetch(2)
    for k in range(4):
        x_keep(k)
    z_step(0)
    for l in range(2):
        arrived(flows["g", l, 1])
        spread_out(l)
    pl.semaphore_wait(credit, 1)
    swap(2)
    pack(1)
    x_steps(1)
    arrived(flows["g", 2, 1])
    to_core(2, part(2, 2))
    z_step(1)
    pack(2)
    x_steps(2)
    spread_out(2)
    arrived(share_swaps)
    for b in range(4):
        share_cols[pl.ds(512 * b, 512), 0:8] = jnp.transpose(near_shares[b])

    stores = []

    def store(m):
        cp = pltpu.make_async_copy(served.at[m], outs[m], os.at[m])
        cp.start()
        stores.append(cp)

    def act_tile(xb, ch):
        t = xb * 2 + ch
        total = jnp.zeros((256, 128), jnp.float32)
        for q in range(16):
            block = tokens[q // 4, q % 4, xb, ch]
            wide[:, 128 * q : 128 * q + 128] = block
            v = block.astype(jnp.float32)
            total = total + v * v
        inv = lax.rsqrt(jnp.sum(total, axis=1, keepdims=True) / 2048.0 + EPSILON)
        dims = (((1,), (1,)), ((), ()))
        rows = pl.ds(pl.multiple_of(t * 256, 256), 256)
        for e in range(2):
            gate_pre = lax.dot_general(wide[...], served[0, e], dims, preferred_element_type=jnp.float32) * inv
            up_pre = lax.dot_general(wide[...], served[1, e], dims, preferred_element_type=jnp.float32) * inv
            act = gate_pre / (1.0 + jnp.exp(-gate_pre)) * up_pre
            acts[e, rows] = (act * share_cols[rows, e : e + 1]).astype(jnp.bfloat16)

    def act_block(hop):
        def one(ch, carry):
            act_tile(along("x", hop), ch)
            return carry

        lax.fori_loop(0, 2, one, 0)

    for k in range(9):
        if k < 8:
            z_step(k + 2)
        if k == 1:
            pass_on(0)
            pass_on(1)
        if k in (5, 6):
            arrived(flows["p", k - 5])
            to_core(k - 5, part(k - 5, 3))
        y_step(k)
    z_step(10)
    z_step(11)
    y_step(9)
    for k in range(8):
        y_landed(k)
    store(0)
    store(1)
    for n in range(3):
        arrived(flows["c", n])
    act_block(0)
    y_step(10)
    pass_on(2)
    y_step(11)
    arrived(flows["c", 4])
    act_block(1)
    arrived(flows["p", 2])
    to_core(5, part(2, 2, {"x": along("x", 2)}))
    arrived(flows["c", 3])
    act_block(3)
    arrived(flows["c", 5])
    act_block(2)
    for k in range(8, 12):
        y_landed(k)
    store(2)

    def down_part(t, n):
        rows = pl.ds(pl.multiple_of(t * 256, 256), 256)
        cols = slice(512 * n, 512 * n + 512)
        v = jnp.dot(acts[0, rows], served[2, 0, :, cols], preferred_element_type=jnp.float32)
        return v + jnp.dot(acts[1, rows], served[2, 1, :, cols], preferred_element_type=jnp.float32)

    given = []
    for i, h in enumerate(STEPS):
        t = along("x", h) * 2 + 1 - c
        for n in range(4):
            v = down_part(t, n)
            for b in range(4):
                give[i, n, b] = v[:, 128 * b : 128 * b + 128].astype(jnp.bfloat16)
        given.append(start(push(give.at[i], near.at[i], ds.at[i], dr.at[i], other)))
    r0, r1, r2 = (pl.ds(*r) for r in ROWS)
    every = slice(None)
    for i, h in enumerate(STEPS):
        t = along("x", h) * 2 + c
        arrived([given[i]])
        for n in range(4):
            v = down_part(t, n)
            for b in range(4):
                total = v[:, 128 * b : 128 * b + 128] + near[i, n, b].astype(jnp.float32)
                held[n, b, i] = total.astype(jnp.bfloat16)
        if i < 3:
            push(held.at[every, every, i, r0], one0.at[i], fs.at[0], fr.at[0], {"x": along("x", h)}).start()
        for j, g in enumerate(HOPS):
            py, pz = along("y", g), along("z", g)
            push(held.at[every, py, i, r1], one1.at[j, :, i], fs.at[1], fr.at[1], {"y": py}).start()
            push(held.at[pz, every, i, r2], one2.at[j, :, i], fs.at[2], fr.at[2], {"z": pz}).start()

    def summed(base, terms):
        v = base.astype(jnp.float32)
        for term in terms:
            v = v + term.astype(jnp.float32)
        return v

    ones, twos, threes = (one0, one1, one2), (two0, two1, two2), (three0, three1, three2)
    adds, sums = (add0, add1, add2), (sum0, sum1, sum2)
    turns = (("y", "z"), ("z", "x"), ("x", "y"))

    def add_first(l, base):
        bulk(ones[l], fs.at[l], fr.at[l]).wait_recv()

        def body(n, carry):
            a, b = n // 4, lax.rem(n, 4)
            adds[l][a, b] = summed(base(a, b), [ones[l][j, a, b] for j in range(3)]).astype(jnp.bfloat16)
            return carry

        lax.fori_loop(0, 16, body, 0)

    def add_second(l, base):
        bulk(twos[l], ss.at[l], sr.at[l]).wait_recv()
        for a in range(4):
            sums[l][a] = summed(base(a), [twos[l][j, a] for j in range(3)]).astype(jnp.bfloat16)

    def send_on(l, s, pick, dst, send, recv):
        axis = turns[l][s]
        for j, h in enumerate(HOPS):
            peer = along(axis, h)
            push(pick(j, peer), dst.at[j], send.at[l], recv.at[l], {axis: peer}).start()

    bases = (lambda a, b: held[a, b, 3, r0], lambda a, b: held[a, y, b, r1], lambda a, b: held[z, a, b, r2])
    picks = (lambda j, p: add0.at[:, p], lambda j, p: add1.at[p], lambda j, p: add2.at[:, j])
    for l in (1, 2, 0):
        add_first(l, bases[l])
        send_on(l, 0, picks[l], twos[l], ss, sr)
    bases = (lambda a: add0[a, y], lambda a: add1[z, a], lambda a: add2[a, 3])
    picks = (lambda j, p: sum0.at[p], lambda j, p: sum1.at[j], lambda j, p: sum2.at[p])
    for l in (1, 2, 0):
        add_second(l, bases[l])
        send_on(l, 1, picks[l], threes[l], ts, tr)
    bases = (lambda: sum0[z], lambda: sum1[3], lambda: sum2[y])
    for l in (1, 2, 0):
        bulk(threes[l], ts.at[l], tr.at[l]).wait_recv()
        total = summed(bases[l](), [threes[l][j] for j in range(3)])
        last[pl.ds(*ROWS[l])] = total.astype(jnp.bfloat16)
    turned[...] = jnp.transpose(last[...].astype(jnp.float32)).astype(jnp.bfloat16)
    rest = turned.at[pl.ds(pl.multiple_of((1 - c) * 64, 64), 64)]
    final = start(push(rest, out.at[:, half], es, er, other))
    out[:, half] = turned[mine]
    final.wait_recv()
    bulk(raw.at[:, 0:3], ps, pr.at[0]).wait_send()
    bulk(over_x.at[:, 0:3], xs, xr.at[0]).wait_send()
    bulk(over_z.at[:, 0:3], zs, zr.at[0]).wait_send()
    for rc in range(2):
        bulk(over_z.at[0:6, 0 : 3 + rc], ys.at[rc], yr.at[0]).wait_send()
    for l in range(3):
        bulk(ones[l], fs.at[l], fr.at[l]).wait_send()
        bulk(twos[l], ss.at[l], sr.at[l]).wait_send()
        bulk(threes[l], ts.at[l], tr.at[l]).wait_send()
    for cp in sends:
        cp.wait_send()
    for cp in stores:
        cp.wait()


def whole_call(gate, up, down, gain, hidden, ids, logits):
    any_space = pl.BlockSpec(memory_space=pl.ANY)
    vmem = pl.BlockSpec(memory_space=pltpu.VMEM)
    bf16, f32 = jnp.bfloat16, jnp.float32
    dma = pltpu.SemaphoreType.DMA
    sizes = [n for _, n in ROWS]
    served = jax.ShapeDtypeStruct((2, 224, 2048), bf16)

    def buffers(*shapes):
        return [pltpu.VMEM(s, bf16) for s in shapes]

    return pl.pallas_call(
        whole,
        out_shape=(served, served, served, jax.ShapeDtypeStruct((64, 512), bf16)),
        in_specs=[any_space] * 3 + [vmem] * 4,
        out_specs=(any_space,) * 3 + (vmem,),
        scratch_shapes=[pltpu.VMEM((2, 4, 128, 1792), f32)] + [pltpu.VMEM((8, 128), f32)] * 2
        + buffers((3, 4, 4, 2, 2, 112, 128), (CHUNKS, 4, 4, 112, 128), (CHUNKS, 4, 4, 112, 128),
                  (3, 2, 224, 2048), (4, 4, 4, 2, 256, 128), (128, 256))
        + [pltpu.VMEM((4, 8, 512), f32)] * 2
        + [pltpu.VMEM((2048, 128), f32)]
        + buffers((256, 2048), (2, 2048, 224), (4, 4, 4, 256, 128), (4, 4, 4, 256, 128), (4, 4, 4, 256, 128))
        + buffers(*[(3, 4, 4, n, 128) for n in sizes])
        + buffers(*[(4, 4, n, 128) for n in sizes])
        + buffers(*[(3, 4, n, 128) for n in sizes])
        + buffers(*[(4, n, 128) for n in sizes])
        + buffers(*[(3, n, 128) for n in sizes])
        + buffers((256, 128), (128, 256))
        + [dma((6,)), dma, dma((6,)), pltpu.SemaphoreType.REGULAR]
        + [dma, dma((CHUNKS,)), dma, dma((CHUNKS,)), dma((2,)), dma((CHUNKS,))]
        + [dma] * 4
        + [dma((3,))] * 2
        + [dma((3, 2, 3))] * 2
        + [dma((3, 4))] * 2
        + [dma((6,))] * 2
        + [dma((3,))]
        + [dma((4,))] * 2
        + [dma((3,))] * 6
        + [dma] * 2,
        compiler_params=pltpu.CompilerParams(
            collective_id=0, has_side_effects=True, vmem_limit_bytes=67043328
        ),
        name="whole",
    )(gate, up, down, gain, hidden, ids, logits)


def deliver(*refs):
    sources, results, held, in_sem, out_sem = refs[:4], refs[4:8], refs[8:12], refs[12], refs[13]

    def view(ref, n, k):
        return ref.at[k // 2, pl.ds(112 * (k % 2), 112)] if n < 3 else ref

    steps = [(n, k) for n in range(4) for k in range(4 if n < 3 else 1)]
    loads = [
        pltpu.make_async_copy(view(sources[n], n, k), view(held[n], n, k), in_sem.at[4 * n + k]) for n, k in steps
    ]
    stores = [
        pltpu.make_async_copy(view(held[n], n, k), view(results[n], n, k), out_sem.at[4 * n + k]) for n, k in steps
    ]
    for cp in loads:
        cp.start()
    for load, store in zip(loads, stores):
        load.wait()
        store.start()
    for cp in stores:
        cp.wait()


def deliver_call(*results):
    any_space = pl.BlockSpec(memory_space=pl.ANY)
    return pl.pallas_call(
        deliver,
        out_shape=tuple(jax.ShapeDtypeStruct(r.shape, r.dtype) for r in results),
        in_specs=[any_space] * 4,
        out_specs=(any_space,) * 4,
        scratch_shapes=[pltpu.VMEM(r.shape, r.dtype) for r in results]
        + [pltpu.SemaphoreType.DMA((13,))] * 2,
        name="deliver",
    )(*results)


def per_device(hidden, norm_gain, gate_master, up_master, down_master, expert_ids, route_logits):
    gain = norm_gain.reshape(1, 64)
    masters = [m.reshape(4, 2, 64, 1792) for m in (gate_master, up_master, down_master)]
    results = whole_call(
        *masters, gain, jnp.transpose(hidden), jnp.transpose(expert_ids), jnp.transpose(route_logits)
    )
    gate, up, down, out = deliver_call(*results)
    return jnp.swapaxes(gate, 1, 2), jnp.swapaxes(up, 1, 2), jnp.swapaxes(down, 1, 2), jnp.transpose(out)


def solution(mesh):
    split = Mesh(mesh.devices.reshape(4, 4, 2, mesh.shape["tp"]), ("z", "y", "c", "x"))
    weight = P(None, FS, "x")
    in_specs = (P("x", FS), P(FS), weight, weight, weight, P("x", None), P("x", None))
    served = P("x", None, FS)
    return jax.shard_map(
        per_device,
        mesh=split,
        in_specs=in_specs,
        out_specs=(served, served, served, P("x", FS)),
        check_vma=False,
    )
```

```python
import functools

import jax
import jax.numpy as jnp
from jax import lax
from jax.experimental import pallas as pl
from jax.experimental.pallas import tpu as pltpu
from jax.sharding import Mesh
from jax.sharding import PartitionSpec as P

MESH = pl.DeviceIdType.MESH
EPSILON = 1e-06
FS = ("z", "y", "c")
HOPS = (1, 3, 2)
STEPS = HOPS + (0,)
FARTHEST_FIRST = (2, 0, 1, 3)
ROWS = ((0, 96), (96, 80), (176, 80))
ROUTES = ((0, 64, "xyz"), (64, 96, "xzy"), (160, 96, "zyx"))
CHUNKS = 12


def along(axis, hop):
    return lax.rem(lax.axis_index(axis) + hop, 4)


def greet():
    barrier = pltpu.get_barrier_semaphore()
    c = lax.axis_index("c")
    peers = [{a: along(a, h)} for a in ("x", "z") for h in HOPS]
    peers += [{"y": along("y", h), "c": lax.rem(c + r, 2)} for r in (0, 1) for h in (STEPS if r else HOPS)]
    for peer in peers:
        pl.semaphore_signal(barrier, inc=1, device_id=peer, device_id_type=MESH)
    pl.semaphore_wait(barrier, len(peers))


def push(src, dst, send, recv, peer):
    return pltpu.make_async_remote_copy(
        src_ref=src, dst_ref=dst, send_sem=send, recv_sem=recv, device_id=peer, device_id_type=MESH
    )


def whole(gate, up, down, gain, hidden, ids, logits,
          gate_out, up_out, down_out, out,
          raw, doubled, gains, sent, over_x, over_z, served, tokens, chip, shares, near_shares, share_cols,
          wide, acts, give, near, held, one0, one1, one2, carry0, carry1, carry2, add0, add1, add2,
          two0, two1, two2, sum0, sum1, sum2, three0, three1, three2, last, turned,
          ls, ps, pr, credit, xs, xr, zs, zr, ys, yr, hs, hr, ns, nr, ws, wr,
          gs, gr, hops, hopr, cs, cr, os, ds, dr, ks, kr0, kr, fs, fr, ss, sr, ts, tr, es, er):
    masters = (gate, up, down)
    outs = (gate_out, up_out, down_out)
    x, y, z, c = (lax.axis_index(a) for a in ("x", "y", "z", "c"))
    other = {"c": 1 - c}
    sends = []

    def start(cp):
        cp.start()
        sends.append(cp)
        return cp

    def bulk(ref, send, recv):
        return push(ref, ref, send, recv, other)

    mine = pl.ds(pl.multiple_of(c * 64, 64), 64)
    def slot(m, i):
        return i if m == 0 else 3 + m

    def fetch(m):
        for i, h in enumerate(STEPS):
            to = along("x", h)
            pltpu.make_async_copy(masters[m].at[to, c], raw.at[m % 2, to, mine], ls.at[slot(m, i)]).start()

    def swap(m):
        for i, h in enumerate(STEPS):
            to = along("x", h)
            push(masters[m].at[to, 1 - c], raw.at[m % 2, to, mine], ps, pr.at[slot(m, i)], other).start()

    def loaded(m, i):
        block = raw.at[0, 0, mine] if m == 0 else raw.at[0, :, mine]
        pltpu.make_async_copy(block, block, ls.at[slot(m, i)]).wait()
        bulk(block, ps, pr.at[slot(m, i)]).wait_recv()

    fetch(0)
    fetch(1)
    half = pl.ds(pl.multiple_of(c * 256, 256), 256)
    far_half = pl.ds(pl.multiple_of((1 - c) * 256, 256), 256)
    chip[mine] = hidden[:, half]
    lane = lax.broadcasted_iota(jnp.int32, (8, 128), 1)
    row = jnp.broadcast_to(gain[...], (8, 64))
    doubled[...] = jnp.concatenate([row, row], axis=1)
    greet()
    halves = start(push(hidden.at[:, far_half], chip.at[mine], hs, hr, other))
    gain_swap = start(push(doubled, gains, ns, nr, other))
    swap(0)

    l0, l1 = logits[0:1], logits[1:2]
    top = jnp.maximum(l0, l1)
    e0, e1 = jnp.exp(l0 - top), jnp.exp(l1 - top)
    w0, w1 = e0 / (e0 + e1), e1 / (e0 + e1)
    for to in range(4):
        expert = lax.broadcasted_iota(jnp.int32, (8, 512), 0) + 2 * to
        shares[to] = jnp.where(ids[0:1] == expert, w0, 0.0) + jnp.where(ids[1:2] == expert, w1, 0.0)
    near_shares[x] = shares[x]
    halves.wait_recv()
    tokens[z, y, x, c] = jnp.transpose(chip[...].astype(jnp.float32)).astype(jnp.bfloat16)
    flows = {}
    spot = {"x": x, "y": y, "z": z}

    def arrived(group):
        for cp in group:
            cp.wait_recv()

    def part(l, s, at=None, half=None):
        first, count, order = ROUTES[l]
        if half is not None:
            first, count = first + half * (count // 2), count // 2
        where = dict(spot, **(at or {}))
        index = tuple(slice(None) if a in order[:s] else where[a] for a in "zyx")
        return tokens.at[index + (c, pl.ds(first, count))]

    def gather(l, s):
        axis = ROUTES[l][2][s]
        flows["g", l, s] = [
            start(push(part(l, s), part(l, s), gs.at[l, s, i], gr.at[l, s, i], {axis: along(axis, h)}))
            for i, h in enumerate(HOPS)
        ]

    for l in range(3):
        gather(l, 0)
    share_swaps = []
    for i, h in enumerate(HOPS):
        peer = along("x", h)
        share_swaps.append(start(push(shares.at[peer], near_shares.at[x], ws.at[i], wr.at[i], {"x": peer})))
    swap(1)
    gain_swap.wait_recv()
    gains[...] = jnp.where((lane < 64) == (c == 0), doubled[...], gains[...])

    def spread_out(l):
        axis = ROUTES[l][2][2]
        flows["n", l] = [
            start(push(part(l, 2), part(l, 2), hops.at[l, i], hopr.at[l, i], {axis: along(axis, h)}))
            for i, h in enumerate((1, 3))
        ]

    def pass_on(l):
        axis = ROUTES[l][2][2]
        flows["p", l] = []
        for i, h in enumerate((1, 3)):
            flows["n", l][i].wait_recv()
            block = part(l, 2, {axis: along(axis, 4 - h)}, i)
            cp = push(block, block, hops.at[l, 2 + i], hopr.at[l, 2 + i], {axis: along(axis, h)})
            flows["p", l].append(start(cp))
            if axis == "x":
                to_core(3 + i, part(l, 2, {axis: along(axis, 4 - h)}))

    def to_core(n, block):
        flows["c", n] = [start(push(block, block, cs.at[n], cr.at[n], other))]

    def pack_one(m, to):
        for t in range(14):
            v = jnp.transpose(raw[m % 2, to, :, 128 * t : 128 * t + 128])
            if m < 2:
                v = v * gains[0:1]
            v = v.astype(jnp.bfloat16)
            at = 128 * t
            while at < 128 * t + 128:
                u, low = divmod(at, 112)
                n = min(112 - low, 128 * t + 128 - at)
                a = at - 128 * t
                sent[m, to, u // 4, (u // 2) % 2, u % 2, low : low + n] = v[a : a + n]
                at += n

    def pack(m):
        loaded(m, 0)

        def one(to, carry):
            pack_one(m, to)
            return carry

        lax.fori_loop(0, 4, one, 0)

    def split(k):
        return k // 4, (k // 2) % 2, k % 2

    def x_send(k, i):
        m, hh, rc = split(k)
        peer = along("x", HOPS[i])
        src = sent.at[m, peer, :, lax.rem(c + rc, 2), hh]
        push(src, over_x.at[k, x], xs, xr.at[k], {"x": peer}).start()

    def x_keep(k):
        m, hh, rc = split(k)
        over_x[k, x] = sent[m, x, :, lax.rem(c + rc, 2), hh]

    def x_steps(m):
        for k in range(4 * m, 4 * m + 4):
            for i in range(3):
                x_send(k, i)
        for k in range(4 * m, 4 * m + 4):
            x_keep(k)

    def z_step(k):
        bulk(over_x.at[k, 0:3], xs, xr.at[k]).wait_recv()
        for h in HOPS:
            peer = along("z", h)
            push(over_x.at[k, peer], over_z.at[k, z], zs, zr.at[k], {"z": peer}).start()
        over_z[k, z] = over_x[k, z]

    def lanes(zz):
        return pl.ds(pl.multiple_of((zz * 4 + y) * 128, 128), 128)

    def y_step(k):
        m, hh, rc = split(k)
        bulk(over_z.at[k, 0:3], zs, zr.at[k]).wait_recv()
        rows = pl.ds(hh * 112, 112)
        for h in STEPS if rc else HOPS:
            py = along("y", h)
            peer = {"y": py, "c": lax.rem(c + rc, 2)}
            for zz in range(4):
                push(over_z.at[k, zz, py], served.at[m, c, rows, lanes(zz)], ys.at[rc], yr.at[k], peer).start()
        if rc == 0:
            for zz in range(4):
                served[m, c, rows, lanes(zz)] = over_z[k, zz, y]

    def y_landed(k):
        rc = k % 2
        bulk(over_z.at[k, 0 : 3 + rc], ys.at[rc], yr.at[k]).wait_recv()

    for i, h in enumerate(STEPS):
        loaded(0, i)
        pack_one(0, along("x", h))
        if i < 3:
            x_send(0, i)
    for k in range(1, 4):
        for i in range(3):
            x_send(k, i)
    for l in range(3):
        arrived(flows["g", l, 0])
        gather(l, 1)
    pl.semaphore_signal(credit, inc=1, device_id=other, device_id_type=MESH)
    fetch(2)
    for k in range(4):
        x_keep(k)
    z_step(0)
    for l in range(2):
        arrived(flows["g", l, 1])
        spread_out(l)
    pl.semaphore_wait(credit, 1)
    swap(2)
    pack(1)
    x_steps(1)
    arrived(flows["g", 2, 1])
    to_core(2, part(2, 2))
    z_step(1)
    pack(2)
    x_steps(2)
    spread_out(2)
    arrived(share_swaps)
    for b in range(4):
        share_cols[pl.ds(512 * b, 512), 0:8] = jnp.transpose(near_shares[b])

    stores = []

    def store(m):
        cp = pltpu.make_async_copy(served.at[m], outs[m], os.at[m])
        cp.start()
        stores.append(cp)

    def act_tile(xb, ch):
        t = xb * 2 + ch
        total = jnp.zeros((256, 128), jnp.float32)
        for q in range(16):
            block = tokens[q // 4, q % 4, xb, ch]
            wide[:, 128 * q : 128 * q + 128] = block
            v = block.astype(jnp.float32)
            total = total + v * v
        inv = lax.rsqrt(jnp.sum(total, axis=1, keepdims=True) / 2048.0 + EPSILON)
        dims = (((1,), (1,)), ((), ()))
        rows = pl.ds(pl.multiple_of(t * 256, 256), 256)
        for e in range(2):
            gate_pre = lax.dot_general(wide[...], served[0, e], dims, preferred_element_type=jnp.float32) * inv
            up_pre = lax.dot_general(wide[...], served[1, e], dims, preferred_element_type=jnp.float32) * inv
            act = gate_pre / (1.0 + jnp.exp(-gate_pre)) * up_pre
            acts[e, rows] = (act * share_cols[rows, e : e + 1]).astype(jnp.bfloat16)

    def act_block(hop):
        def one(ch, carry):
            act_tile(along("x", hop), ch)
            return carry

        lax.fori_loop(0, 2, one, 0)

    for k in range(9):
        if k < 8:
            z_step(k + 2)
        if k == 1:
            pass_on(0)
            pass_on(1)
        if k in (5, 6):
            arrived(flows["p", k - 5])
            to_core(k - 5, part(k - 5, 3))
        y_step(k)
    z_step(10)
    z_step(11)
    y_step(9)
    for k in range(8):
        y_landed(k)
    store(0)
    store(1)
    for n in range(3):
        arrived(flows["c", n])
    act_block(0)
    y_step(10)
    pass_on(2)
    arrived(flows["c", 4])
    act_block(1)
    y_step(11)
    arrived(flows["p", 2])
    to_core(5, part(2, 2, {"x": along("x", 2)}))
    arrived(flows["c", 3])
    act_block(3)
    arrived(flows["c", 5])
    act_block(2)
    for k in range(8, 12):
        y_landed(k)
    store(2)

    def down_part(t, n):
        rows = pl.ds(pl.multiple_of(t * 256, 256), 256)
        cols = slice(512 * n, 512 * n + 512)
        v = jnp.dot(acts[0, rows], served[2, 0, :, cols], preferred_element_type=jnp.float32)
        return v + jnp.dot(acts[1, rows], served[2, 1, :, cols], preferred_element_type=jnp.float32)

    given = {}
    for i in FARTHEST_FIRST:
        t = along("x", STEPS[i]) * 2 + 1 - c
        for n in range(4):
            v = down_part(t, n)
            for b in range(4):
                give[i, n, b] = v[:, 128 * b : 128 * b + 128].astype(jnp.bfloat16)
        given[i] = [start(push(give.at[i], near.at[i], ds.at[i], dr.at[i], other))]
    r0, r1, r2 = (pl.ds(*r) for r in ROWS)
    every = slice(None)
    quarter = ROWS[0][1] // 2
    low, high = pl.ds(0, quarter), pl.ds(quarter, quarter)

    def y_block(zz, hop, i):
        return held.at[zz, along("y", hop), i, r1]

    def z_block(yy, hop, i):
        return held.at[along("z", hop), yy, i, r2]

    routes = ((1, "y", y_block, one1, carry1), (2, "z", z_block, one2, carry2))
    pairs = (slice(0, 2), slice(2, 4))

    def send_first(i):
        if i == 2:
            for d, h in enumerate((1, 3)):
                block = held.at[every, every, 2, (low, high)[d]]
                push(block, carry0.at[d], ks.at[0], kr0.at[d], {"x": along("x", h)}).start()
        if i < 2:
            h, rows = STEPS[i], (high, low)[i]
            push(held.at[every, every, i, rows], one0.at[i, every, every, rows], fs.at[0], fr.at[0],
                 {"x": along("x", h)}).start()
        for l, axis, block, one, carry in routes:
            for d, h in enumerate((1, 3)):
                peer = {axis: along(axis, h)}
                push(block(pairs[d], 2, i), carry.at[d, i], ks.at[l], kr.at[l - 1, d, i], peer).start()
            for d, h in enumerate((1, 3)):
                peer = {axis: along(axis, h)}
                rest = pairs[1 - d]
                push(block(rest, h, i), one.at[d, rest, i], fs.at[l], fr.at[l], peer).start()

    def send_carried(i):
        if i == 2:
            for d, h in enumerate((1, 3)):
                bulk(carry0.at[d], ks.at[0], kr0.at[d]).wait_recv()
                rows = (low, high)[d]

                def body(n, carry):
                    a, b = n // 4, lax.rem(n, 4)
                    v = held[a, b, d, rows].astype(jnp.float32) + carry0[d, a, b].astype(jnp.float32)
                    held[a, b, d, rows] = v.astype(jnp.bfloat16)
                    return carry

                lax.fori_loop(0, 16, body, 0)
                push(held.at[every, every, d, rows], one0.at[d, every, every, rows], fs.at[0], fr.at[0],
                     {"x": along("x", h)}).start()
        for l, axis, block, one, carry in routes:
            for d, h in enumerate((1, 3)):
                bulk(carry.at[d, i], ks.at[l], kr.at[l - 1, d, i]).wait_recv()
                ref = block(pairs[d], h, i)
                ref[...] = (ref[...].astype(jnp.float32) + carry[d, i].astype(jnp.float32)).astype(jnp.bfloat16)
                push(block(pairs[d], h, i), one.at[d, pairs[d], i], fs.at[l], fr.at[l],
                     {axis: along(axis, h)}).start()

    for i in FARTHEST_FIRST:
        t = along("x", STEPS[i]) * 2 + c
        arrived(given[i])
        for n in range(4):
            v = down_part(t, n)
            for b in range(4):
                total = v[:, 128 * b : 128 * b + 128] + near[i, n, b].astype(jnp.float32)
                held[n, b, i] = total.astype(jnp.bfloat16)
        send_first(i)
    for i in FARTHEST_FIRST:
        send_carried(i)

    def summed(base, terms):
        v = base.astype(jnp.float32)
        for term in terms:
            v = v + term.astype(jnp.float32)
        return v

    ones, twos, threes = (one0, one1, one2), (two0, two1, two2), (three0, three1, three2)
    adds, sums = (add0, add1, add2), (sum0, sum1, sum2)
    turns = (("y", "z"), ("z", "x"), ("x", "y"))

    def add_first(l, base):
        bulk(ones[l], fs.at[l], fr.at[l]).wait_recv()

        def body(n, carry):
            a, b = n // 4, lax.rem(n, 4)
            adds[l][a, b] = summed(base(a, b), [ones[l][j, a, b] for j in range(2)]).astype(jnp.bfloat16)
            return carry

        lax.fori_loop(0, 16, body, 0)

    def add_second(l, base):
        bulk(twos[l], ss.at[l], sr.at[l]).wait_recv()
        for a in range(4):
            sums[l][a] = summed(base(a), [twos[l][j, a] for j in range(3)]).astype(jnp.bfloat16)

    def send_on(l, s, pick, dst, send, recv):
        axis = turns[l][s]
        for j, h in enumerate(HOPS):
            peer = along(axis, h)
            push(pick(j, peer), dst.at[j], send.at[l], recv.at[l], {axis: peer}).start()

    bases = (lambda a, b: held[a, b, 3, r0], lambda a, b: held[a, y, b, r1], lambda a, b: held[z, a, b, r2])
    picks = (lambda j, p: add0.at[:, p], lambda j, p: add1.at[p], lambda j, p: add2.at[:, j])
    for l in (1, 2, 0):
        add_first(l, bases[l])
        send_on(l, 0, picks[l], twos[l], ss, sr)
    bases = (lambda a: add0[a, y], lambda a: add1[z, a], lambda a: add2[a, 3])
    picks = (lambda j, p: sum0.at[p], lambda j, p: sum1.at[j], lambda j, p: sum2.at[p])
    for l in (1, 2, 0):
        add_second(l, bases[l])
        send_on(l, 1, picks[l], threes[l], ts, tr)
    bases = (lambda: sum0[z], lambda: sum1[3], lambda: sum2[y])
    for l in (1, 2, 0):
        bulk(threes[l], ts.at[l], tr.at[l]).wait_recv()
        total = summed(bases[l](), [threes[l][j] for j in range(3)])
        last[pl.ds(*ROWS[l])] = total.astype(jnp.bfloat16)
    turned[...] = jnp.transpose(last[...].astype(jnp.float32)).astype(jnp.bfloat16)
    rest = turned.at[pl.ds(pl.multiple_of((1 - c) * 64, 64), 64)]
    final = start(push(rest, out.at[:, half], es, er, other))
    out[:, half] = turned[mine]
    final.wait_recv()
    bulk(raw.at[:, 0:3], ps, pr.at[0]).wait_send()
    bulk(over_x.at[:, 0:3], xs, xr.at[0]).wait_send()
    bulk(over_z.at[:, 0:3], zs, zr.at[0]).wait_send()
    for rc in range(2):
        bulk(over_z.at[0:6, 0 : 3 + rc], ys.at[rc], yr.at[0]).wait_send()
    for l, carry in enumerate((carry0, carry1, carry2)):
        bulk(carry, ks.at[l], fr.at[l]).wait_send()
    for l in range(3):
        bulk(ones[l], fs.at[l], fr.at[l]).wait_send()
        bulk(twos[l], ss.at[l], sr.at[l]).wait_send()
        bulk(threes[l], ts.at[l], tr.at[l]).wait_send()
    for cp in sends:
        cp.wait_send()
    for cp in stores:
        cp.wait()


def whole_call(gate, up, down, gain, hidden, ids, logits):
    any_space = pl.BlockSpec(memory_space=pl.ANY)
    vmem = pl.BlockSpec(memory_space=pltpu.VMEM)
    bf16, f32 = jnp.bfloat16, jnp.float32
    dma = pltpu.SemaphoreType.DMA
    sizes = [n for _, n in ROWS]
    served = jax.ShapeDtypeStruct((2, 224, 2048), bf16)

    def buffers(*shapes):
        return [pltpu.VMEM(s, bf16) for s in shapes]

    return pl.pallas_call(
        whole,
        out_shape=(served, served, served, jax.ShapeDtypeStruct((64, 512), bf16)),
        in_specs=[any_space] * 3 + [vmem] * 4,
        out_specs=(any_space,) * 3 + (vmem,),
        scratch_shapes=[pltpu.VMEM((2, 4, 128, 1792), f32)] + [pltpu.VMEM((8, 128), f32)] * 2
        + buffers((3, 4, 4, 2, 2, 112, 128), (CHUNKS, 4, 4, 112, 128), (CHUNKS, 4, 4, 112, 128),
                  (3, 2, 224, 2048), (4, 4, 4, 2, 256, 128), (128, 256))
        + [pltpu.VMEM((4, 8, 512), f32)] * 2
        + [pltpu.VMEM((2048, 128), f32)]
        + buffers((256, 2048), (2, 2048, 224), (4, 4, 4, 256, 128), (4, 4, 4, 256, 128), (4, 4, 4, 256, 128))
        + buffers(*[(2, 4, 4, n, 128) for n in sizes])
        + buffers((2, 4, 4, sizes[0] // 2, 128), (2, 4, 2, sizes[1], 128), (2, 4, 2, sizes[2], 128))
        + buffers(*[(4, 4, n, 128) for n in sizes])
        + buffers(*[(3, 4, n, 128) for n in sizes])
        + buffers(*[(4, n, 128) for n in sizes])
        + buffers(*[(3, n, 128) for n in sizes])
        + buffers((256, 128), (128, 256))
        + [dma((6,)), dma, dma((6,)), pltpu.SemaphoreType.REGULAR]
        + [dma, dma((CHUNKS,)), dma, dma((CHUNKS,)), dma((2,)), dma((CHUNKS,))]
        + [dma] * 4
        + [dma((3,))] * 2
        + [dma((3, 2, 3))] * 2
        + [dma((3, 4))] * 2
        + [dma((6,))] * 2
        + [dma((3,))]
        + [dma((4,))] * 2
        + [dma((3,)), dma((2,)), dma((2, 2, 4))]
        + [dma((3,))] * 6
        + [dma] * 2,
        compiler_params=pltpu.CompilerParams(
            collective_id=0, has_side_effects=True, vmem_limit_bytes=67043328
        ),
        name="whole",
    )(gate, up, down, gain, hidden, ids, logits)


def deliver(*refs):
    sources, results, held, in_sem, out_sem = refs[:4], refs[4:8], refs[8:12], refs[12], refs[13]

    def view(ref, n, k):
        return ref.at[k // 2, pl.ds(112 * (k % 2), 112)] if n < 3 else ref

    steps = [(n, k) for n in range(4) for k in range(4 if n < 3 else 1)]
    loads = [
        pltpu.make_async_copy(view(sources[n], n, k), view(held[n], n, k), in_sem.at[4 * n + k]) for n, k in steps
    ]
    stores = [
        pltpu.make_async_copy(view(held[n], n, k), view(results[n], n, k), out_sem.at[4 * n + k]) for n, k in steps
    ]
    for cp in loads:
        cp.start()
    for load, store in zip(loads, stores):
        load.wait()
        store.start()
    for cp in stores:
        cp.wait()


def deliver_call(*results):
    any_space = pl.BlockSpec(memory_space=pl.ANY)
    return pl.pallas_call(
        deliver,
        out_shape=tuple(jax.ShapeDtypeStruct(r.shape, r.dtype) for r in results),
        in_specs=[any_space] * 4,
        out_specs=(any_space,) * 4,
        scratch_shapes=[pltpu.VMEM(r.shape, r.dtype) for r in results]
        + [pltpu.SemaphoreType.DMA((13,))] * 2,
        name="deliver",
    )(*results)


def per_device(hidden, norm_gain, gate_master, up_master, down_master, expert_ids, route_logits):
    gain = norm_gain.reshape(1, 64)
    masters = [m.reshape(4, 2, 64, 1792) for m in (gate_master, up_master, down_master)]
    results = whole_call(
        *masters, gain, jnp.transpose(hidden), jnp.transpose(expert_ids), jnp.transpose(route_logits)
    )
    gate, up, down, out = deliver_call(*results)
    return jnp.swapaxes(gate, 1, 2), jnp.swapaxes(up, 1, 2), jnp.swapaxes(down, 1, 2), jnp.transpose(out)


def solution(mesh):
    split = Mesh(mesh.devices.reshape(4, 4, 2, mesh.shape["tp"]), ("z", "y", "c", "x"))
    weight = P(None, FS, "x")
    in_specs = (P("x", FS), P(FS), weight, weight, weight, P("x", None), P("x", None))
    served = P("x", None, FS)
    return jax.shard_map(
        per_device,
        mesh=split,
        in_specs=in_specs,
        out_specs=(served, served, served, P("x", FS)),
        check_vma=False,
    )
```

```python
import functools

import jax
import jax.numpy as jnp
from jax import lax
from jax.experimental import pallas as pl
from jax.experimental.pallas import tpu as pltpu
from jax.sharding import Mesh
from jax.sharding import PartitionSpec as P

MESH = pl.DeviceIdType.MESH
EPSILON = 1e-06
FS = ("z", "y", "c")
HOPS = (1, 3, 2)
STEPS = HOPS + (0,)
FARTHEST_FIRST = (2, 0, 1, 3)
ROWS = ((0, 96), (96, 80), (176, 80))
ROUTES = ((0, 64, "xyz"), (64, 96, "xzy"), (160, 96, "zyx"))
CHUNKS = 12
PARTS = tuple((k, 0, 112) for k in range(4)) + tuple((k, r, n) for k in range(4, CHUNKS) for r, n in ((0, 64), (64, 48)))


def along(axis, hop):
    return lax.rem(lax.axis_index(axis) + hop, 4)


def greet():
    barrier = pltpu.get_barrier_semaphore()
    c = lax.axis_index("c")
    peers = [{a: along(a, h)} for a in ("x", "z") for h in HOPS]
    peers += [{"y": along("y", h), "c": lax.rem(c + r, 2)} for r in (0, 1) for h in (STEPS if r else HOPS)]
    for peer in peers:
        pl.semaphore_signal(barrier, inc=1, device_id=peer, device_id_type=MESH)
    pl.semaphore_wait(barrier, len(peers))


def push(src, dst, send, recv, peer):
    return pltpu.make_async_remote_copy(
        src_ref=src, dst_ref=dst, send_sem=send, recv_sem=recv, device_id=peer, device_id_type=MESH
    )


def whole(gate, up, down, gain, hidden, ids, logits,
          gate_out, up_out, down_out, out,
          raw, doubled, gains, sent, over_x, over_z, served, tokens, chip, shares, near_shares, share_cols,
          wide, acts, give, near, held, one0, one1, one2, carry0, carry1, carry2, add0, add1, add2,
          two0, two1, two2, sum0, sum1, sum2, three0, three1, three2, last, turned,
          ls, ps, pr, credit, xs, xr, zs, zr, ys, yr, hs, hr, ns, nr, ws, wr,
          gs, gr, hops, hopr, cs, cr, os, ds, dr, ks, kr0, kr, fs, fr, ss, sr, ts, tr, es, er):
    masters = (gate, up, down)
    outs = (gate_out, up_out, down_out)
    x, y, z, c = (lax.axis_index(a) for a in ("x", "y", "z", "c"))
    other = {"c": 1 - c}
    sends = []

    def start(cp):
        cp.start()
        sends.append(cp)
        return cp

    def bulk(ref, send, recv):
        return push(ref, ref, send, recv, other)

    mine = pl.ds(pl.multiple_of(c * 64, 64), 64)
    def slot(m, i):
        return i if m == 0 else 3 + m

    def fetch(m):
        for i, h in enumerate(STEPS):
            to = along("x", h)
            pltpu.make_async_copy(masters[m].at[to, c], raw.at[m % 2, to, mine], ls.at[slot(m, i)]).start()

    def swap(m):
        for i, h in enumerate(STEPS):
            to = along("x", h)
            push(masters[m].at[to, 1 - c], raw.at[m % 2, to, mine], ps, pr.at[slot(m, i)], other).start()

    def loaded(m, i):
        block = raw.at[0, 0, mine] if m == 0 else raw.at[0, :, mine]
        pltpu.make_async_copy(block, block, ls.at[slot(m, i)]).wait()
        bulk(block, ps, pr.at[slot(m, i)]).wait_recv()

    fetch(0)
    fetch(1)
    half = pl.ds(pl.multiple_of(c * 256, 256), 256)
    far_half = pl.ds(pl.multiple_of((1 - c) * 256, 256), 256)
    chip[mine] = hidden[:, half]
    lane = lax.broadcasted_iota(jnp.int32, (8, 128), 1)
    row = jnp.broadcast_to(gain[...], (8, 64))
    doubled[...] = jnp.concatenate([row, row], axis=1)
    greet()
    halves = start(push(hidden.at[:, far_half], chip.at[mine], hs, hr, other))
    gain_swap = start(push(doubled, gains, ns, nr, other))
    swap(0)

    l0, l1 = logits[0:1], logits[1:2]
    top = jnp.maximum(l0, l1)
    e0, e1 = jnp.exp(l0 - top), jnp.exp(l1 - top)
    w0, w1 = e0 / (e0 + e1), e1 / (e0 + e1)
    for to in range(4):
        expert = lax.broadcasted_iota(jnp.int32, (8, 512), 0) + 2 * to
        shares[to] = jnp.where(ids[0:1] == expert, w0, 0.0) + jnp.where(ids[1:2] == expert, w1, 0.0)
    near_shares[x] = shares[x]
    halves.wait_recv()
    tokens[z, y, x, c] = jnp.transpose(chip[...].astype(jnp.float32)).astype(jnp.bfloat16)
    flows = {}
    spot = {"x": x, "y": y, "z": z}

    def arrived(group):
        for cp in group:
            cp.wait_recv()

    def part(l, s, at=None, half=None):
        first, count, order = ROUTES[l]
        if half is not None:
            first, count = first + half * (count // 2), count // 2
        where = dict(spot, **(at or {}))
        index = tuple(slice(None) if a in order[:s] else where[a] for a in "zyx")
        return tokens.at[index + (c, pl.ds(first, count))]

    def gather(l, s):
        axis = ROUTES[l][2][s]
        flows["g", l, s] = [
            start(push(part(l, s), part(l, s), gs.at[l, s, i], gr.at[l, s, i], {axis: along(axis, h)}))
            for i, h in enumerate(HOPS)
        ]

    for l in range(3):
        gather(l, 0)
    share_swaps = []
    for i, h in enumerate(HOPS):
        peer = along("x", h)
        share_swaps.append(start(push(shares.at[peer], near_shares.at[x], ws.at[i], wr.at[i], {"x": peer})))
    swap(1)
    gain_swap.wait_recv()
    gains[...] = jnp.where((lane < 64) == (c == 0), doubled[...], gains[...])

    def spread_out(l):
        axis = ROUTES[l][2][2]
        flows["n", l] = [
            start(push(part(l, 2), part(l, 2), hops.at[l, i], hopr.at[l, i], {axis: along(axis, h)}))
            for i, h in enumerate((1, 3))
        ]

    def pass_on(l):
        axis = ROUTES[l][2][2]
        flows["p", l] = []
        for i, h in enumerate((1, 3)):
            flows["n", l][i].wait_recv()
            block = part(l, 2, {axis: along(axis, 4 - h)}, i)
            cp = push(block, block, hops.at[l, 2 + i], hopr.at[l, 2 + i], {axis: along(axis, h)})
            flows["p", l].append(start(cp))
            if axis == "x":
                to_core(3 + i, part(l, 2, {axis: along(axis, 4 - h)}))

    def to_core(n, block):
        flows["c", n] = [start(push(block, block, cs.at[n], cr.at[n], other))]

    def pack_one(m, to):
        for t in range(14):
            v = jnp.transpose(raw[m % 2, to, :, 128 * t : 128 * t + 128])
            if m < 2:
                v = v * gains[0:1]
            v = v.astype(jnp.bfloat16)
            at = 128 * t
            while at < 128 * t + 128:
                u, low = divmod(at, 112)
                n = min(112 - low, 128 * t + 128 - at)
                a = at - 128 * t
                sent[m, to, u // 4, (u // 2) % 2, u % 2, low : low + n] = v[a : a + n]
                at += n

    def pack(m):
        loaded(m, 0)

        def one(to, carry):
            pack_one(m, to)
            return carry

        lax.fori_loop(0, 4, one, 0)

    def split(k):
        return k // 4, (k // 2) % 2, k % 2

    def x_send(p, i):
        k, r, n = PARTS[p]
        m, hh, rc = split(k)
        peer = along("x", HOPS[i])
        src = sent.at[m, peer, :, lax.rem(c + rc, 2), hh, pl.ds(r, n)]
        push(src, over_x.at[k, x, :, pl.ds(r, n)], xs, xr.at[p], {"x": peer}).start()

    def x_keep(k):
        m, hh, rc = split(k)
        over_x[k, x] = sent[m, x, :, lax.rem(c + rc, 2), hh]

    def x_steps(m):
        for p, (k, _, _) in enumerate(PARTS):
            if k // 4 == m:
                for i in range(3):
                    x_send(p, i)
        for k in range(4 * m, 4 * m + 4):
            x_keep(k)

    def z_step(p):
        k, r, n = PARTS[p]
        rows = pl.ds(r, n)
        bulk(over_x.at[k, 0:3, :, rows], xs, xr.at[p]).wait_recv()
        for h in HOPS:
            peer = along("z", h)
            push(over_x.at[k, peer, :, rows], over_z.at[k, z, :, rows], zs, zr.at[p], {"z": peer}).start()
        over_z[k, z, :, rows] = over_x[k, z, :, rows]

    def lanes(zz):
        return pl.ds(pl.multiple_of((zz * 4 + y) * 128, 128), 128)

    def y_step(p):
        k, r, n = PARTS[p]
        m, hh, rc = split(k)
        bulk(over_z.at[k, 0:3, :, pl.ds(r, n)], zs, zr.at[p]).wait_recv()
        rows = pl.ds(hh * 112 + r, n)
        for h in STEPS if rc else HOPS:
            py = along("y", h)
            peer = {"y": py, "c": lax.rem(c + rc, 2)}
            for zz in range(4):
                push(over_z.at[k, zz, py, pl.ds(r, n)], served.at[m, c, rows, lanes(zz)],
                     ys.at[rc], yr.at[p], peer).start()
        if rc == 0:
            for zz in range(4):
                served[m, c, rows, lanes(zz)] = over_z[k, zz, y, pl.ds(r, n)]

    def y_landed(p):
        k, r, n = PARTS[p]
        rc = k % 2
        bulk(over_z.at[k, 0 : 3 + rc, :, pl.ds(r, n)], ys.at[rc], yr.at[p]).wait_recv()

    for i, h in enumerate(STEPS):
        loaded(0, i)
        pack_one(0, along("x", h))
        if i < 3:
            x_send(0, i)
    for k in range(1, 4):
        for i in range(3):
            x_send(k, i)
    for l in range(3):
        arrived(flows["g", l, 0])
        gather(l, 1)
    pl.semaphore_signal(credit, inc=1, device_id=other, device_id_type=MESH)
    fetch(2)
    for k in range(4):
        x_keep(k)
    z_step(0)
    for l in range(2):
        arrived(flows["g", l, 1])
        spread_out(l)
    pl.semaphore_wait(credit, 1)
    swap(2)
    pack(1)
    x_steps(1)
    arrived(flows["g", 2, 1])
    to_core(2, part(2, 2))
    z_step(1)
    pack(2)
    x_steps(2)
    spread_out(2)
    arrived(share_swaps)
    for b in range(4):
        share_cols[pl.ds(512 * b, 512), 0:8] = jnp.transpose(near_shares[b])

    stores = []

    def store(m):
        cp = pltpu.make_async_copy(served.at[m], outs[m], os.at[m])
        cp.start()
        stores.append(cp)

    early, late = ROUTES[2][0], ROUTES[2][1]

    def act_rows(blocks, first, count):
        m = count * len(blocks)
        total = jnp.zeros((m, 128), jnp.float32)
        for q in range(16):
            block = [tokens[q // 4, q % 4, xb, ch, first : first + count] for xb, ch in blocks]
            block = jnp.concatenate(block, axis=0)
            wide[0:m, 128 * q : 128 * q + 128] = block
            v = block.astype(jnp.float32)
            total = total + v * v
        inv = lax.rsqrt(jnp.sum(total, axis=1, keepdims=True) / 2048.0 + EPSILON)
        dims = (((1,), (1,)), ((), ()))
        for e in range(2):
            gate_pre = lax.dot_general(wide[0:m], served[0, e], dims, preferred_element_type=jnp.float32) * inv
            up_pre = lax.dot_general(wide[0:m], served[1, e], dims, preferred_element_type=jnp.float32) * inv
            act = gate_pre / (1.0 + jnp.exp(-gate_pre)) * up_pre
            for n, (xb, ch) in enumerate(blocks):
                rows = pl.ds(pl.multiple_of((xb * 2 + ch) * 256 + first, 16), count)
                piece = act[count * n : count * n + count] * share_cols[rows, e : e + 1]
                acts[e, rows] = piece.astype(jnp.bfloat16)

    def act_early(xb):
        act_rows([(xb, 0), (xb, 1)], 0, early)

    def act_late(hops):
        act_rows([(along("x", h), ch) for h in hops for ch in (0, 1)], early, late)

    ahead = 2
    for p in range(14):
        while ahead <= min(p + (2 if p < 4 else 4), 19):
            z_step(ahead)
            ahead += 1
        if p == 1:
            pass_on(0)
            pass_on(1)
        if p in (6, 8):
            n = (p - 6) // 2
            arrived(flows["p", n])
            to_core(n, part(n, 3))
        y_step(p)
    z_step(18)
    z_step(19)
    for p in range(12):
        y_landed(p)
    store(0)
    store(1)
    for n in range(2):
        arrived(flows["c", n])
    act_early(0)
    y_step(14)
    act_early(1)
    y_step(15)
    act_early(2)
    y_step(16)
    act_early(3)
    y_step(17)
    pass_on(2)
    arrived(flows["c", 2])
    act_late((0,))
    y_step(18)
    arrived(flows["c", 4])
    arrived(flows["c", 3])
    act_late((1, 3))
    y_step(19)
    arrived(flows["p", 2])
    to_core(5, part(2, 2, {"x": along("x", 2)}))
    arrived(flows["c", 5])
    act_late((2,))
    for p in range(12, 20):
        y_landed(p)
    store(2)

    def down_part(t, n):
        rows = pl.ds(pl.multiple_of(t * 256, 256), 256)
        cols = slice(512 * n, 512 * n + 512)
        v = jnp.dot(acts[0, rows], served[2, 0, :, cols], preferred_element_type=jnp.float32)
        return v + jnp.dot(acts[1, rows], served[2, 1, :, cols], preferred_element_type=jnp.float32)

    given = {}
    for i in FARTHEST_FIRST:
        t = along("x", STEPS[i]) * 2 + 1 - c
        for n in range(4):
            v = down_part(t, n)
            for b in range(4):
                give[i, n, b] = v[:, 128 * b : 128 * b + 128].astype(jnp.bfloat16)
        given[i] = [start(push(give.at[i], near.at[i], ds.at[i], dr.at[i], other))]
    r0, r1, r2 = (pl.ds(*r) for r in ROWS)
    every = slice(None)
    quarter = ROWS[0][1] // 2
    low, high = pl.ds(0, quarter), pl.ds(quarter, quarter)

    def y_block(zz, hop, i):
        return held.at[zz, along("y", hop), i, r1]

    def z_block(yy, hop, i):
        return held.at[along("z", hop), yy, i, r2]

    routes = ((1, "y", y_block, one1, carry1), (2, "z", z_block, one2, carry2))
    pairs = (slice(0, 2), slice(2, 4))

    def send_first(i):
        if i == 2:
            for d, h in enumerate((1, 3)):
                block = held.at[every, every, 2, (low, high)[d]]
                push(block, carry0.at[d], ks.at[0], kr0.at[d], {"x": along("x", h)}).start()
        if i < 2:
            h, rows = STEPS[i], (high, low)[i]
            push(held.at[every, every, i, rows], one0.at[i, every, every, rows], fs.at[0], fr.at[0],
                 {"x": along("x", h)}).start()
        for l, axis, block, one, carry in routes:
            for d, h in enumerate((1, 3)):
                peer = {axis: along(axis, h)}
                push(block(pairs[d], 2, i), carry.at[d, i], ks.at[l], kr.at[l - 1, d, i], peer).start()
            for d, h in enumerate((1, 3)):
                peer = {axis: along(axis, h)}
                rest = pairs[1 - d]
                push(block(rest, h, i), one.at[d, rest, i], fs.at[l], fr.at[l], peer).start()

    def send_carried(i):
        if i == 2:
            for d, h in enumerate((1, 3)):
                bulk(carry0.at[d], ks.at[0], kr0.at[d]).wait_recv()
                rows = (low, high)[d]

                def body(n, carry):
                    a, b = n // 4, lax.rem(n, 4)
                    v = held[a, b, d, rows].astype(jnp.float32) + carry0[d, a, b].astype(jnp.float32)
                    held[a, b, d, rows] = v.astype(jnp.bfloat16)
                    return carry

                lax.fori_loop(0, 16, body, 0)
                push(held.at[every, every, d, rows], one0.at[d, every, every, rows], fs.at[0], fr.at[0],
                     {"x": along("x", h)}).start()
        for l, axis, block, one, carry in routes:
            for d, h in enumerate((1, 3)):
                bulk(carry.at[d, i], ks.at[l], kr.at[l - 1, d, i]).wait_recv()
                ref = block(pairs[d], h, i)
                ref[...] = (ref[...].astype(jnp.float32) + carry[d, i].astype(jnp.float32)).astype(jnp.bfloat16)
                push(block(pairs[d], h, i), one.at[d, pairs[d], i], fs.at[l], fr.at[l],
                     {axis: along(axis, h)}).start()

    for i in FARTHEST_FIRST:
        t = along("x", STEPS[i]) * 2 + c
        arrived(given[i])
        for n in range(4):
            v = down_part(t, n)
            for b in range(4):
                total = v[:, 128 * b : 128 * b + 128] + near[i, n, b].astype(jnp.float32)
                held[n, b, i] = total.astype(jnp.bfloat16)
        send_first(i)
    for i in FARTHEST_FIRST:
        send_carried(i)

    def summed(base, terms):
        v = base.astype(jnp.float32)
        for term in terms:
            v = v + term.astype(jnp.float32)
        return v

    ones, twos, threes = (one0, one1, one2), (two0, two1, two2), (three0, three1, three2)
    adds, sums = (add0, add1, add2), (sum0, sum1, sum2)
    turns = (("y", "z"), ("z", "x"), ("x", "y"))

    def add_first(l, base):
        bulk(ones[l], fs.at[l], fr.at[l]).wait_recv()

        def body(n, carry):
            a, b = n // 4, lax.rem(n, 4)
            adds[l][a, b] = summed(base(a, b), [ones[l][j, a, b] for j in range(2)]).astype(jnp.bfloat16)
            return carry

        lax.fori_loop(0, 16, body, 0)

    def add_second(l, base):
        bulk(twos[l], ss.at[l], sr.at[l]).wait_recv()
        for a in range(4):
            sums[l][a] = summed(base(a), [twos[l][j, a] for j in range(3)]).astype(jnp.bfloat16)

    def send_on(l, s, pick, dst, send, recv):
        axis = turns[l][s]
        for j, h in enumerate(HOPS):
            peer = along(axis, h)
            push(pick(j, peer), dst.at[j], send.at[l], recv.at[l], {axis: peer}).start()

    bases = (lambda a, b: held[a, b, 3, r0], lambda a, b: held[a, y, b, r1], lambda a, b: held[z, a, b, r2])
    picks = (lambda j, p: add0.at[:, p], lambda j, p: add1.at[p], lambda j, p: add2.at[:, j])
    for l in (1, 2, 0):
        add_first(l, bases[l])
        send_on(l, 0, picks[l], twos[l], ss, sr)
    bases = (lambda a: add0[a, y], lambda a: add1[z, a], lambda a: add2[a, 3])
    picks = (lambda j, p: sum0.at[p], lambda j, p: sum1.at[j], lambda j, p: sum2.at[p])
    for l in (1, 2, 0):
        add_second(l, bases[l])
        send_on(l, 1, picks[l], threes[l], ts, tr)
    bases = (lambda: sum0[z], lambda: sum1[3], lambda: sum2[y])
    for l in (1, 2, 0):
        bulk(threes[l], ts.at[l], tr.at[l]).wait_recv()
        total = summed(bases[l](), [threes[l][j] for j in range(3)])
        last[pl.ds(*ROWS[l])] = total.astype(jnp.bfloat16)
    turned[...] = jnp.transpose(last[...].astype(jnp.float32)).astype(jnp.bfloat16)
    rest = turned.at[pl.ds(pl.multiple_of((1 - c) * 64, 64), 64)]
    final = start(push(rest, out.at[:, half], es, er, other))
    out[:, half] = turned[mine]
    final.wait_recv()
    bulk(raw.at[:, 0:3], ps, pr.at[0]).wait_send()
    bulk(over_x.at[:, 0:3], xs, xr.at[0]).wait_send()
    bulk(over_z.at[:, 0:3], zs, zr.at[0]).wait_send()
    for rc in range(2):
        bulk(over_z.at[0:6, 0 : 3 + rc], ys.at[rc], yr.at[0]).wait_send()
    for l, carry in enumerate((carry0, carry1, carry2)):
        bulk(carry, ks.at[l], fr.at[l]).wait_send()
    for l in range(3):
        bulk(ones[l], fs.at[l], fr.at[l]).wait_send()
        bulk(twos[l], ss.at[l], sr.at[l]).wait_send()
        bulk(threes[l], ts.at[l], tr.at[l]).wait_send()
    for cp in sends:
        cp.wait_send()
    for cp in stores:
        cp.wait()


def whole_call(gate, up, down, gain, hidden, ids, logits):
    any_space = pl.BlockSpec(memory_space=pl.ANY)
    vmem = pl.BlockSpec(memory_space=pltpu.VMEM)
    bf16, f32 = jnp.bfloat16, jnp.float32
    dma = pltpu.SemaphoreType.DMA
    sizes = [n for _, n in ROWS]
    served = jax.ShapeDtypeStruct((2, 224, 2048), bf16)

    def buffers(*shapes):
        return [pltpu.VMEM(s, bf16) for s in shapes]

    return pl.pallas_call(
        whole,
        out_shape=(served, served, served, jax.ShapeDtypeStruct((64, 512), bf16)),
        in_specs=[any_space] * 3 + [vmem] * 4,
        out_specs=(any_space,) * 3 + (vmem,),
        scratch_shapes=[pltpu.VMEM((2, 4, 128, 1792), f32)] + [pltpu.VMEM((8, 128), f32)] * 2
        + buffers((3, 4, 4, 2, 2, 112, 128), (CHUNKS, 4, 4, 112, 128), (CHUNKS, 4, 4, 112, 128),
                  (3, 2, 224, 2048), (4, 4, 4, 2, 256, 128), (128, 256))
        + [pltpu.VMEM((4, 8, 512), f32)] * 2
        + [pltpu.VMEM((2048, 128), f32)]
        + buffers((384, 2048), (2, 2048, 224), (4, 4, 4, 256, 128), (4, 4, 4, 256, 128), (4, 4, 4, 256, 128))
        + buffers(*[(2, 4, 4, n, 128) for n in sizes])
        + buffers((2, 4, 4, sizes[0] // 2, 128), (2, 4, 2, sizes[1], 128), (2, 4, 2, sizes[2], 128))
        + buffers(*[(4, 4, n, 128) for n in sizes])
        + buffers(*[(3, 4, n, 128) for n in sizes])
        + buffers(*[(4, n, 128) for n in sizes])
        + buffers(*[(3, n, 128) for n in sizes])
        + buffers((256, 128), (128, 256))
        + [dma((6,)), dma, dma((6,)), pltpu.SemaphoreType.REGULAR]
        + [dma, dma((len(PARTS),)), dma, dma((len(PARTS),)), dma((2,)), dma((len(PARTS),))]
        + [dma] * 4
        + [dma((3,))] * 2
        + [dma((3, 2, 3))] * 2
        + [dma((3, 4))] * 2
        + [dma((6,))] * 2
        + [dma((3,))]
        + [dma((4,))] * 2
        + [dma((3,)), dma((2,)), dma((2, 2, 4))]
        + [dma((3,))] * 6
        + [dma] * 2,
        compiler_params=pltpu.CompilerParams(
            collective_id=0, has_side_effects=True, vmem_limit_bytes=67043328
        ),
        name="whole",
    )(gate, up, down, gain, hidden, ids, logits)


def deliver(*refs):
    sources, results, held, in_sem, out_sem = refs[:4], refs[4:8], refs[8:12], refs[12], refs[13]

    def view(ref, n, k):
        return ref.at[k // 2, pl.ds(112 * (k % 2), 112)] if n < 3 else ref

    steps = [(n, k) for n in range(4) for k in range(4 if n < 3 else 1)]
    loads = [
        pltpu.make_async_copy(view(sources[n], n, k), view(held[n], n, k), in_sem.at[4 * n + k]) for n, k in steps
    ]
    stores = [
        pltpu.make_async_copy(view(held[n], n, k), view(results[n], n, k), out_sem.at[4 * n + k]) for n, k in steps
    ]
    for cp in loads:
        cp.start()
    for load, store in zip(loads, stores):
        load.wait()
        store.start()
    for cp in stores:
        cp.wait()


def deliver_call(*results):
    any_space = pl.BlockSpec(memory_space=pl.ANY)
    return pl.pallas_call(
        deliver,
        out_shape=tuple(jax.ShapeDtypeStruct(r.shape, r.dtype) for r in results),
        in_specs=[any_space] * 4,
        out_specs=(any_space,) * 4,
        scratch_shapes=[pltpu.VMEM(r.shape, r.dtype) for r in results]
        + [pltpu.SemaphoreType.DMA((13,))] * 2,
        name="deliver",
    )(*results)


def per_device(hidden, norm_gain, gate_master, up_master, down_master, expert_ids, route_logits):
    gain = norm_gain.reshape(1, 64)
    masters = [m.reshape(4, 2, 64, 1792) for m in (gate_master, up_master, down_master)]
    results = whole_call(
        *masters, gain, jnp.transpose(hidden), jnp.transpose(expert_ids), jnp.transpose(route_logits)
    )
    gate, up, down, out = deliver_call(*results)
    return jnp.swapaxes(gate, 1, 2), jnp.swapaxes(up, 1, 2), jnp.swapaxes(down, 1, 2), jnp.transpose(out)


def solution(mesh):
    split = Mesh(mesh.devices.reshape(4, 4, 2, mesh.shape["tp"]), ("z", "y", "c", "x"))
    weight = P(None, FS, "x")
    in_specs = (P("x", FS), P(FS), weight, weight, weight, P("x", None), P("x", None))
    served = P("x", None, FS)
    return jax.shard_map(
        per_device,
        mesh=split,
        in_specs=in_specs,
        out_specs=(served, served, served, P("x", FS)),
        check_vma=False,
    )
```

```python
import functools

import jax
import jax.numpy as jnp
from jax import lax
from jax.experimental import pallas as pl
from jax.experimental.pallas import tpu as pltpu
from jax.sharding import Mesh
from jax.sharding import PartitionSpec as P

MESH = pl.DeviceIdType.MESH
EPSILON = 1e-06
FS = ("z", "y", "c")
HOPS = (1, 3, 2)
STEPS = HOPS + (0,)
FARTHEST_FIRST = (2, 0, 1, 3)
ROWS = ((0, 96), (96, 80), (176, 80))
ROUTES = ((0, 64, "xyz"), (64, 96, "xzy"), (160, 96, "zyx"))
CHUNKS = 12
PARTS = tuple((k, r, n) for k in range(CHUNKS) for r, n in ((0, 64), (64, 48)))


def along(axis, hop):
    return lax.rem(lax.axis_index(axis) + hop, 4)


def greet():
    barrier = pltpu.get_barrier_semaphore()
    c = lax.axis_index("c")
    peers = [{a: along(a, h)} for a in ("x", "z") for h in HOPS]
    peers += [{"y": along("y", h), "c": lax.rem(c + r, 2)} for r in (0, 1) for h in (STEPS if r else HOPS)]
    for peer in peers:
        pl.semaphore_signal(barrier, inc=1, device_id=peer, device_id_type=MESH)
    pl.semaphore_wait(barrier, len(peers))


def push(src, dst, send, recv, peer):
    return pltpu.make_async_remote_copy(
        src_ref=src, dst_ref=dst, send_sem=send, recv_sem=recv, device_id=peer, device_id_type=MESH
    )


def whole(gate, up, down, gain, hidden, ids, logits,
          gate_out, up_out, down_out, out,
          raw, doubled, gains, sent, over_x, over_z, served, tokens, chip, shares, near_shares, share_cols,
          wide, acts, far_acts, far_down, held, one0, one1, one2, carry0, carry1, carry2, add0, add1, add2,
          two0, two1, two2, sum0, sum1, sum2, three0, three1, three2, last, turned,
          ls, ps, pr, credit, xs, xr, zs, zr, ys, yr, hs, hr, ns, nr, ws, wr,
          gs, gr, hops, hopr, cs, cr, os, das, dar, dws, dwr, ks, kr0, kr, fs, fr, ss, sr, ts, tr, es, er):
    masters = (gate, up, down)
    outs = (gate_out, up_out, down_out)
    x, y, z, c = (lax.axis_index(a) for a in ("x", "y", "z", "c"))
    other = {"c": 1 - c}
    sends = []

    def start(cp):
        cp.start()
        sends.append(cp)
        return cp

    def bulk(ref, send, recv):
        return push(ref, ref, send, recv, other)

    mine = pl.ds(pl.multiple_of(c * 64, 64), 64)
    def slot(m, i):
        return i if m == 0 else 3 + m

    def fetch(m):
        for i, h in enumerate(STEPS):
            to = along("x", h)
            pltpu.make_async_copy(masters[m].at[to, c], raw.at[m % 2, to, mine], ls.at[slot(m, i)]).start()

    def swap(m):
        for i, h in enumerate(STEPS):
            to = along("x", h)
            push(masters[m].at[to, 1 - c], raw.at[m % 2, to, mine], ps, pr.at[slot(m, i)], other).start()

    def loaded(m, i):
        block = raw.at[0, 0, mine] if m == 0 else raw.at[0, :, mine]
        pltpu.make_async_copy(block, block, ls.at[slot(m, i)]).wait()
        bulk(block, ps, pr.at[slot(m, i)]).wait_recv()

    fetch(0)
    fetch(1)
    half = pl.ds(pl.multiple_of(c * 256, 256), 256)
    far_half = pl.ds(pl.multiple_of((1 - c) * 256, 256), 256)
    chip[mine] = hidden[:, half]
    lane = lax.broadcasted_iota(jnp.int32, (8, 128), 1)
    row = jnp.broadcast_to(gain[...], (8, 64))
    doubled[...] = jnp.concatenate([row, row], axis=1)
    greet()
    halves = start(push(hidden.at[:, far_half], chip.at[mine], hs, hr, other))
    gain_swap = start(push(doubled, gains, ns, nr, other))
    swap(0)

    l0, l1 = logits[0:1], logits[1:2]
    top = jnp.maximum(l0, l1)
    e0, e1 = jnp.exp(l0 - top), jnp.exp(l1 - top)
    w0, w1 = e0 / (e0 + e1), e1 / (e0 + e1)
    for to in range(4):
        expert = lax.broadcasted_iota(jnp.int32, (8, 512), 0) + 2 * to
        shares[to] = jnp.where(ids[0:1] == expert, w0, 0.0) + jnp.where(ids[1:2] == expert, w1, 0.0)
    near_shares[x] = shares[x]
    halves.wait_recv()
    tokens[z, y, x, c] = jnp.transpose(chip[...].astype(jnp.float32)).astype(jnp.bfloat16)
    flows = {}
    spot = {"x": x, "y": y, "z": z}

    def arrived(group):
        for cp in group:
            cp.wait_recv()

    def part(l, s, at=None, half=None):
        first, count, order = ROUTES[l]
        if half is not None:
            first, count = first + half * (count // 2), count // 2
        where = dict(spot, **(at or {}))
        index = tuple(slice(None) if a in order[:s] else where[a] for a in "zyx")
        return tokens.at[index + (c, pl.ds(first, count))]

    def gather(l, s):
        axis = ROUTES[l][2][s]
        flows["g", l, s] = [
            start(push(part(l, s), part(l, s), gs.at[l, s, i], gr.at[l, s, i], {axis: along(axis, h)}))
            for i, h in enumerate(HOPS)
        ]

    for l in range(3):
        gather(l, 0)
    share_swaps = []
    for i, h in enumerate(HOPS):
        peer = along("x", h)
        share_swaps.append(start(push(shares.at[peer], near_shares.at[x], ws.at[i], wr.at[i], {"x": peer})))
    swap(1)
    gain_swap.wait_recv()
    gains[...] = jnp.where((lane < 64) == (c == 0), doubled[...], gains[...])

    def spread_out(l):
        axis = ROUTES[l][2][2]
        flows["n", l] = [
            start(push(part(l, 2), part(l, 2), hops.at[l, i], hopr.at[l, i], {axis: along(axis, h)}))
            for i, h in enumerate((1, 3))
        ]

    def pass_on(l):
        axis = ROUTES[l][2][2]
        flows["p", l] = []
        for i, h in enumerate((1, 3)):
            flows["n", l][i].wait_recv()
            block = part(l, 2, {axis: along(axis, 4 - h)}, i)
            cp = push(block, block, hops.at[l, 2 + i], hopr.at[l, 2 + i], {axis: along(axis, h)})
            flows["p", l].append(start(cp))
            if axis == "x":
                to_core(3 + i, part(l, 2, {axis: along(axis, 4 - h)}))

    def to_core(n, block):
        flows["c", n] = [start(push(block, block, cs.at[n], cr.at[n], other))]

    def pack_one(m, to):
        for t in range(14):
            v = jnp.transpose(raw[m % 2, to, :, 128 * t : 128 * t + 128])
            if m < 2:
                v = v * gains[0:1]
            v = v.astype(jnp.bfloat16)
            at = 128 * t
            while at < 128 * t + 128:
                u, low = divmod(at, 112)
                n = min(112 - low, 128 * t + 128 - at)
                a = at - 128 * t
                sent[m, to, u // 4, (u // 2) % 2, u % 2, low : low + n] = v[a : a + n]
                at += n

    def pack(m):
        loaded(m, 0)

        def one(to, carry):
            pack_one(m, to)
            return carry

        lax.fori_loop(0, 4, one, 0)

    def split(k):
        return k // 4, (k // 2) % 2, k % 2

    def x_send(p, i):
        k, r, n = PARTS[p]
        m, hh, rc = split(k)
        peer = along("x", HOPS[i])
        src = sent.at[m, peer, :, lax.rem(c + rc, 2), hh, pl.ds(r, n)]
        push(src, over_x.at[k, x, :, pl.ds(r, n)], xs, xr.at[p], {"x": peer}).start()

    def x_keep(k):
        m, hh, rc = split(k)
        over_x[k, x] = sent[m, x, :, lax.rem(c + rc, 2), hh]

    def x_steps(m):
        for p, (k, _, _) in enumerate(PARTS):
            if k // 4 == m:
                for i in range(3):
                    x_send(p, i)
        for k in range(4 * m, 4 * m + 4):
            x_keep(k)

    def z_step(p):
        k, r, n = PARTS[p]
        rows = pl.ds(r, n)
        bulk(over_x.at[k, 0:3, :, rows], xs, xr.at[p]).wait_recv()
        for h in HOPS:
            peer = along("z", h)
            push(over_x.at[k, peer, :, rows], over_z.at[k, z, :, rows], zs, zr.at[p], {"z": peer}).start()
        over_z[k, z, :, rows] = over_x[k, z, :, rows]

    def lanes(zz):
        return pl.ds(pl.multiple_of((zz * 4 + y) * 128, 128), 128)

    def y_step(p):
        k, r, n = PARTS[p]
        m, hh, rc = split(k)
        bulk(over_z.at[k, 0:3, :, pl.ds(r, n)], zs, zr.at[p]).wait_recv()
        rows = pl.ds(hh * 112 + r, n)
        for h in STEPS if rc else HOPS:
            py = along("y", h)
            peer = {"y": py, "c": lax.rem(c + rc, 2)}
            for zz in range(4):
                push(over_z.at[k, zz, py, pl.ds(r, n)], served.at[m, c, rows, lanes(zz)],
                     ys.at[rc], yr.at[p], peer).start()
        if rc == 0:
            for zz in range(4):
                served[m, c, rows, lanes(zz)] = over_z[k, zz, y, pl.ds(r, n)]

    def y_landed(p):
        k, r, n = PARTS[p]
        rc = k % 2
        bulk(over_z.at[k, 0 : 3 + rc, :, pl.ds(r, n)], ys.at[rc], yr.at[p]).wait_recv()

    for i, h in enumerate(STEPS):
        loaded(0, i)
        pack_one(0, along("x", h))
        if i < 3:
            x_send(0, i)
    for p in range(1, 8):
        for i in range(3):
            x_send(p, i)
    for l in range(3):
        arrived(flows["g", l, 0])
        gather(l, 1)
    pl.semaphore_signal(credit, inc=1, device_id=other, device_id_type=MESH)
    fetch(2)
    for k in range(4):
        x_keep(k)
    z_step(0)
    z_step(1)
    for l in range(2):
        arrived(flows["g", l, 1])
        spread_out(l)
    pl.semaphore_wait(credit, 1)
    swap(2)
    pack(1)
    x_steps(1)
    arrived(flows["g", 2, 1])
    to_core(2, part(2, 2))
    z_step(2)
    z_step(3)
    pack(2)
    x_steps(2)
    spread_out(2)
    arrived(share_swaps)
    for b in range(4):
        share_cols[pl.ds(512 * b, 512), 0:8] = jnp.transpose(near_shares[b])

    stores = []

    def store(m):
        cp = pltpu.make_async_copy(served.at[m], outs[m], os.at[m])
        cp.start()
        stores.append(cp)

    early, late = ROUTES[2][0], ROUTES[2][1]

    def act_rows(blocks, first, count):
        m = count * len(blocks)
        total = jnp.zeros((m, 128), jnp.float32)
        for q in range(16):
            block = [tokens[q // 4, q % 4, xb, ch, first : first + count] for xb, ch in blocks]
            block = jnp.concatenate(block, axis=0)
            wide[0:m, 128 * q : 128 * q + 128] = block
            v = block.astype(jnp.float32)
            total = total + v * v
        inv = lax.rsqrt(jnp.sum(total, axis=1, keepdims=True) / 2048.0 + EPSILON)
        dims = (((1,), (1,)), ((), ()))
        for e in range(2):
            gate_pre = lax.dot_general(wide[0:m], served[0, e], dims, preferred_element_type=jnp.float32) * inv
            up_pre = lax.dot_general(wide[0:m], served[1, e], dims, preferred_element_type=jnp.float32) * inv
            act = gate_pre / (1.0 + jnp.exp(-gate_pre)) * up_pre
            for n, (xb, ch) in enumerate(blocks):
                rows = pl.ds(pl.multiple_of((xb * 2 + ch) * 256 + first, 16), count)
                piece = act[count * n : count * n + count] * share_cols[rows, e : e + 1]
                acts[e, rows] = piece.astype(jnp.bfloat16)

    def swap_acts(i):
        rows = pl.ds(pl.multiple_of((along("x", STEPS[i]) * 2 + 1 - c) * 256, 256), 256)
        for e in range(2):
            push(acts.at[e, rows], far_acts.at[i, e], das, dar.at[i], other).start()

    def swap_down(p):
        k, r, n = PARTS[p]
        _, hh, rc = split(k)
        y_landed(p)
        rows = pl.ds(hh * 112 + r, n)
        e = lax.rem(c + rc, 2)
        push(served.at[2, e, rows], far_down.at[e, rows], dws, dwr.at[p - 16], other).start()

    def act_early(xb):
        act_rows([(xb, 0), (xb, 1)], 0, early)

    def act_late(hops):
        act_rows([(along("x", h), ch) for h in hops for ch in (0, 1)], early, late)

    ahead = 4
    for p in range(18):
        while ahead <= p + (3 if p < 8 else 4):
            z_step(ahead)
            ahead += 1
        if p == 3:
            pass_on(0)
            pass_on(1)
        if p in (10, 12):
            n = (p - 10) // 2
            arrived(flows["p", n])
            to_core(n, part(n, 3))
        y_step(p)
    z_step(22)
    z_step(23)
    for p in range(16):
        y_landed(p)
    store(0)
    store(1)
    for n in range(2):
        arrived(flows["c", n])
    act_early(0)
    y_step(18)
    act_early(1)
    y_step(19)
    act_early(2)
    y_step(20)
    act_early(3)
    y_step(21)
    pass_on(2)
    arrived(flows["c", 2])
    act_late((0,))
    y_step(22)
    swap_acts(3)
    for p in range(16, 20):
        swap_down(p)
    arrived(flows["c", 4])
    arrived(flows["c", 3])
    act_late((1, 3))
    y_step(23)
    swap_acts(0)
    swap_acts(1)
    swap_down(20)
    swap_down(21)
    arrived(flows["p", 2])
    to_core(5, part(2, 2, {"x": along("x", 2)}))
    arrived(flows["c", 5])
    act_late((2,))
    swap_acts(2)
    swap_down(22)
    swap_down(23)
    store(2)

    def down_part(i, n):
        rows = pl.ds(pl.multiple_of((along("x", STEPS[i]) * 2 + c) * 256, 256), 256)
        cols = slice(512 * n, 512 * n + 512)
        v = 0.0
        for e in range(2):
            v = v + jnp.dot(acts[e, rows], served[2, e, :, cols], preferred_element_type=jnp.float32)
        for e in range(2):
            v = v + jnp.dot(far_acts[i, e], far_down[e, :, cols], preferred_element_type=jnp.float32)
        return v

    for p in range(16, 24):
        k, r, n = PARTS[p]
        block = far_down.at[0, pl.ds(0, n)]
        bulk(block, dws, dwr.at[p - 16]).wait_recv()
    r0, r1, r2 = (pl.ds(*r) for r in ROWS)
    every = slice(None)
    quarter = ROWS[0][1] // 2
    low, high = pl.ds(0, quarter), pl.ds(quarter, quarter)

    def y_block(zz, hop, i):
        return held.at[zz, along("y", hop), i, r1]

    def z_block(yy, hop, i):
        return held.at[along("z", hop), yy, i, r2]

    routes = ((1, "y", y_block, one1, carry1), (2, "z", z_block, one2, carry2))
    pairs = (slice(0, 2), slice(2, 4))

    def send_first(i):
        if i == 2:
            for d, h in enumerate((1, 3)):
                block = held.at[every, every, 2, (low, high)[d]]
                push(block, carry0.at[d], ks.at[0], kr0.at[d], {"x": along("x", h)}).start()
        if i < 2:
            h, rows = STEPS[i], (high, low)[i]
            push(held.at[every, every, i, rows], one0.at[i, every, every, rows], fs.at[0], fr.at[0],
                 {"x": along("x", h)}).start()
        for l, axis, block, one, carry in routes:
            for d, h in enumerate((1, 3)):
                peer = {axis: along(axis, h)}
                push(block(pairs[d], 2, i), carry.at[d, i], ks.at[l], kr.at[l - 1, d, i], peer).start()
            for d, h in enumerate((1, 3)):
                peer = {axis: along(axis, h)}
                rest = pairs[1 - d]
                push(block(rest, h, i), one.at[d, rest, i], fs.at[l], fr.at[l], peer).start()

    def send_carried(i):
        if i == 2:
            for d, h in enumerate((1, 3)):
                bulk(carry0.at[d], ks.at[0], kr0.at[d]).wait_recv()
                rows = (low, high)[d]

                def body(n, carry):
                    a, b = n // 4, lax.rem(n, 4)
                    v = held[a, b, d, rows].astype(jnp.float32) + carry0[d, a, b].astype(jnp.float32)
                    held[a, b, d, rows] = v.astype(jnp.bfloat16)
                    return carry

                lax.fori_loop(0, 16, body, 0)
                push(held.at[every, every, d, rows], one0.at[d, every, every, rows], fs.at[0], fr.at[0],
                     {"x": along("x", h)}).start()
        for l, axis, block, one, carry in routes:
            for d, h in enumerate((1, 3)):
                bulk(carry.at[d, i], ks.at[l], kr.at[l - 1, d, i]).wait_recv()
                ref = block(pairs[d], h, i)
                ref[...] = (ref[...].astype(jnp.float32) + carry[d, i].astype(jnp.float32)).astype(jnp.bfloat16)
                push(block(pairs[d], h, i), one.at[d, pairs[d], i], fs.at[l], fr.at[l],
                     {axis: along(axis, h)}).start()

    for i in FARTHEST_FIRST:
        bulk(far_acts.at[i], das, dar.at[i]).wait_recv()
        for n in range(4):
            v = down_part(i, n).astype(jnp.bfloat16)
            for b in range(4):
                held[n, b, i] = v[:, 128 * b : 128 * b + 128]
        send_first(i)
    for i in FARTHEST_FIRST:
        send_carried(i)

    def summed(base, terms):
        v = base.astype(jnp.float32)
        for term in terms:
            v = v + term.astype(jnp.float32)
        return v

    ones, twos, threes = (one0, one1, one2), (two0, two1, two2), (three0, three1, three2)
    adds, sums = (add0, add1, add2), (sum0, sum1, sum2)
    turns = (("y", "z"), ("z", "x"), ("x", "y"))

    def add_first(l, base):
        bulk(ones[l], fs.at[l], fr.at[l]).wait_recv()

        def body(n, carry):
            a, b = n // 4, lax.rem(n, 4)
            adds[l][a, b] = summed(base(a, b), [ones[l][j, a, b] for j in range(2)]).astype(jnp.bfloat16)
            return carry

        lax.fori_loop(0, 16, body, 0)

    def add_second(l, base):
        bulk(twos[l], ss.at[l], sr.at[l]).wait_recv()
        for a in range(4):
            sums[l][a] = summed(base(a), [twos[l][j, a] for j in range(3)]).astype(jnp.bfloat16)

    def send_on(l, s, pick, dst, send, recv):
        axis = turns[l][s]
        for j in (2, 0, 1):
            peer = along(axis, HOPS[j])
            push(pick(j, peer), dst.at[j], send.at[l], recv.at[l], {axis: peer}).start()

    bases = (lambda a, b: held[a, b, 3, r0], lambda a, b: held[a, y, b, r1], lambda a, b: held[z, a, b, r2])
    picks = (lambda j, p: add0.at[:, p], lambda j, p: add1.at[p], lambda j, p: add2.at[:, j])
    for l in (1, 2, 0):
        add_first(l, bases[l])
        send_on(l, 0, picks[l], twos[l], ss, sr)
    bases = (lambda a: add0[a, y], lambda a: add1[z, a], lambda a: add2[a, 3])
    picks = (lambda j, p: sum0.at[p], lambda j, p: sum1.at[j], lambda j, p: sum2.at[p])
    for l in (1, 2, 0):
        add_second(l, bases[l])
        send_on(l, 1, picks[l], threes[l], ts, tr)
    bases = (lambda: sum0[z], lambda: sum1[3], lambda: sum2[y])
    for l in (1, 2, 0):
        bulk(threes[l], ts.at[l], tr.at[l]).wait_recv()
        total = summed(bases[l](), [threes[l][j] for j in range(3)])
        last[pl.ds(*ROWS[l])] = total.astype(jnp.bfloat16)
    turned[...] = jnp.transpose(last[...].astype(jnp.float32)).astype(jnp.bfloat16)
    rest = turned.at[pl.ds(pl.multiple_of((1 - c) * 64, 64), 64)]
    final = start(push(rest, out.at[:, half], es, er, other))
    out[:, half] = turned[mine]
    final.wait_recv()
    bulk(raw.at[:, 0:3], ps, pr.at[0]).wait_send()
    bulk(over_x.at[:, 0:3], xs, xr.at[0]).wait_send()
    bulk(over_z.at[:, 0:3], zs, zr.at[0]).wait_send()
    for rc in range(2):
        bulk(over_z.at[0:6, 0 : 3 + rc], ys.at[rc], yr.at[0]).wait_send()
    bulk(far_acts, das, dar.at[0]).wait_send()
    bulk(far_down, dws, dwr.at[0]).wait_send()
    for l, carry in enumerate((carry0, carry1, carry2)):
        bulk(carry, ks.at[l], fr.at[l]).wait_send()
    for l in range(3):
        bulk(ones[l], fs.at[l], fr.at[l]).wait_send()
        bulk(twos[l], ss.at[l], sr.at[l]).wait_send()
        bulk(threes[l], ts.at[l], tr.at[l]).wait_send()
    for cp in sends:
        cp.wait_send()
    for cp in stores:
        cp.wait()


def whole_call(gate, up, down, gain, hidden, ids, logits):
    any_space = pl.BlockSpec(memory_space=pl.ANY)
    vmem = pl.BlockSpec(memory_space=pltpu.VMEM)
    bf16, f32 = jnp.bfloat16, jnp.float32
    dma = pltpu.SemaphoreType.DMA
    sizes = [n for _, n in ROWS]
    served = jax.ShapeDtypeStruct((2, 224, 2048), bf16)

    def buffers(*shapes):
        return [pltpu.VMEM(s, bf16) for s in shapes]

    return pl.pallas_call(
        whole,
        out_shape=(served, served, served, jax.ShapeDtypeStruct((64, 512), bf16)),
        in_specs=[any_space] * 3 + [vmem] * 4,
        out_specs=(any_space,) * 3 + (vmem,),
        scratch_shapes=[pltpu.VMEM((2, 4, 128, 1792), f32)] + [pltpu.VMEM((8, 128), f32)] * 2
        + buffers((3, 4, 4, 2, 2, 112, 128), (CHUNKS, 4, 4, 112, 128), (CHUNKS, 4, 4, 112, 128),
                  (3, 2, 224, 2048), (4, 4, 4, 2, 256, 128), (128, 256))
        + [pltpu.VMEM((4, 8, 512), f32)] * 2
        + [pltpu.VMEM((2048, 128), f32)]
        + buffers((384, 2048), (2, 2048, 224), (4, 2, 256, 224), (2, 224, 2048), (4, 4, 4, 256, 128))
        + buffers(*[(2, 4, 4, n, 128) for n in sizes])
        + buffers((2, 4, 4, sizes[0] // 2, 128), (2, 4, 2, sizes[1], 128), (2, 4, 2, sizes[2], 128))
        + buffers(*[(4, 4, n, 128) for n in sizes])
        + buffers(*[(3, 4, n, 128) for n in sizes])
        + buffers(*[(4, n, 128) for n in sizes])
        + buffers(*[(3, n, 128) for n in sizes])
        + buffers((256, 128), (128, 256))
        + [dma((6,)), dma, dma((6,)), pltpu.SemaphoreType.REGULAR]
        + [dma, dma((len(PARTS),)), dma, dma((len(PARTS),)), dma((2,)), dma((len(PARTS),))]
        + [dma] * 4
        + [dma((3,))] * 2
        + [dma((3, 2, 3))] * 2
        + [dma((3, 4))] * 2
        + [dma((6,))] * 2
        + [dma((3,))]
        + [dma, dma((4,)), dma, dma((8,))]
        + [dma((3,)), dma((2,)), dma((2, 2, 4))]
        + [dma((3,))] * 6
        + [dma] * 2,
        compiler_params=pltpu.CompilerParams(
            collective_id=0, has_side_effects=True, vmem_limit_bytes=67043328
        ),
        name="whole",
    )(gate, up, down, gain, hidden, ids, logits)


def deliver(*refs):
    sources, results, held, in_sem, out_sem = refs[:4], refs[4:8], refs[8:12], refs[12], refs[13]

    def view(ref, n, k):
        return ref.at[k // 2, pl.ds(112 * (k % 2), 112)] if n < 3 else ref

    steps = [(n, k) for n in range(4) for k in range(4 if n < 3 else 1)]
    loads = [
        pltpu.make_async_copy(view(sources[n], n, k), view(held[n], n, k), in_sem.at[4 * n + k]) for n, k in steps
    ]
    stores = [
        pltpu.make_async_copy(view(held[n], n, k), view(results[n], n, k), out_sem.at[4 * n + k]) for n, k in steps
    ]
    for cp in loads:
        cp.start()
    for load, store in zip(loads, stores):
        load.wait()
        store.start()
    for cp in stores:
        cp.wait()


def deliver_call(*results):
    any_space = pl.BlockSpec(memory_space=pl.ANY)
    return pl.pallas_call(
        deliver,
        out_shape=tuple(jax.ShapeDtypeStruct(r.shape, r.dtype) for r in results),
        in_specs=[any_space] * 4,
        out_specs=(any_space,) * 4,
        scratch_shapes=[pltpu.VMEM(r.shape, r.dtype) for r in results]
        + [pltpu.SemaphoreType.DMA((13,))] * 2,
        name="deliver",
    )(*results)


def per_device(hidden, norm_gain, gate_master, up_master, down_master, expert_ids, route_logits):
    gain = norm_gain.reshape(1, 64)
    masters = [m.reshape(4, 2, 64, 1792) for m in (gate_master, up_master, down_master)]
    results = whole_call(
        *masters, gain, jnp.transpose(hidden), jnp.transpose(expert_ids), jnp.transpose(route_logits)
    )
    gate, up, down, out = deliver_call(*results)
    return jnp.swapaxes(gate, 1, 2), jnp.swapaxes(up, 1, 2), jnp.swapaxes(down, 1, 2), jnp.transpose(out)


def solution(mesh):
    split = Mesh(mesh.devices.reshape(4, 4, 2, mesh.shape["tp"]), ("z", "y", "c", "x"))
    weight = P(None, FS, "x")
    in_specs = (P("x", FS), P(FS), weight, weight, weight, P("x", None), P("x", None))
    served = P("x", None, FS)
    return jax.shard_map(
        per_device,
        mesh=split,
        in_specs=in_specs,
        out_specs=(served, served, served, P("x", FS)),
        check_vma=False,
    )
```

```python
import functools

import jax
import jax.numpy as jnp
from jax import lax
from jax.experimental import pallas as pl
from jax.experimental.pallas import tpu as pltpu
from jax.sharding import Mesh
from jax.sharding import PartitionSpec as P

MESH = pl.DeviceIdType.MESH
EPSILON = 1e-06
FS = ("z", "y", "c")
HOPS = (1, 3, 2)
STEPS = HOPS + (0,)
FARTHEST_FIRST = (2, 0, 1, 3)
ROWS = ((0, 96), (96, 80), (176, 80))
ROUTES = ((0, 64, "xyz"), (64, 96, "xzy"), (160, 96, "zyx"))
CHUNKS = 12
PARTS = tuple((k, r, n) for k in range(CHUNKS) for r, n in ((0, 64), (64, 48)))


def along(axis, hop):
    return lax.rem(lax.axis_index(axis) + hop, 4)


def greet():
    barrier = pltpu.get_barrier_semaphore()
    c = lax.axis_index("c")
    peers = [{a: along(a, h)} for a in ("x", "z") for h in HOPS]
    peers += [{"y": along("y", h), "c": lax.rem(c + r, 2)} for r in (0, 1) for h in (STEPS if r else HOPS)]
    for peer in peers:
        pl.semaphore_signal(barrier, inc=1, device_id=peer, device_id_type=MESH)
    pl.semaphore_wait(barrier, len(peers))


def push(src, dst, send, recv, peer):
    return pltpu.make_async_remote_copy(
        src_ref=src, dst_ref=dst, send_sem=send, recv_sem=recv, device_id=peer, device_id_type=MESH
    )


def whole(gate, up, down, gain, hidden, ids, logits,
          gate_out, up_out, down_out, out,
          raw, doubled, gains, sent, over_x, over_z, served, tokens, chip, shares, near_shares, share_cols,
          wide, acts, far_acts, far_down, held, one0, one1, one2, carry0, carry1, carry2, add0, add1, add2,
          two0, two1, two2, sum0, sum1, sum2, three0, three1, three2, last, turned,
          ls, ps, pr, credit, xs, xr, zs, zr, ys, yr, hs, hr, ns, nr, ws, wr,
          gs, gr, hops, hopr, cs, cr, os, das, dar, dws, dwr, ks, kr0, kr, fs, fr, ss, sr, ts, tr, es, er):
    masters = (gate, up, down)
    outs = (gate_out, up_out, down_out)
    x, y, z, c = (lax.axis_index(a) for a in ("x", "y", "z", "c"))
    other = {"c": 1 - c}
    sends = []

    def start(cp):
        cp.start()
        sends.append(cp)
        return cp

    def bulk(ref, send, recv):
        return push(ref, ref, send, recv, other)

    mine = pl.ds(pl.multiple_of(c * 64, 64), 64)
    def slot(m, i):
        return i if m == 0 else 3 + m

    def fetch(m):
        for i, h in enumerate(STEPS):
            to = along("x", h)
            pltpu.make_async_copy(masters[m].at[to, c], raw.at[m % 2, to, mine], ls.at[slot(m, i)]).start()

    def swap(m):
        for i, h in enumerate(STEPS):
            to = along("x", h)
            push(masters[m].at[to, 1 - c], raw.at[m % 2, to, mine], ps, pr.at[slot(m, i)], other).start()

    def loaded(m, i):
        block = raw.at[0, 0, mine] if m == 0 else raw.at[0, :, mine]
        pltpu.make_async_copy(block, block, ls.at[slot(m, i)]).wait()
        bulk(block, ps, pr.at[slot(m, i)]).wait_recv()

    fetch(0)
    fetch(1)
    half = pl.ds(pl.multiple_of(c * 256, 256), 256)
    far_half = pl.ds(pl.multiple_of((1 - c) * 256, 256), 256)
    chip[mine] = hidden[:, half]
    lane = lax.broadcasted_iota(jnp.int32, (8, 128), 1)
    row = jnp.broadcast_to(gain[...], (8, 64))
    doubled[...] = jnp.concatenate([row, row], axis=1)
    greet()
    halves = start(push(hidden.at[:, far_half], chip.at[mine], hs, hr, other))
    gain_swap = start(push(doubled, gains, ns, nr, other))
    swap(0)

    l0, l1 = logits[0:1], logits[1:2]
    top = jnp.maximum(l0, l1)
    e0, e1 = jnp.exp(l0 - top), jnp.exp(l1 - top)
    w0, w1 = e0 / (e0 + e1), e1 / (e0 + e1)
    for to in range(4):
        expert = lax.broadcasted_iota(jnp.int32, (8, 512), 0) + 2 * to
        shares[to] = jnp.where(ids[0:1] == expert, w0, 0.0) + jnp.where(ids[1:2] == expert, w1, 0.0)
    near_shares[x] = shares[x]
    halves.wait_recv()
    tokens[z, y, x, c] = jnp.transpose(chip[...].astype(jnp.float32)).astype(jnp.bfloat16)
    flows = {}
    spot = {"x": x, "y": y, "z": z}

    def arrived(group):
        for cp in group:
            cp.wait_recv()

    def part(l, s, at=None, half=None):
        first, count, order = ROUTES[l]
        if half is not None:
            first, count = first + half * (count // 2), count // 2
        where = dict(spot, **(at or {}))
        index = tuple(slice(None) if a in order[:s] else where[a] for a in "zyx")
        return tokens.at[index + (c, pl.ds(first, count))]

    def gather(l, s):
        axis = ROUTES[l][2][s]
        flows["g", l, s] = [
            start(push(part(l, s), part(l, s), gs.at[l, s, i], gr.at[l, s, i], {axis: along(axis, h)}))
            for i, h in enumerate(HOPS)
        ]

    for l in range(3):
        gather(l, 0)
    share_swaps = []
    for i, h in enumerate(HOPS):
        peer = along("x", h)
        share_swaps.append(start(push(shares.at[peer], near_shares.at[x], ws.at[i], wr.at[i], {"x": peer})))
    swap(1)
    gain_swap.wait_recv()
    gains[...] = jnp.where((lane < 64) == (c == 0), doubled[...], gains[...])

    def spread_out(l):
        axis = ROUTES[l][2][2]
        flows["n", l] = [
            start(push(part(l, 2), part(l, 2), hops.at[l, i], hopr.at[l, i], {axis: along(axis, h)}))
            for i, h in enumerate((1, 3))
        ]

    def pass_on(l):
        axis = ROUTES[l][2][2]
        flows["p", l] = []
        for i, h in enumerate((1, 3)):
            flows["n", l][i].wait_recv()
            block = part(l, 2, {axis: along(axis, 4 - h)}, i)
            cp = push(block, block, hops.at[l, 2 + i], hopr.at[l, 2 + i], {axis: along(axis, h)})
            flows["p", l].append(start(cp))
            if axis == "x":
                to_core(3 + i, part(l, 2, {axis: along(axis, 4 - h)}))

    def to_core(n, block):
        flows["c", n] = [start(push(block, block, cs.at[n], cr.at[n], other))]

    def pack_one(m, to):
        for t in range(14):
            v = jnp.transpose(raw[m % 2, to, :, 128 * t : 128 * t + 128])
            if m < 2:
                v = v * gains[0:1]
            v = v.astype(jnp.bfloat16)
            at = 128 * t
            while at < 128 * t + 128:
                u, low = divmod(at, 112)
                n = min(112 - low, 128 * t + 128 - at)
                a = at - 128 * t
                sent[m, to, u // 4, (u // 2) % 2, u % 2, low : low + n] = v[a : a + n]
                at += n

    def pack(m):
        loaded(m, 0)

        def one(to, carry):
            pack_one(m, to)
            return carry

        lax.fori_loop(0, 4, one, 0)

    def split(k):
        return k // 4, (k // 2) % 2, k % 2

    def x_send(p, i):
        k, r, n = PARTS[p]
        m, hh, rc = split(k)
        peer = along("x", HOPS[i])
        src = sent.at[m, peer, :, lax.rem(c + rc, 2), hh, pl.ds(r, n)]
        push(src, over_x.at[k, x, :, pl.ds(r, n)], xs, xr.at[p], {"x": peer}).start()

    def x_keep(k):
        m, hh, rc = split(k)
        over_x[k, x] = sent[m, x, :, lax.rem(c + rc, 2), hh]

    def x_steps(m):
        for p, (k, _, _) in enumerate(PARTS):
            if k // 4 == m:
                for i in range(3):
                    x_send(p, i)
        for k in range(4 * m, 4 * m + 4):
            x_keep(k)

    def z_step(p):
        k, r, n = PARTS[p]
        rows = pl.ds(r, n)
        bulk(over_x.at[k, 0:3, :, rows], xs, xr.at[p]).wait_recv()
        for h in HOPS:
            peer = along("z", h)
            push(over_x.at[k, peer, :, rows], over_z.at[k, z, :, rows], zs, zr.at[p], {"z": peer}).start()
        over_z[k, z, :, rows] = over_x[k, z, :, rows]

    def lanes(zz):
        return pl.ds(pl.multiple_of((zz * 4 + y) * 128, 128), 128)

    def y_step(p):
        k, r, n = PARTS[p]
        m, hh, rc = split(k)
        bulk(over_z.at[k, 0:3, :, pl.ds(r, n)], zs, zr.at[p]).wait_recv()
        rows = pl.ds(hh * 112 + r, n)
        for h in STEPS if rc else HOPS:
            py = along("y", h)
            peer = {"y": py, "c": lax.rem(c + rc, 2)}
            for zz in range(4):
                push(over_z.at[k, zz, py, pl.ds(r, n)], served.at[m, c, rows, lanes(zz)],
                     ys.at[rc], yr.at[p], peer).start()
        if rc == 0:
            for zz in range(4):
                served[m, c, rows, lanes(zz)] = over_z[k, zz, y, pl.ds(r, n)]

    def y_landed(p):
        k, r, n = PARTS[p]
        rc = k % 2
        bulk(over_z.at[k, 0 : 3 + rc, :, pl.ds(r, n)], ys.at[rc], yr.at[p]).wait_recv()

    for i, h in enumerate(STEPS):
        loaded(0, i)
        pack_one(0, along("x", h))
        if i < 3:
            x_send(0, i)
    for p in range(1, 8):
        for i in range(3):
            x_send(p, i)
    for l in range(3):
        arrived(flows["g", l, 0])
        gather(l, 1)
    pl.semaphore_signal(credit, inc=1, device_id=other, device_id_type=MESH)
    fetch(2)
    for k in range(4):
        x_keep(k)
    z_step(0)
    z_step(1)
    for l in range(2):
        arrived(flows["g", l, 1])
        spread_out(l)
    pl.semaphore_wait(credit, 1)
    swap(2)
    pack(1)
    x_steps(1)
    arrived(flows["g", 2, 1])
    to_core(2, part(2, 2))
    z_step(2)
    z_step(3)
    pack(2)
    x_steps(2)
    spread_out(2)
    arrived(share_swaps)
    for b in range(4):
        share_cols[pl.ds(512 * b, 512), 0:8] = jnp.transpose(near_shares[b])

    stores = []

    def store(m):
        cp = pltpu.make_async_copy(served.at[m], outs[m], os.at[m])
        cp.start()
        stores.append(cp)

    early, late = ROUTES[2][0], ROUTES[2][1]

    def act_rows(blocks, first, count):
        m = count * len(blocks)
        total = jnp.zeros((m, 128), jnp.float32)
        for q in range(16):
            block = [tokens[q // 4, q % 4, xb, ch, first : first + count] for xb, ch in blocks]
            block = jnp.concatenate(block, axis=0)
            wide[0:m, 128 * q : 128 * q + 128] = block
            v = block.astype(jnp.float32)
            total = total + v * v
        inv = lax.rsqrt(jnp.sum(total, axis=1, keepdims=True) / 2048.0 + EPSILON)
        dims = (((1,), (1,)), ((), ()))
        for e in range(2):
            gate_pre = lax.dot_general(wide[0:m], served[0, e], dims, preferred_element_type=jnp.float32) * inv
            up_pre = lax.dot_general(wide[0:m], served[1, e], dims, preferred_element_type=jnp.float32) * inv
            act = gate_pre / (1.0 + jnp.exp(-gate_pre)) * up_pre
            for n, (xb, ch) in enumerate(blocks):
                rows = pl.ds(pl.multiple_of((xb * 2 + ch) * 256 + first, 16), count)
                piece = act[count * n : count * n + count] * share_cols[rows, e : e + 1]
                acts[e, rows] = piece.astype(jnp.bfloat16)

    def swap_acts(i):
        rows = pl.ds(pl.multiple_of((along("x", STEPS[i]) * 2 + 1 - c) * 256, 256), 256)
        for e in range(2):
            push(acts.at[e, rows], far_acts.at[i, e], das, dar.at[i], other).start()

    def swap_down(p):
        k, r, n = PARTS[p]
        _, hh, rc = split(k)
        y_landed(p)
        rows = pl.ds(hh * 112 + r, n)
        e = lax.rem(c + rc, 2)
        push(served.at[2, e, rows], far_down.at[e, rows], dws, dwr.at[p - 16], other).start()

    def act_early(xb):
        act_rows([(xb, 0), (xb, 1)], 0, early)

    def act_late(hops):
        act_rows([(along("x", h), ch) for h in hops for ch in (0, 1)], early, late)

    ahead = 4
    for p in range(18):
        while ahead <= p + (3 if p < 8 else 4):
            z_step(ahead)
            ahead += 1
        if p == 3:
            pass_on(0)
            pass_on(1)
        if p in (10, 12):
            n = (p - 10) // 2
            arrived(flows["p", n])
            to_core(n, part(n, 3))
        y_step(p)
    z_step(22)
    z_step(23)
    for p in range(16):
        y_landed(p)
    store(0)
    store(1)
    for n in range(2):
        arrived(flows["c", n])
    act_early(0)
    y_step(18)
    act_early(1)
    y_step(19)
    act_early(2)
    y_step(20)
    act_early(3)
    y_step(21)
    pass_on(2)
    arrived(flows["c", 2])
    act_late((0,))
    y_step(22)
    swap_acts(3)
    for p in range(16, 20):
        swap_down(p)
    arrived(flows["c", 4])
    arrived(flows["c", 3])
    act_late((1, 3))
    y_step(23)
    swap_acts(0)
    swap_acts(1)
    swap_down(20)
    swap_down(21)
    arrived(flows["p", 2])
    to_core(5, part(2, 2, {"x": along("x", 2)}))
    arrived(flows["c", 5])
    act_late((2,))
    swap_acts(2)
    swap_down(22)
    swap_down(23)
    store(2)

    def down_near(i, n):
        rows = pl.ds(pl.multiple_of((along("x", STEPS[i]) * 2 + c) * 256, 256), 256)
        cols = slice(512 * n, 512 * n + 512)
        v = 0.0
        for e in range(2):
            v = v + jnp.dot(acts[e, rows], served[2, e, :, cols], preferred_element_type=jnp.float32)
        return v

    def down_far(i, n, v):
        cols = slice(512 * n, 512 * n + 512)
        for e in range(2):
            v = v + jnp.dot(far_acts[i, e], far_down[e, :, cols], preferred_element_type=jnp.float32)
        return v

    nears = [down_near(FARTHEST_FIRST[0], n) for n in range(4)]
    for p in range(16, 24):
        k, r, n = PARTS[p]
        block = far_down.at[0, pl.ds(0, n)]
        bulk(block, dws, dwr.at[p - 16]).wait_recv()
    r0, r1, r2 = (pl.ds(*r) for r in ROWS)
    every = slice(None)
    quarter = ROWS[0][1] // 2
    low, high = pl.ds(0, quarter), pl.ds(quarter, quarter)

    def y_block(zz, hop, i):
        return held.at[zz, along("y", hop), i, r1]

    def z_block(yy, hop, i):
        return held.at[along("z", hop), yy, i, r2]

    routes = ((1, "y", y_block, one1, carry1), (2, "z", z_block, one2, carry2))
    pairs = (slice(0, 2), slice(2, 4))

    def send_first(i):
        if i < 2:
            h, rows = STEPS[i], (high, low)[i]
            push(held.at[every, every, i, rows], one0.at[i, every, every, rows], fs.at[0], fr.at[0],
                 {"x": along("x", h)}).start()
        for l, axis, block, one, carry in routes:
            for d, h in enumerate((1, 3)):
                peer = {axis: along(axis, h)}
                push(block(pairs[d], 2, i), carry.at[d, i], ks.at[l], kr.at[l - 1, d, i], peer).start()
            for d, h in enumerate((1, 3)):
                peer = {axis: along(axis, h)}
                rest = pairs[1 - d]
                push(block(rest, h, i), one.at[d, rest, i], fs.at[l], fr.at[l], peer).start()

    def send_carried(i):
        if i == 2:
            for d, h in enumerate((1, 3)):
                bulk(carry0.at[d], ks.at[0], kr0.at[d]).wait_recv()
                rows = (low, high)[d]

                def body(n, carry):
                    a, b = n // 4, lax.rem(n, 4)
                    v = held[a, b, d, rows].astype(jnp.float32) + carry0[d, a, b].astype(jnp.float32)
                    held[a, b, d, rows] = v.astype(jnp.bfloat16)
                    return carry

                lax.fori_loop(0, 16, body, 0)
                push(held.at[every, every, d, rows], one0.at[d, every, every, rows], fs.at[0], fr.at[0],
                     {"x": along("x", h)}).start()
        for l, axis, block, one, carry in routes:
            for d, h in enumerate((1, 3)):
                bulk(carry.at[d, i], ks.at[l], kr.at[l - 1, d, i]).wait_recv()
                ref = block(pairs[d], h, i)
                ref[...] = (ref[...].astype(jnp.float32) + carry[d, i].astype(jnp.float32)).astype(jnp.bfloat16)
                push(block(pairs[d], h, i), one.at[d, pairs[d], i], fs.at[l], fr.at[l],
                     {axis: along(axis, h)}).start()

    for i in FARTHEST_FIRST:
        bulk(far_acts.at[i], das, dar.at[i]).wait_recv()
        for n in range(4):
            v = nears[n] if i == FARTHEST_FIRST[0] else down_near(i, n)
            v = down_far(i, n, v).astype(jnp.bfloat16)
            for b in range(4):
                held[n, b, i] = v[:, 128 * b : 128 * b + 128]
            if i == 2:
                for d, h in enumerate((1, 3)):
                    block = held.at[n, every, 2, (low, high)[d]]
                    push(block, carry0.at[d, n], ks.at[0], kr0.at[d], {"x": along("x", h)}).start()
        send_first(i)
    for i in FARTHEST_FIRST:
        send_carried(i)

    def summed(base, terms):
        v = base.astype(jnp.float32)
        for term in terms:
            v = v + term.astype(jnp.float32)
        return v

    ones, twos, threes = (one0, one1, one2), (two0, two1, two2), (three0, three1, three2)
    adds, sums = (add0, add1, add2), (sum0, sum1, sum2)
    turns = (("y", "z"), ("z", "x"), ("x", "y"))

    def add_first(l, base):
        bulk(ones[l], fs.at[l], fr.at[l]).wait_recv()

        def body(n, carry):
            a, b = n // 4, lax.rem(n, 4)
            adds[l][a, b] = summed(base(a, b), [ones[l][j, a, b] for j in range(2)]).astype(jnp.bfloat16)
            return carry

        lax.fori_loop(0, 16, body, 0)

    def add_second(l, base):
        bulk(twos[l], ss.at[l], sr.at[l]).wait_recv()
        for a in range(4):
            sums[l][a] = summed(base(a), [twos[l][j, a] for j in range(3)]).astype(jnp.bfloat16)

    def send_on(l, s, pick, dst, send, recv):
        axis = turns[l][s]
        for j in (2, 0, 1):
            peer = along(axis, HOPS[j])
            push(pick(j, peer), dst.at[j], send.at[l], recv.at[l], {axis: peer}).start()

    bases = (lambda a, b: held[a, b, 3, r0], lambda a, b: held[a, y, b, r1], lambda a, b: held[z, a, b, r2])
    picks = (lambda j, p: add0.at[:, p], lambda j, p: add1.at[p], lambda j, p: add2.at[:, j])
    for l in (1, 2, 0):
        add_first(l, bases[l])
        send_on(l, 0, picks[l], twos[l], ss, sr)
    bases = (lambda a: add0[a, y], lambda a: add1[z, a], lambda a: add2[a, 3])
    picks = (lambda j, p: sum0.at[p], lambda j, p: sum1.at[j], lambda j, p: sum2.at[p])
    for l in (1, 2, 0):
        add_second(l, bases[l])
        send_on(l, 1, picks[l], threes[l], ts, tr)
    bases = (lambda: sum0[z], lambda: sum1[3], lambda: sum2[y])
    for l in (1, 2, 0):
        bulk(threes[l], ts.at[l], tr.at[l]).wait_recv()
        total = summed(bases[l](), [threes[l][j] for j in range(3)])
        last[pl.ds(*ROWS[l])] = total.astype(jnp.bfloat16)
    turned[...] = jnp.transpose(last[...].astype(jnp.float32)).astype(jnp.bfloat16)
    rest = turned.at[pl.ds(pl.multiple_of((1 - c) * 64, 64), 64)]
    final = start(push(rest, out.at[:, half], es, er, other))
    out[:, half] = turned[mine]
    final.wait_recv()
    bulk(raw.at[:, 0:3], ps, pr.at[0]).wait_send()
    bulk(over_x.at[:, 0:3], xs, xr.at[0]).wait_send()
    bulk(over_z.at[:, 0:3], zs, zr.at[0]).wait_send()
    for rc in range(2):
        bulk(over_z.at[0:6, 0 : 3 + rc], ys.at[rc], yr.at[0]).wait_send()
    bulk(far_acts, das, dar.at[0]).wait_send()
    bulk(far_down, dws, dwr.at[0]).wait_send()
    for l, carry in enumerate((carry0, carry1, carry2)):
        bulk(carry, ks.at[l], fr.at[l]).wait_send()
    for l in range(3):
        bulk(ones[l], fs.at[l], fr.at[l]).wait_send()
        bulk(twos[l], ss.at[l], sr.at[l]).wait_send()
        bulk(threes[l], ts.at[l], tr.at[l]).wait_send()
    for cp in sends:
        cp.wait_send()
    for cp in stores:
        cp.wait()


def whole_call(gate, up, down, gain, hidden, ids, logits):
    any_space = pl.BlockSpec(memory_space=pl.ANY)
    vmem = pl.BlockSpec(memory_space=pltpu.VMEM)
    bf16, f32 = jnp.bfloat16, jnp.float32
    dma = pltpu.SemaphoreType.DMA
    sizes = [n for _, n in ROWS]
    served = jax.ShapeDtypeStruct((2, 224, 2048), bf16)

    def buffers(*shapes):
        return [pltpu.VMEM(s, bf16) for s in shapes]

    return pl.pallas_call(
        whole,
        out_shape=(served, served, served, jax.ShapeDtypeStruct((64, 512), bf16)),
        in_specs=[any_space] * 3 + [vmem] * 4,
        out_specs=(any_space,) * 3 + (vmem,),
        scratch_shapes=[pltpu.VMEM((2, 4, 128, 1792), f32)] + [pltpu.VMEM((8, 128), f32)] * 2
        + buffers((3, 4, 4, 2, 2, 112, 128), (CHUNKS, 4, 4, 112, 128), (CHUNKS, 4, 4, 112, 128),
                  (3, 2, 224, 2048), (4, 4, 4, 2, 256, 128), (128, 256))
        + [pltpu.VMEM((4, 8, 512), f32)] * 2
        + [pltpu.VMEM((2048, 128), f32)]
        + buffers((384, 2048), (2, 2048, 224), (4, 2, 256, 224), (2, 224, 2048), (4, 4, 4, 256, 128))
        + buffers(*[(2, 4, 4, n, 128) for n in sizes])
        + buffers((2, 4, 4, sizes[0] // 2, 128), (2, 4, 2, sizes[1], 128), (2, 4, 2, sizes[2], 128))
        + buffers(*[(4, 4, n, 128) for n in sizes])
        + buffers(*[(3, 4, n, 128) for n in sizes])
        + buffers(*[(4, n, 128) for n in sizes])
        + buffers(*[(3, n, 128) for n in sizes])
        + buffers((256, 128), (128, 256))
        + [dma((6,)), dma, dma((6,)), pltpu.SemaphoreType.REGULAR]
        + [dma, dma((len(PARTS),)), dma, dma((len(PARTS),)), dma((2,)), dma((len(PARTS),))]
        + [dma] * 4
        + [dma((3,))] * 2
        + [dma((3, 2, 3))] * 2
        + [dma((3, 4))] * 2
        + [dma((6,))] * 2
        + [dma((3,))]
        + [dma, dma((4,)), dma, dma((8,))]
        + [dma((3,)), dma((2,)), dma((2, 2, 4))]
        + [dma((3,))] * 6
        + [dma] * 2,
        compiler_params=pltpu.CompilerParams(
            collective_id=0, has_side_effects=True, vmem_limit_bytes=67043328
        ),
        name="whole",
    )(gate, up, down, gain, hidden, ids, logits)


def deliver(*refs):
    sources, results, held, in_sem, out_sem = refs[:4], refs[4:8], refs[8:12], refs[12], refs[13]

    def view(ref, n, k):
        return ref.at[k // 2, pl.ds(112 * (k % 2), 112)] if n < 3 else ref

    steps = [(n, k) for n in range(4) for k in range(4 if n < 3 else 1)]
    loads = [
        pltpu.make_async_copy(view(sources[n], n, k), view(held[n], n, k), in_sem.at[4 * n + k]) for n, k in steps
    ]
    stores = [
        pltpu.make_async_copy(view(held[n], n, k), view(results[n], n, k), out_sem.at[4 * n + k]) for n, k in steps
    ]
    for cp in loads:
        cp.start()
    for load, store in zip(loads, stores):
        load.wait()
        store.start()
    for cp in stores:
        cp.wait()


def deliver_call(*results):
    any_space = pl.BlockSpec(memory_space=pl.ANY)
    return pl.pallas_call(
        deliver,
        out_shape=tuple(jax.ShapeDtypeStruct(r.shape, r.dtype) for r in results),
        in_specs=[any_space] * 4,
        out_specs=(any_space,) * 4,
        scratch_shapes=[pltpu.VMEM(r.shape, r.dtype) for r in results]
        + [pltpu.SemaphoreType.DMA((13,))] * 2,
        name="deliver",
    )(*results)


def per_device(hidden, norm_gain, gate_master, up_master, down_master, expert_ids, route_logits):
    gain = norm_gain.reshape(1, 64)
    masters = [m.reshape(4, 2, 64, 1792) for m in (gate_master, up_master, down_master)]
    results = whole_call(
        *masters, gain, jnp.transpose(hidden), jnp.transpose(expert_ids), jnp.transpose(route_logits)
    )
    gate, up, down, out = deliver_call(*results)
    return jnp.swapaxes(gate, 1, 2), jnp.swapaxes(up, 1, 2), jnp.swapaxes(down, 1, 2), jnp.transpose(out)


def solution(mesh):
    split = Mesh(mesh.devices.reshape(4, 4, 2, mesh.shape["tp"]), ("z", "y", "c", "x"))
    weight = P(None, FS, "x")
    in_specs = (P("x", FS), P(FS), weight, weight, weight, P("x", None), P("x", None))
    served = P("x", None, FS)
    return jax.shard_map(
        per_device,
        mesh=split,
        in_specs=in_specs,
        out_specs=(served, served, served, P("x", FS)),
        check_vma=False,
    )
```

```python
import functools

import jax
import jax.numpy as jnp
from jax import lax
from jax.experimental import pallas as pl
from jax.experimental.pallas import tpu as pltpu
from jax.sharding import Mesh
from jax.sharding import PartitionSpec as P

MESH = pl.DeviceIdType.MESH
EPSILON = 1e-06
FS = ("z", "y", "c")
HOPS = (1, 3, 2)
STEPS = HOPS + (0,)
FARTHEST_FIRST = (2, 0, 1, 3)
ROWS = ((0, 96), (96, 80), (176, 80))
ROUTES = ((0, 64, "xyz"), (64, 96, "xzy"), (160, 96, "zyx"))
CHUNKS = 12
PARTS = tuple((k, r, n) for k in range(CHUNKS) for r, n in ((0, 64), (64, 48)))


def along(axis, hop):
    return lax.rem(lax.axis_index(axis) + hop, 4)


def greet():
    barrier = pltpu.get_barrier_semaphore()
    c = lax.axis_index("c")
    peers = [{a: along(a, h)} for a in ("x", "z") for h in HOPS]
    peers += [{"y": along("y", h), "c": lax.rem(c + r, 2)} for r in (0, 1) for h in (STEPS if r else HOPS)]
    for peer in peers:
        pl.semaphore_signal(barrier, inc=1, device_id=peer, device_id_type=MESH)
    pl.semaphore_wait(barrier, len(peers))


def push(src, dst, send, recv, peer):
    return pltpu.make_async_remote_copy(
        src_ref=src, dst_ref=dst, send_sem=send, recv_sem=recv, device_id=peer, device_id_type=MESH
    )


def whole(gate, up, down, gain, hidden, ids, logits,
          gate_out, up_out, down_out, out,
          raw, doubled, gains, sent, over_x, over_z, served, tokens, chip, shares, near_shares, share_cols,
          wide, acts, far_acts, far_down, held, one0, one1, one2, carry0, carry1, carry2, add0, add1, add2,
          two0, two1, two2, sum0, sum1, sum2, three0, three1, three2, last, turned,
          ls, ps, pr, credit, xs, xr, zs, zr, ys, yr, hs, hr, ns, nr, ws, wr,
          gs, gr, hops, hopr, cs, cr, os, das, dar, dws, dwr, ks, kr0, kr, fs, fr, ss, sr, ts, tr, es, er):
    masters = (gate, up, down)
    outs = (gate_out, up_out, down_out)
    x, y, z, c = (lax.axis_index(a) for a in ("x", "y", "z", "c"))
    other = {"c": 1 - c}
    sends = []

    def start(cp):
        cp.start()
        sends.append(cp)
        return cp

    def bulk(ref, send, recv):
        return push(ref, ref, send, recv, other)

    mine = pl.ds(pl.multiple_of(c * 64, 64), 64)
    def slot(m, i):
        return i if m == 0 else 3 + m

    def fetch(m):
        for i, h in enumerate(STEPS):
            to = along("x", h)
            pltpu.make_async_copy(masters[m].at[to, c], raw.at[m % 2, to, mine], ls.at[slot(m, i)]).start()

    def swap(m):
        for i, h in enumerate(STEPS):
            to = along("x", h)
            push(masters[m].at[to, 1 - c], raw.at[m % 2, to, mine], ps, pr.at[slot(m, i)], other).start()

    def loaded(m, i):
        block = raw.at[0, 0, mine] if m == 0 else raw.at[0, :, mine]
        pltpu.make_async_copy(block, block, ls.at[slot(m, i)]).wait()
        bulk(block, ps, pr.at[slot(m, i)]).wait_recv()

    fetch(0)
    fetch(1)
    half = pl.ds(pl.multiple_of(c * 256, 256), 256)
    far_half = pl.ds(pl.multiple_of((1 - c) * 256, 256), 256)
    chip[mine] = hidden[:, half]
    lane = lax.broadcasted_iota(jnp.int32, (8, 128), 1)
    row = jnp.broadcast_to(gain[...], (8, 64))
    doubled[...] = jnp.concatenate([row, row], axis=1)
    greet()
    halves = start(push(hidden.at[:, far_half], chip.at[mine], hs, hr, other))
    gain_swap = start(push(doubled, gains, ns, nr, other))
    swap(0)

    l0, l1 = logits[0:1], logits[1:2]
    top = jnp.maximum(l0, l1)
    e0, e1 = jnp.exp(l0 - top), jnp.exp(l1 - top)
    w0, w1 = e0 / (e0 + e1), e1 / (e0 + e1)
    for to in range(4):
        expert = lax.broadcasted_iota(jnp.int32, (8, 512), 0) + 2 * to
        shares[to] = jnp.where(ids[0:1] == expert, w0, 0.0) + jnp.where(ids[1:2] == expert, w1, 0.0)
    near_shares[x] = shares[x]
    halves.wait_recv()
    tokens[z, y, x, c] = jnp.transpose(chip[...].astype(jnp.float32)).astype(jnp.bfloat16)
    flows = {}
    spot = {"x": x, "y": y, "z": z}

    def arrived(group):
        for cp in group:
            cp.wait_recv()

    def part(l, s, at=None, half=None):
        first, count, order = ROUTES[l]
        if half is not None:
            first, count = first + half * (count // 2), count // 2
        where = dict(spot, **(at or {}))
        index = tuple(slice(None) if a in order[:s] else where[a] for a in "zyx")
        return tokens.at[index + (c, pl.ds(first, count))]

    def gather(l, s):
        axis = ROUTES[l][2][s]
        for h in HOPS:
            push(part(l, s), part(l, s), gs.at[l, s], gr.at[l, s], {axis: along(axis, h)}).start()
        rows = pl.ds(0, ROUTES[l][1])
        three = tokens.at[0, 0:3, :, 0, rows] if s else tokens.at[0, 0, 0:3, 0, rows]
        all_three = bulk(three, gs.at[l, s], gr.at[l, s])
        sends.append(all_three)
        flows["g", l, s] = [all_three]

    for l in range(3):
        gather(l, 0)
    share_swaps = []
    for i, h in enumerate(HOPS):
        peer = along("x", h)
        share_swaps.append(start(push(shares.at[peer], near_shares.at[x], ws.at[i], wr.at[i], {"x": peer})))
    swap(1)
    gain_swap.wait_recv()
    gains[...] = jnp.where((lane < 64) == (c == 0), doubled[...], gains[...])

    def spread_out(l):
        axis = ROUTES[l][2][2]
        flows["n", l] = [
            start(push(part(l, 2), part(l, 2), hops.at[l, i], hopr.at[l, i], {axis: along(axis, h)}))
            for i, h in enumerate((1, 3))
        ]

    def pass_on(l):
        axis = ROUTES[l][2][2]
        flows["p", l] = []
        for i, h in enumerate((1, 3)):
            flows["n", l][i].wait_recv()
            block = part(l, 2, {axis: along(axis, 4 - h)}, i)
            cp = push(block, block, hops.at[l, 2 + i], hopr.at[l, 2 + i], {axis: along(axis, h)})
            flows["p", l].append(start(cp))
            if axis == "x":
                to_core(3 + i, part(l, 2, {axis: along(axis, 4 - h)}))

    def to_core(n, block):
        flows["c", n] = [start(push(block, block, cs.at[n], cr.at[n], other))]

    def pack_one(m, to):
        for t in range(14):
            v = jnp.transpose(raw[m % 2, to, :, 128 * t : 128 * t + 128])
            if m < 2:
                v = v * gains[0:1]
            v = v.astype(jnp.bfloat16)
            at = 128 * t
            while at < 128 * t + 128:
                u, low = divmod(at, 112)
                n = min(112 - low, 128 * t + 128 - at)
                a = at - 128 * t
                sent[m, to, u // 4, (u // 2) % 2, u % 2, low : low + n] = v[a : a + n]
                at += n

    def pack(m):
        loaded(m, 0)

        def one(to, carry):
            pack_one(m, to)
            return carry

        lax.fori_loop(0, 4, one, 0)

    def split(k):
        return k // 4, (k // 2) % 2, k % 2

    def x_send(p, i):
        k, r, n = PARTS[p]
        m, hh, rc = split(k)
        peer = along("x", HOPS[i])
        src = sent.at[m, peer, :, lax.rem(c + rc, 2), hh, pl.ds(r, n)]
        push(src, over_x.at[k, x, :, pl.ds(r, n)], xs, xr.at[p], {"x": peer}).start()

    def x_keep(k):
        m, hh, rc = split(k)
        over_x[k, x] = sent[m, x, :, lax.rem(c + rc, 2), hh]

    def x_steps(m):
        for p, (k, _, _) in enumerate(PARTS):
            if k // 4 == m:
                for i in range(3):
                    x_send(p, i)
        for k in range(4 * m, 4 * m + 4):
            x_keep(k)

    def z_step(p):
        k, r, n = PARTS[p]
        rows = pl.ds(r, n)
        bulk(over_x.at[k, 0:3, :, rows], xs, xr.at[p]).wait_recv()
        for h in HOPS:
            peer = along("z", h)
            push(over_x.at[k, peer, :, rows], over_z.at[k, z, :, rows], zs, zr.at[p], {"z": peer}).start()
        over_z[k, z, :, rows] = over_x[k, z, :, rows]

    def lanes(zz):
        return pl.ds(pl.multiple_of((zz * 4 + y) * 128, 128), 128)

    def y_step(p):
        k, r, n = PARTS[p]
        m, hh, rc = split(k)
        bulk(over_z.at[k, 0:3, :, pl.ds(r, n)], zs, zr.at[p]).wait_recv()
        rows = pl.ds(hh * 112 + r, n)
        for h in STEPS if rc else HOPS:
            py = along("y", h)
            peer = {"y": py, "c": lax.rem(c + rc, 2)}
            for zz in range(4):
                push(over_z.at[k, zz, py, pl.ds(r, n)], served.at[m, c, rows, lanes(zz)],
                     ys.at[rc], yr.at[p], peer).start()
        if rc == 0:
            for zz in range(4):
                served[m, c, rows, lanes(zz)] = over_z[k, zz, y, pl.ds(r, n)]

    def y_landed(p):
        k, r, n = PARTS[p]
        rc = k % 2
        bulk(over_z.at[k, 0 : 3 + rc, :, pl.ds(r, n)], ys.at[rc], yr.at[p]).wait_recv()

    for i, h in enumerate(STEPS):
        loaded(0, i)
        pack_one(0, along("x", h))
        if i < 3:
            x_send(0, i)
    for p in range(1, 8):
        for i in range(3):
            x_send(p, i)
    for l in range(3):
        arrived(flows["g", l, 0])
        gather(l, 1)
    pl.semaphore_signal(credit, inc=1, device_id=other, device_id_type=MESH)
    fetch(2)
    for k in range(4):
        x_keep(k)
    z_step(0)
    z_step(1)
    for l in range(2):
        arrived(flows["g", l, 1])
        spread_out(l)
    pl.semaphore_wait(credit, 1)
    swap(2)
    pack(1)
    x_steps(1)
    arrived(flows["g", 2, 1])
    to_core(2, part(2, 2))
    z_step(2)
    z_step(3)
    pack(2)
    x_steps(2)
    spread_out(2)
    arrived(share_swaps)
    for b in range(4):
        share_cols[pl.ds(512 * b, 512), 0:8] = jnp.transpose(near_shares[b])

    stores = []

    def store(m):
        cp = pltpu.make_async_copy(served.at[m], outs[m], os.at[m])
        cp.start()
        stores.append(cp)

    early, late = ROUTES[2][0], ROUTES[2][1]

    def act_rows(blocks, first, count):
        m = count * len(blocks)
        total = jnp.zeros((m, 128), jnp.float32)
        for q in range(16):
            block = [tokens[q // 4, q % 4, xb, ch, first : first + count] for xb, ch in blocks]
            block = jnp.concatenate(block, axis=0)
            wide[0:m, 128 * q : 128 * q + 128] = block
            v = block.astype(jnp.float32)
            total = total + v * v
        inv = lax.rsqrt(jnp.sum(total, axis=1, keepdims=True) / 2048.0 + EPSILON)
        dims = (((1,), (1,)), ((), ()))
        for e in range(2):
            gate_pre = lax.dot_general(wide[0:m], served[0, e], dims, preferred_element_type=jnp.float32) * inv
            up_pre = lax.dot_general(wide[0:m], served[1, e], dims, preferred_element_type=jnp.float32) * inv
            act = gate_pre / (1.0 + jnp.exp(-gate_pre)) * up_pre
            for n, (xb, ch) in enumerate(blocks):
                rows = pl.ds(pl.multiple_of((xb * 2 + ch) * 256 + first, 16), count)
                piece = act[count * n : count * n + count] * share_cols[rows, e : e + 1]
                acts[e, rows] = piece.astype(jnp.bfloat16)

    def swap_acts(i):
        rows = pl.ds(pl.multiple_of((along("x", STEPS[i]) * 2 + 1 - c) * 256, 256), 256)
        for e in range(2):
            push(acts.at[e, rows], far_acts.at[i, e], das, dar.at[i], other).start()

    def swap_down(p):
        k, r, n = PARTS[p]
        _, hh, rc = split(k)
        y_landed(p)
        rows = pl.ds(hh * 112 + r, n)
        e = lax.rem(c + rc, 2)
        push(served.at[2, e, rows], far_down.at[e, rows], dws, dwr.at[p - 16], other).start()

    def act_early(xb):
        act_rows([(xb, 0), (xb, 1)], 0, early)

    def act_late(hops):
        act_rows([(along("x", h), ch) for h in hops for ch in (0, 1)], early, late)

    ahead = 4
    for p in range(18):
        while ahead <= p + (3 if p < 8 else 4):
            z_step(ahead)
            ahead += 1
        if p == 3:
            pass_on(0)
            pass_on(1)
        if p in (10, 12):
            n = (p - 10) // 2
            arrived(flows["p", n])
            to_core(n, part(n, 3))
        y_step(p)
    z_step(22)
    z_step(23)
    for p in range(16):
        y_landed(p)
    store(0)
    store(1)
    for n in range(2):
        arrived(flows["c", n])
    act_early(0)
    y_step(18)
    act_early(1)
    y_step(19)
    act_early(2)
    y_step(20)
    act_early(3)
    y_step(21)
    pass_on(2)
    arrived(flows["c", 2])
    act_late((0,))
    y_step(22)
    swap_acts(3)
    for p in range(16, 20):
        swap_down(p)
    arrived(flows["c", 4])
    arrived(flows["c", 3])
    act_late((1, 3))
    y_step(23)
    swap_acts(0)
    swap_acts(1)
    swap_down(20)
    swap_down(21)
    arrived(flows["p", 2])
    to_core(5, part(2, 2, {"x": along("x", 2)}))
    arrived(flows["c", 5])
    act_late((2,))
    swap_acts(2)
    swap_down(22)
    swap_down(23)
    store(2)

    def down_near(i, n):
        rows = pl.ds(pl.multiple_of((along("x", STEPS[i]) * 2 + c) * 256, 256), 256)
        cols = slice(512 * n, 512 * n + 512)
        v = 0.0
        for e in range(2):
            v = v + jnp.dot(acts[e, rows], served[2, e, :, cols], preferred_element_type=jnp.float32)
        return v

    def down_far(i, n, v):
        cols = slice(512 * n, 512 * n + 512)
        for e in range(2):
            v = v + jnp.dot(far_acts[i, e], far_down[e, :, cols], preferred_element_type=jnp.float32)
        return v

    nears = [down_near(FARTHEST_FIRST[0], n) for n in range(4)]
    for p in range(16, 24):
        k, r, n = PARTS[p]
        block = far_down.at[0, pl.ds(0, n)]
        bulk(block, dws, dwr.at[p - 16]).wait_recv()
    r0, r1, r2 = (pl.ds(*r) for r in ROWS)
    every = slice(None)
    quarter = ROWS[0][1] // 2
    low, high = pl.ds(0, quarter), pl.ds(quarter, quarter)

    def y_block(zz, hop, i):
        return held.at[zz, along("y", hop), i, r1]

    def z_block(yy, hop, i):
        return held.at[along("z", hop), yy, i, r2]

    routes = ((1, "y", y_block, one1, carry1), (2, "z", z_block, one2, carry2))
    pairs = (slice(0, 2), slice(2, 4))

    def send_first(i):
        if i < 2:
            h, rows = STEPS[i], (high, low)[i]
            push(held.at[every, every, i, rows], one0.at[i, every, every, rows], fs.at[0], fr.at[0],
                 {"x": along("x", h)}).start()
        for l, axis, block, one, carry in routes:
            for d, h in enumerate((1, 3)):
                peer = {axis: along(axis, h)}
                push(block(pairs[d], 2, i), carry.at[d, i], ks.at[l], kr.at[l - 1, d, i], peer).start()
            for d, h in enumerate((1, 3)):
                peer = {axis: along(axis, h)}
                rest = pairs[1 - d]
                push(block(rest, h, i), one.at[d, rest, i], fs.at[l], fr.at[l], peer).start()

    def send_carried(i):
        if i == 2:
            for d, h in enumerate((1, 3)):
                bulk(carry0.at[d], ks.at[0], kr0.at[d]).wait_recv()
                rows = (low, high)[d]

                def body(n, carry):
                    a, b = n // 4, lax.rem(n, 4)
                    v = held[a, b, d, rows].astype(jnp.float32) + carry0[d, a, b].astype(jnp.float32)
                    held[a, b, d, rows] = v.astype(jnp.bfloat16)
                    return carry

                lax.fori_loop(0, 16, body, 0)
                push(held.at[every, every, d, rows], one0.at[d, every, every, rows], fs.at[0], fr.at[0],
                     {"x": along("x", h)}).start()
        for l, axis, block, one, carry in routes:
            for d, h in enumerate((1, 3)):
                bulk(carry.at[d, i], ks.at[l], kr.at[l - 1, d, i]).wait_recv()
                ref = block(pairs[d], h, i)
                ref[...] = (ref[...].astype(jnp.float32) + carry[d, i].astype(jnp.float32)).astype(jnp.bfloat16)
                push(block(pairs[d], h, i), one.at[d, pairs[d], i], fs.at[l], fr.at[l],
                     {axis: along(axis, h)}).start()

    for i in FARTHEST_FIRST:
        bulk(far_acts.at[i], das, dar.at[i]).wait_recv()
        for n in range(4):
            v = nears[n] if i == FARTHEST_FIRST[0] else down_near(i, n)
            v = down_far(i, n, v).astype(jnp.bfloat16)
            for b in range(4):
                held[n, b, i] = v[:, 128 * b : 128 * b + 128]
            if i == 2:
                for d, h in enumerate((1, 3)):
                    block = held.at[n, every, 2, (low, high)[d]]
                    push(block, carry0.at[d, n], ks.at[0], kr0.at[d], {"x": along("x", h)}).start()
        send_first(i)
    for i in FARTHEST_FIRST:
        send_carried(i)

    def summed(base, terms):
        v = base.astype(jnp.float32)
        for term in terms:
            v = v + term.astype(jnp.float32)
        return v

    ones, twos, threes = (one0, one1, one2), (two0, two1, two2), (three0, three1, three2)
    adds, sums = (add0, add1, add2), (sum0, sum1, sum2)
    turns = (("y", "z"), ("z", "x"), ("x", "y"))

    def add_first(l, base):
        bulk(ones[l], fs.at[l], fr.at[l]).wait_recv()

        def body(n, carry):
            a, b = n // 4, lax.rem(n, 4)
            adds[l][a, b] = summed(base(a, b), [ones[l][j, a, b] for j in range(2)]).astype(jnp.bfloat16)
            return carry

        lax.fori_loop(0, 16, body, 0)

    def add_second(l, base):
        bulk(twos[l], ss.at[l], sr.at[l]).wait_recv()
        for a in range(4):
            sums[l][a] = summed(base(a), [twos[l][j, a] for j in range(3)]).astype(jnp.bfloat16)

    def send_on(l, s, pick, dst, send, recv):
        axis = turns[l][s]
        for j in (2, 0, 1):
            peer = along(axis, HOPS[j])
            push(pick(j, peer), dst.at[j], send.at[l], recv.at[l], {axis: peer}).start()

    bases = (lambda a, b: held[a, b, 3, r0], lambda a, b: held[a, y, b, r1], lambda a, b: held[z, a, b, r2])
    picks = (lambda j, p: add0.at[:, p], lambda j, p: add1.at[p], lambda j, p: add2.at[:, j])
    for l in (1, 2, 0):
        add_first(l, bases[l])
        send_on(l, 0, picks[l], twos[l], ss, sr)
    bases = (lambda a: add0[a, y], lambda a: add1[z, a], lambda a: add2[a, 3])
    picks = (lambda j, p: sum0.at[p], lambda j, p: sum1.at[j], lambda j, p: sum2.at[p])
    for l in (1, 2, 0):
        add_second(l, bases[l])
        send_on(l, 1, picks[l], threes[l], ts, tr)
    bases = (lambda: sum0[z], lambda: sum1[3], lambda: sum2[y])
    for l in (1, 2, 0):
        bulk(threes[l], ts.at[l], tr.at[l]).wait_recv()
        total = summed(bases[l](), [threes[l][j] for j in range(3)])
        last[pl.ds(*ROWS[l])] = total.astype(jnp.bfloat16)
    turned[...] = jnp.transpose(last[...].astype(jnp.float32)).astype(jnp.bfloat16)
    rest = turned.at[pl.ds(pl.multiple_of((1 - c) * 64, 64), 64)]
    final = start(push(rest, out.at[:, half], es, er, other))
    out[:, half] = turned[mine]
    final.wait_recv()
    bulk(raw.at[:, 0:3], ps, pr.at[0]).wait_send()
    bulk(over_x.at[:, 0:3], xs, xr.at[0]).wait_send()
    bulk(over_z.at[:, 0:3], zs, zr.at[0]).wait_send()
    for rc in range(2):
        bulk(over_z.at[0:6, 0 : 3 + rc], ys.at[rc], yr.at[0]).wait_send()
    bulk(far_acts, das, dar.at[0]).wait_send()
    bulk(far_down, dws, dwr.at[0]).wait_send()
    for l, carry in enumerate((carry0, carry1, carry2)):
        bulk(carry, ks.at[l], fr.at[l]).wait_send()
    for l in range(3):
        bulk(ones[l], fs.at[l], fr.at[l]).wait_send()
        bulk(twos[l], ss.at[l], sr.at[l]).wait_send()
        bulk(threes[l], ts.at[l], tr.at[l]).wait_send()
    for cp in sends:
        cp.wait_send()
    for cp in stores:
        cp.wait()


def whole_call(gate, up, down, gain, hidden, ids, logits):
    any_space = pl.BlockSpec(memory_space=pl.ANY)
    vmem = pl.BlockSpec(memory_space=pltpu.VMEM)
    bf16, f32 = jnp.bfloat16, jnp.float32
    dma = pltpu.SemaphoreType.DMA
    sizes = [n for _, n in ROWS]
    served = jax.ShapeDtypeStruct((2, 224, 2048), bf16)

    def buffers(*shapes):
        return [pltpu.VMEM(s, bf16) for s in shapes]

    return pl.pallas_call(
        whole,
        out_shape=(served, served, served, jax.ShapeDtypeStruct((64, 512), bf16)),
        in_specs=[any_space] * 3 + [vmem] * 4,
        out_specs=(any_space,) * 3 + (vmem,),
        scratch_shapes=[pltpu.VMEM((2, 4, 128, 1792), f32)] + [pltpu.VMEM((8, 128), f32)] * 2
        + buffers((3, 4, 4, 2, 2, 112, 128), (CHUNKS, 4, 4, 112, 128), (CHUNKS, 4, 4, 112, 128),
                  (3, 2, 224, 2048), (4, 4, 4, 2, 256, 128), (128, 256))
        + [pltpu.VMEM((4, 8, 512), f32)] * 2
        + [pltpu.VMEM((2048, 128), f32)]
        + buffers((384, 2048), (2, 2048, 224), (4, 2, 256, 224), (2, 224, 2048), (4, 4, 4, 256, 128))
        + buffers(*[(2, 4, 4, n, 128) for n in sizes])
        + buffers((2, 4, 4, sizes[0] // 2, 128), (2, 4, 2, sizes[1], 128), (2, 4, 2, sizes[2], 128))
        + buffers(*[(4, 4, n, 128) for n in sizes])
        + buffers(*[(3, 4, n, 128) for n in sizes])
        + buffers(*[(4, n, 128) for n in sizes])
        + buffers(*[(3, n, 128) for n in sizes])
        + buffers((256, 128), (128, 256))
        + [dma((6,)), dma, dma((6,)), pltpu.SemaphoreType.REGULAR]
        + [dma, dma((len(PARTS),)), dma, dma((len(PARTS),)), dma((2,)), dma((len(PARTS),))]
        + [dma] * 4
        + [dma((3,))] * 2
        + [dma((3, 2))] * 2
        + [dma((3, 4))] * 2
        + [dma((6,))] * 2
        + [dma((3,))]
        + [dma, dma((4,)), dma, dma((8,))]
        + [dma((3,)), dma((2,)), dma((2, 2, 4))]
        + [dma((3,))] * 6
        + [dma] * 2,
        compiler_params=pltpu.CompilerParams(
            collective_id=0, has_side_effects=True, vmem_limit_bytes=67043328
        ),
        name="whole",
    )(gate, up, down, gain, hidden, ids, logits)


def deliver(*refs):
    sources, results, held, in_sem, out_sem = refs[:4], refs[4:8], refs[8:12], refs[12], refs[13]

    def view(ref, n, k):
        return ref.at[k // 2, pl.ds(112 * (k % 2), 112)] if n < 3 else ref

    steps = [(n, k) for n in range(4) for k in range(4 if n < 3 else 1)]
    loads = [
        pltpu.make_async_copy(view(sources[n], n, k), view(held[n], n, k), in_sem.at[4 * n + k]) for n, k in steps
    ]
    stores = [
        pltpu.make_async_copy(view(held[n], n, k), view(results[n], n, k), out_sem.at[4 * n + k]) for n, k in steps
    ]
    for cp in loads:
        cp.start()
    for load, store in zip(loads, stores):
        load.wait()
        store.start()
    for cp in stores:
        cp.wait()


def deliver_call(*results):
    any_space = pl.BlockSpec(memory_space=pl.ANY)
    return pl.pallas_call(
        deliver,
        out_shape=tuple(jax.ShapeDtypeStruct(r.shape, r.dtype) for r in results),
        in_specs=[any_space] * 4,
        out_specs=(any_space,) * 4,
        scratch_shapes=[pltpu.VMEM(r.shape, r.dtype) for r in results]
        + [pltpu.SemaphoreType.DMA((13,))] * 2,
        name="deliver",
    )(*results)


def per_device(hidden, norm_gain, gate_master, up_master, down_master, expert_ids, route_logits):
    gain = norm_gain.reshape(1, 64)
    masters = [m.reshape(4, 2, 64, 1792) for m in (gate_master, up_master, down_master)]
    results = whole_call(
        *masters, gain, jnp.transpose(hidden), jnp.transpose(expert_ids), jnp.transpose(route_logits)
    )
    gate, up, down, out = deliver_call(*results)
    return jnp.swapaxes(gate, 1, 2), jnp.swapaxes(up, 1, 2), jnp.swapaxes(down, 1, 2), jnp.transpose(out)


def solution(mesh):
    split = Mesh(mesh.devices.reshape(4, 4, 2, mesh.shape["tp"]), ("z", "y", "c", "x"))
    weight = P(None, FS, "x")
    in_specs = (P("x", FS), P(FS), weight, weight, weight, P("x", None), P("x", None))
    served = P("x", None, FS)
    return jax.shard_map(
        per_device,
        mesh=split,
        in_specs=in_specs,
        out_specs=(served, served, served, P("x", FS)),
        check_vma=False,
    )
```
